32 devices in a mesh: grp: 2 (over y), dp: 2 (over x), kv: 4 (over z), tp: 2 (over core).
Axes of the slice: x: 2, y: 2, z: 4, core: 2. Of those that a mesh axis runs over, the one named last changes fastest.
Arguments:
- tokens: bfloat16 [64, 4, 4096], P(('grp', 'dp'), None, 'kv'), parts along dimension 0, may hold values from -6 to 6
- w_query: bfloat16 [4096, 2048], P('kv', 'tp'), may hold values from -0.09375 to 0.09375
- w_forget: bfloat16 [4096, 2048], P('kv', 'tp'), may hold values from -0.09375 to 0.09375
- w_input: bfloat16 [4096, 2048], P('kv', 'tp'), may hold values from -0.09375 to 0.09375
- w_gate: bfloat16 [4096, 2048], P('kv', 'tp'), may hold values from -0.09375 to 0.09375
- w_out: bfloat16 [2048, 4096], P('tp', 'kv'), may hold values from -0.125 to 0.125
- gain: float32 [4096], replicated, may hold values from 0.1 to 1.9
- head_gain: float32 [2048], replicated, may hold values from 0.1 to 1.9
- lower_bound: float32 [2048], replicated, may hold values from 0.05 to 0.9
- state: float32 [64, 16, 128, 128], P(('grp', 'dp', 'kv'), 'tp'), parts along dimension 0, may hold values from -2.4 to 2.4
- last_forget: float32 [64, 4, 2048], P(('grp', 'dp', 'kv'), None, 'tp'), parts along dimension 0, may hold values from 0.3 to 0.99
- last_values: bfloat16 [64, 4, 2048], P(('grp', 'dp', 'kv'), None, 'tp'), parts along dimension 0, may hold values from -6 to 6
- accepted: int32 [64], P(('grp', 'dp', 'kv')), parts along dimension 0, may hold values from 0 to 4
Outputs:
- mixed_out: bfloat16 [64, 4, 4096], P(('grp', 'dp'), None, ('kv', 'tp')), parts along dimension 0
- taken: float32 [64, 16, 128, 128], P(('grp', 'dp', 'kv'), 'tp'), parts along dimension 0
The draws below stay inside these ranges and needn't reach their ends.
There are 2 independent parts, one for each index of `grp`. The reference program is written for one: setup_inputs(seed, part) draws one part's arguments, and reference() takes and returns one part's arrays. A program takes and returns all parts, laid end to end along the dimension named above; an argument that names none is the same for every part. Nothing has to cross between parts.
All inputs are finite; a program needn't handle non-finite values.
Results may differ from the reference program's by a relative error of at most 0.0071.
Values may be sent and summed in bfloat16 or wider, within the bound.
A program may use at most 64 MiB of HBM per device.

```python
import jax
import jax.numpy as jnp
from jax import lax

D = 4096
HEADS = 16
HEAD = 128
PROPOSALS = 4
SEQS = 32
N_TP = 2


def touch_ends(drawn, rng, least, high):
    longest = drawn.shape.index(max(drawn.shape))
    spots = []
    for shift in (0, 1):
        where = [jax.random.randint(jax.random.fold_in(rng, axis), (), 0, length) for axis, length in enumerate(drawn.shape)]
        where[longest] = (where[longest] + shift) % drawn.shape[longest]
        spots.append(tuple(where))
    return drawn.at[spots[0]].set(least).at[spots[1]].set(high)


def shard_levels(stream_key, extent, pieces, smallest, high):
    level = 1.0
    for dim, blocks in pieces:
        steps = jax.random.uniform(jax.random.fold_in(jax.random.fold_in(stream_key, 6), dim), (blocks,), jnp.float32, smallest / len(pieces), high / len(pieces))
        level = level * jnp.repeat(jnp.exp(steps), extent[dim] // blocks).reshape((-1,) + (1,) * (len(extent) - 1 - dim))
    return level


def bell_draw(key, shape, spread, most, pieces=(), held_as=jnp.bfloat16):
    array = jax.random.normal(key, shape, jnp.float32) * spread
    if len(pieces) > 0:
        array = shard_levels(key, shape, pieces, -0.22, 0.18) * array
    return jnp.clip(array, min=-most, max=most).astype(held_as)


def setup_inputs(seed: int = 0, part: int = 0) -> dict:
    keys = jax.random.split(jax.random.key(seed), 14)
    part_keys = jax.random.split(jax.random.fold_in(keys[13], part), 14)
    return {
        "tokens": bell_draw(part_keys[0], (SEQS, PROPOSALS, D), 1.0, 6.0, ((0, 2), (2, 4))),
        "w_query": bell_draw(keys[1], (D, HEADS * HEAD), D ** -0.5, 0.09375, ((0, 4), (1, 2))),
        "w_forget": bell_draw(keys[2], (D, HEADS * HEAD), D ** -0.5, 0.09375, ((0, 4), (1, 2))),
        "w_input": bell_draw(keys[3], (D, HEADS * HEAD), D ** -0.5, 0.09375, ((0, 4), (1, 2))),
        "w_gate": bell_draw(keys[4], (D, HEADS * HEAD), D ** -0.5, 0.09375, ((0, 4), (1, 2))),
        "w_out": bell_draw(keys[5], (HEADS * HEAD, D), (HEADS * HEAD) ** -0.5, 0.125, ((0, 2), (1, 4))),
        "gain": jnp.clip(1.0 + 0.18 * jax.random.normal(keys[6], (D,), jnp.float32), 0.1, 1.9),
        "head_gain": jnp.clip(1.0 + 0.18 * jax.random.normal(keys[7], (HEADS * HEAD,), jnp.float32), 0.1, 1.9),
        "lower_bound": jnp.clip(jax.random.uniform(keys[8], (HEADS * HEAD,), jnp.float32, 0.05, 0.9), 0.05, 0.9),
        "state": bell_draw(part_keys[9], (SEQS, HEADS, HEAD, HEAD), 0.3, 2.4, ((0, 8), (1, 2)), jnp.float32),
        "last_forget": jnp.clip(0.3 + 0.69 * jax.random.uniform(part_keys[10], (SEQS, PROPOSALS, HEADS * HEAD), jnp.float32) ** shard_levels(part_keys[10], (SEQS, PROPOSALS, HEADS * HEAD), ((0, 8), (2, 2)), -0.2, 0.2), 0.3, 0.99),
        "last_values": bell_draw(part_keys[11], (SEQS, PROPOSALS, HEADS * HEAD), 1.0, 6.0, ((0, 8), (2, 2))),
        "accepted": touch_ends(jax.random.randint(part_keys[12], (SEQS,), 0, PROPOSALS + 1), jax.random.fold_in(part_keys[12], 1), 0, PROPOSALS).astype(jnp.int32),
    }


EPSILON = 1e-05

def reference(tokens, w_query, w_forget, w_input, w_gate, w_out, gain, head_gain, lower_bound, state, last_forget, last_values, accepted):
    seqs, props, width = tokens.shape
    heads = w_query.shape[1] // HEAD
    tokens_f32 = tokens.astype(jnp.float32)
    row_scale = lax.rsqrt(lax.optimization_barrier(jnp.mean(tokens_f32 * tokens_f32, -1)) + EPSILON).reshape(-1, 1)
    scaled = (tokens_f32 * gain).astype(jnp.bfloat16).reshape(-1, width)

    def project(weight):
        product = jnp.dot(scaled, weight, preferred_element_type=jnp.float32) * row_scale
        return product.reshape(seqs, props, heads, HEAD)
    floor_gate = lower_bound.reshape(heads, HEAD)
    forget = floor_gate + (1.0 - floor_gate) * jax.nn.sigmoid(project(w_forget))
    queries = jax.nn.silu(project(w_query)) * HEAD ** (-0.5)
    values_new = project(w_input)
    gate_path = jax.nn.silu(project(w_gate))
    old_forget = last_forget.reshape(seqs, props, heads, HEAD)
    old_values = last_values.astype(jnp.float32).reshape(seqs, props, heads, HEAD)
    taken = state
    for position in range(PROPOSALS):
        advanced = old_forget[:, position, :, :, None] * taken + (1.0 - old_forget[:, position])[..., None] * old_values[:, position, :, None, :]
        taken = jnp.where((position < accepted)[:, None, None, None], advanced, taken)
    carried = taken
    outputs = []
    for position in range(PROPOSALS):
        carried = forget[:, position, :, :, None] * carried + (1.0 - forget[:, position])[..., None] * values_new[:, position, :, None, :]
        outputs.append(jnp.einsum('shk,shkv->shv', queries[:, position], carried, precision=lax.Precision.HIGHEST))
    recurrent = jnp.stack(outputs, 1)
    normed = recurrent * lax.rsqrt(lax.optimization_barrier(jnp.mean(recurrent * recurrent, -1, keepdims=True)) + EPSILON)
    heads_out = (normed * head_gain.reshape(heads, HEAD) * gate_path).astype(jnp.bfloat16).reshape(seqs * props, heads * HEAD)
    head_cols = heads * HEAD // N_TP
    summed = jnp.zeros((seqs * props, width), jnp.float32)
    for group in range(N_TP):
        part = jnp.dot(heads_out[:, group * head_cols:(group + 1) * head_cols], w_out[group * head_cols:(group + 1) * head_cols], preferred_element_type=jnp.float32)
        summed = summed + lax.optimization_barrier(part.astype(jnp.bfloat16)).astype(jnp.float32)
    return (summed.astype(jnp.bfloat16).reshape(seqs, props, width), taken)
```

```python
import functools

import jax
import jax.numpy as jnp
from jax import lax
from jax.experimental import pallas as pl
from jax.experimental.pallas import tpu as pltpu
from jax.sharding import PartitionSpec as P

HEAD = 128
EPSILON = 1e-05
CHUNK_HEADS = 4
LINE = 4
LINE_HEADS = 2
VMEM_MIB = 56
F32 = jnp.float32
BF16 = jnp.bfloat16

MESSAGES = {
    "0 for 3": (0, 1, 3, 2),
    "0 for 2": (0, 1, 2, 3),
    "0 to 1": (0, 1, 1, 0),
    "1 to 0": (1, 0, 0, 0),
    "1 to 3": (1, 3, 3, 0),
    "1 to 2": (1, 2, 2, 0),
    "2 to 3": (2, 3, 3, 1),
    "2 to 0": (2, 0, 0, 1),
    "2 to 1": (2, 1, 1, 1),
    "3 for 0": (3, 2, 0, 2),
    "3 to 1": (3, 1, 1, 4),
    "3 to 2": (3, 2, 2, 1),
}
ORDER = {name: i % 3 for i, name in enumerate(MESSAGES)}
FIRST = {0: ("0 for 3",), 1: ("1 to 0",), 2: ("2 to 1", "2 to 3"), 3: ("3 for 0",)}
THEN = {0: ("0 for 2", "0 to 1"), 3: ("3 to 1", "3 to 2")}
ONWARD = {
    1: (("0 for 3", "1 to 3"), ("0 for 2", "1 to 2")),
    2: (("3 for 0", "2 to 0"), None),
}
PEERS = ((3, 2, 1), (3, 2, 0), (0, 1, 3), (0, 1, 2))


def kernel_any(
    kv,
    tp,
    tokens,
    w_query,
    w_forget,
    w_input,
    w_gate,
    w_out,
    gain,
    head_gain,
    lower_bound,
    state,
    last_forget,
    last_values,
    accepted,
    tk_v,
    own_v,
    peer_v,
    tok_v,
    gain_v,
    hg_v,
    lb_v,
    lf_v,
    lv_v,
    rows_v,
    scaled_v,
    w_v,
    wo_v,
    st_v,
    tkb_v,
    lfr_v,
    lvr_v,
    ssq_v,
    ssq_r,
    prod_v,
    send_v,
    recv_v,
    gath_v,
    acc_v,
    part_v,
    relay_v,
    load_sem,
    w_sem,
    wo_sem,
    st_sem,
    ssq_ssem,
    ssq_rsem,
    rs_ssem,
    rs_rsem,
    relay_ssem,
    relay_rsem,
    ag_ssem,
    ag_rsem,
    tp_ssem,
    tp_rsem,
):
    me = lax.axis_index("kv")
    tme = lax.axis_index("tp")
    seqs, props, feat = tokens.shape
    own_seqs, heads_dev = state.shape[0], state.shape[1]
    own_rows = own_seqs * props
    rows = seqs * props
    width = gain.shape[1]
    head_cols = heads_dev * HEAD
    chunks = heads_dev // CHUNK_HEADS
    cw = CHUNK_HEADS * HEAD
    half = w_out.shape[1] // tp
    weights = (w_query, w_forget, w_input, w_gate)

    def local(src, dst, sem):
        copy = pltpu.make_async_copy(src, dst, sem)
        copy.start()
        return copy

    tok_c = local(tokens, tok_v, load_sem.at[0])
    gain_c = local(gain, gain_v, load_sem.at[1])

    def load_w(c):
        return [
            local(w.at[:, pl.ds(c * cw, cw)], w_v.at[c, :, pl.ds(i * cw, cw)], w_sem.at[c, i])
            for i, w in enumerate(weights)
        ]

    def load_state(c):
        hs = pl.ds(c * CHUNK_HEADS, CHUNK_HEADS)
        return local(state.at[:, hs], st_v.at[:, hs], st_sem.at[c])

    w_c = [load_w(0)]
    small_c = [
        local(last_forget, lf_v, load_sem.at[2]),
        local(last_values, lv_v, load_sem.at[3]),
        local(head_gain, hg_v, load_sem.at[4]),
        local(lower_bound, lb_v, load_sem.at[5]),
    ]
    st_c = []
    for c in range(chunks):
        st_c.append(load_state(c))
        if c + 1 < chunks:
            w_c.append(load_w(c + 1))
    wo_c = []
    for o in range(tp):
        column = pl.multiple_of(lax.rem(tme + o, tp) * half, half)
        wo_c.append(local(w_out.at[:, pl.ds(column, half)], wo_v.at[o], wo_sem.at[o]))

    barrier = pltpu.get_barrier_semaphore()
    kv_peers = [lax.rem(me + o, kv) for o in range(1, kv)]
    tp_peers = [lax.rem(tme + o, tp) for o in range(1, tp)]
    for peer in kv_peers:
        pl.semaphore_signal(barrier, inc=1, device_id={"kv": peer}, device_id_type=pl.DeviceIdType.MESH)
    for peer in tp_peers:
        pl.semaphore_signal(barrier, inc=1, device_id={"tp": peer}, device_id_type=pl.DeviceIdType.MESH)

    def remote(src, dst, ssem, rsem, axis, peer):
        copy = pltpu.make_async_remote_copy(
            src_ref=src,
            dst_ref=dst,
            send_sem=ssem,
            recv_sem=rsem,
            device_id={axis: peer},
            device_id_type=pl.DeviceIdType.MESH,
        )
        copy.start()
        return copy

    tok_c.wait()
    gain_c.wait()
    for s in range(seqs):
        rows_v[pl.ds(s * props, props), :] = tok_v[s].astype(F32)
    x = rows_v[...]
    my_gain = gain_v[:, pl.ds(pl.multiple_of(me * feat, feat), feat)]
    scaled_v[...] = (x * my_gain).astype(BF16)
    ssq_v[...] = jnp.broadcast_to(jnp.sum(x * x, axis=1, keepdims=True), (rows, HEAD))

    pl.semaphore_wait(barrier, kv - 1 + tp - 1)

    def rows_of(device):
        return pl.ds(pl.multiple_of(device * own_rows, own_rows), own_rows)

    ssq_c = [
        remote(
            ssq_v.at[rows_of(peer)], ssq_r.at[o], ssq_ssem.at[o], ssq_rsem.at[o], "kv", peer
        )
        for o, peer in enumerate(kv_peers)
    ]

    place = lax.broadcasted_iota(jnp.int32, (own_rows, 1), 0)
    prop = lax.rem(place, props)
    seq = place // props

    def old_terms():
        for copy in small_c:
            copy.wait()
        for s in range(own_seqs):
            lfr_v[pl.ds(s * props, props), :] = lf_v[s]
            lvr_v[pl.ds(s * props, props), :] = lv_v[s].astype(F32)
        limit = jnp.zeros((own_rows, 1), jnp.int32)
        for s in range(own_seqs):
            limit = jnp.where(seq == s, accepted[s], limit)
        mask = prop < limit
        old = lfr_v[...]
        decay = jnp.where(mask, old, 1.0)
        weight = jnp.where(mask, 1.0 - old, 0.0)
        after = jnp.ones_like(decay)
        for lag in range(1, props):
            after = after * jnp.where(
                prop < props - lag, pltpu.roll(decay, own_rows - lag, 0), 1.0
            )
        return decay * after, weight * after, lvr_v[...].astype(BF16)

    def take(c, ends, old_weight, old_values):
        st_c[c].wait()
        lane_seq = lax.broadcasted_iota(jnp.int32, (1, own_rows), 1) // props
        for h in range(c * CHUNK_HEADS, (c + 1) * CHUNK_HEADS):
            cols = slice(h * HEAD, (h + 1) * HEAD)
            end_t = ends[:, cols].T
            weight_t = old_weight[:, cols].T
            for s in range(own_seqs):
                mine = jnp.where(lane_seq == s, weight_t, 0.0).astype(BF16)
                added = jnp.dot(mine, old_values[:, cols], preferred_element_type=F32)
                new = end_t[:, s * props : s * props + 1] * st_v[s, h] + added
                tk_v[s, h] = new
                tkb_v[h, pl.ds(s * HEAD, HEAD), :] = new.astype(BF16)

    relayed = kv == 4
    at_end = jnp.logical_or(me == 0, me == kv - 1)
    first = me == 0
    last = me == kv - 1
    if relayed:

        @pl.when(last)
        def _():
            recv_v[:, kv - 2] = jnp.zeros_like(recv_v[:, kv - 2])

        @pl.when(first)
        def _():
            recv_v[:, 0] = jnp.zeros_like(recv_v[:, 0])

    def rs_copy(c, o):
        return pltpu.make_async_remote_copy(
            src_ref=send_v.at[c, rows_of(kv_peers[o])],
            dst_ref=recv_v.at[c, o],
            send_sem=rs_ssem.at[c, o],
            recv_sem=rs_rsem.at[c, o],
            device_id={"kv": kv_peers[o]},
            device_id_type=pl.DeviceIdType.MESH,
        )

    def relay_copy(c, end):
        far, near = (kv - 1, 1) if end == 0 else (0, kv - 2)
        return pltpu.make_async_remote_copy(
            src_ref=send_v.at[c, rows_of(far)],
            dst_ref=relay_v.at[c],
            send_sem=relay_ssem.at[c],
            recv_sem=relay_rsem.at[c],
            device_id={"kv": near},
            device_id_type=pl.DeviceIdType.MESH,
        )

    def send_blocks(c):
        if not relayed:
            for o in range(kv - 1):
                rs_copy(c, o).start()
            return

        @pl.when(first)
        def _():
            relay_copy(c, 0).start()
            rs_copy(c, 1).start()
            if c > 0:
                rs_copy(c - 1, 0).start()
            if c == chunks - 1:
                rs_copy(c, 0).start()

        @pl.when(last)
        def _():
            relay_copy(c, kv - 1).start()
            rs_copy(c, 1).start()
            if c > 0:
                rs_copy(c - 1, 2).start()
            if c == chunks - 1:
                rs_copy(c, 2).start()

        @pl.when(jnp.logical_not(at_end))
        def _():
            rs_copy(c, 0).start()
            rs_copy(c, 2).start()

    def send_on(c):
        if relayed:

            @pl.when(jnp.logical_not(at_end))
            def _():
                relay_copy(c, 0).wait_recv()
                far = rows_of(kv_peers[1])
                send_v[c, far, :] = (prod_v[c, far, :] + relay_v[c].astype(F32)).astype(BF16)
                rs_copy(c, 1).start()

    def wait_blocks(c):
        for o in range(kv - 1):
            if relayed and o == 0:
                pl.when(jnp.logical_not(first))(lambda o=o: rs_copy(c, o).wait_recv())
            elif relayed and o == kv - 2:
                pl.when(jnp.logical_not(last))(lambda o=o: rs_copy(c, o).wait_recv())
            else:
                rs_copy(c, o).wait_recv()

    def wait_sent(c):
        if not relayed:
            for o in range(kv - 1):
                rs_copy(c, o).wait_send()
            return
        rs_copy(c, 1).wait_send()

        @pl.when(first)
        def _():
            relay_copy(c, 0).wait_send()
            rs_copy(c, 0).wait_send()

        @pl.when(last)
        def _():
            relay_copy(c, kv - 1).wait_send()
            rs_copy(c, 2).wait_send()

        @pl.when(jnp.logical_not(at_end))
        def _():
            rs_copy(c, 0).wait_send()
            rs_copy(c, 2).wait_send()

    terms = None
    for c in range(chunks):
        for copy in w_c[c]:
            copy.wait()
        product = jnp.dot(scaled_v[...], w_v[c], preferred_element_type=F32)
        prod_v[c] = product
        send_v[c] = product.astype(BF16)
        send_blocks(c)
        if terms is None:
            terms = old_terms()
        if c > 0:
            send_on(c - 1)
        take(c, *terms)
    send_on(chunks - 1)

    squares = ssq_v[rows_of(me), :]
    for o in range(kv - 1):
        ssq_c[o].wait_recv()
        squares = squares + ssq_r[o]
    row_scale = lax.rsqrt(squares[:, :1] / width + EPSILON)
    mine_rows = rows_of(me)
    ag_c = []

    def recur(c):
        wait_blocks(c)

        def projected(i):
            total = prod_v[c, mine_rows, pl.ds(i * cw, cw)]
            for o in range(kv - 1):
                total = total + recv_v[c, o, :, pl.ds(i * cw, cw)].astype(F32)
            return total * row_scale

        column = pl.multiple_of(tme * head_cols + c * cw, cw)
        floor_gate = lb_v[:, pl.ds(column, cw)]
        forget = floor_gate + (1.0 - floor_gate) * jax.nn.sigmoid(projected(1))
        keys = 1.0 - forget
        queries = jax.nn.silu(projected(0)) * HEAD ** (-0.5)
        values = projected(2)
        gate = jax.nn.silu(projected(3)) * hg_v[:, pl.ds(column, cw)]
        start = forget
        for lag in range(1, props):
            start = start * jnp.where(prop >= lag, pltpu.roll(forget, lag, 0), 1.0)
        reading = queries * start
        results = []
        for h in range(CHUNK_HEADS):
            cols = slice(h * HEAD, (h + 1) * HEAD)
            lhs = jnp.concatenate(
                [jnp.where(seq == s, reading[:, cols], 0.0) for s in range(own_seqs)], axis=1
            ).astype(BF16)
            results.append(
                jnp.dot(lhs, tkb_v[c * CHUNK_HEADS + h], preferred_element_type=F32)
            )
        decay = queries
        for lag in range(props):
            if lag > 0:
                decay = decay * (forget if lag == 1 else pltpu.roll(forget, lag - 1, 0))
            pair = decay * (keys if lag == 0 else pltpu.roll(keys, lag, 0))
            pair = jnp.where(prop >= lag, pair, 0.0)
            moved = values if lag == 0 else pltpu.roll(values, lag, 0)
            for h in range(CHUNK_HEADS):
                cols = slice(h * HEAD, (h + 1) * HEAD)
                score = jnp.sum(pair[:, cols], axis=1, keepdims=True)
                results[h] = results[h] + score * moved[:, cols]
        outs = []
        for h in range(CHUNK_HEADS):
            cols = slice(h * HEAD, (h + 1) * HEAD)
            r = results[h]
            normed = r * lax.rsqrt(jnp.mean(r * r, axis=1, keepdims=True) + EPSILON)
            outs.append((normed * gate[:, cols]).astype(BF16))
        gath_v[c, mine_rows, :] = jnp.concatenate(outs, axis=1)
        ag_c.append(
            [
                remote(
                    gath_v.at[c, mine_rows],
                    gath_v.at[c, mine_rows],
                    ag_ssem.at[c, o],
                    ag_rsem.at[c, o],
                    "kv",
                    peer,
                )
                for o, peer in enumerate(kv_peers)
            ]
        )

    def product_of(c, o):
        term = jnp.dot(
            gath_v[c], wo_v[o, pl.ds(c * cw, cw), :], preferred_element_type=F32
        )
        return term if c == 0 else acc_v[o] + term

    def gathered(c):
        for o in range(kv - 1):
            ag_c[c][o].wait_recv()

    for c in range(chunks):
        recur(c)
    for copy in wo_c:
        copy.wait()
    for c in range(chunks - 1):
        gathered(c)
        for o in range(tp):
            acc_v[o] = product_of(c, o)
    gathered(chunks - 1)
    tp_c = []
    for o in range(1, tp):
        part_v[o - 1] = product_of(chunks - 1, o).astype(BF16)
        tp_c.append(
            remote(
                part_v.at[o - 1],
                peer_v.at[o - 1],
                tp_ssem.at[o - 1],
                tp_rsem.at[o - 1],
                "tp",
                tp_peers[o - 1],
            )
        )
    own_v[...] = product_of(chunks - 1, 0).astype(BF16)
    for copy in tp_c:
        copy.wait_recv()
    for c in range(chunks):
        wait_sent(c)
    for copies in [ssq_c, *ag_c, tp_c]:
        for copy in copies:
            copy.wait_send()


def kernel_line(
    tp,
    tokens,
    w_query,
    w_forget,
    w_input,
    w_gate,
    w_out,
    gain,
    head_gain,
    lower_bound,
    state,
    last_forget,
    last_values,
    accepted,
    tk_v,
    own_v,
    peer_v,
    tok_v,
    gain_v,
    hg_v,
    lb_v,
    lf_v,
    lv_v,
    rows_v,
    scaled_v,
    w_v,
    wo_v,
    st_v,
    tkb_v,
    lfr_v,
    lvr_v,
    ssq_v,
    ssq_s,
    ssq_r,
    prod_v,
    send_v,
    recv_v,
    gath_v,
    acc_v,
    part_v,
    acc_s,
    load_sem,
    w_sem,
    wo_sem,
    st_sem,
    ssq_ssem,
    ssq_rsem,
    rs_ssem,
    rs_rsem,
    ag_ssem,
    ag_rsem,
    tp_ssem,
    tp_rsem,
    go_sem,
):
    kv = LINE
    me = lax.axis_index("kv")
    tme = lax.axis_index("tp")
    seqs, props, feat = tokens.shape
    own_seqs, heads_dev = state.shape[0], state.shape[1]
    own_rows = own_seqs * props
    rows = seqs * props
    width = gain.shape[1]
    head_cols = heads_dev * HEAD
    chunks = heads_dev // LINE_HEADS
    cw = LINE_HEADS * HEAD
    half = w_out.shape[1] // tp
    weights = (w_query, w_forget, w_input, w_gate)

    at_end = jnp.logical_or(me == 0, me == kv - 1)

    def local(src, dst, sem):
        copy = pltpu.make_async_copy(src, dst, sem)
        copy.start()
        return copy

    tok_c = local(tokens, tok_v, load_sem.at[0])
    gain_c = local(gain, gain_v, load_sem.at[1])

    def load_w(c):
        return [
            local(w.at[:, pl.ds(c * cw, cw)], w_v.at[c, :, pl.ds(i * cw, cw)], w_sem.at[c, i])
            for i, w in enumerate(weights)
        ]

    def load_late():
        small = [
            local(last_forget, lf_v, load_sem.at[2]),
            local(last_values, lv_v, load_sem.at[3]),
            local(head_gain, hg_v, load_sem.at[4]),
            local(lower_bound, lb_v, load_sem.at[5]),
            local(accepted, acc_s, load_sem.at[6]),
        ]
        states = []
        for c in range(chunks):
            hs = pl.ds(c * LINE_HEADS, LINE_HEADS)
            states.append(local(state.at[:, hs], st_v.at[:, hs], st_sem.at[c]))
        return small, states

    def load_out(o):
        column = pl.multiple_of(lax.rem(tme + o, tp) * half, half)
        return local(w_out.at[:, pl.ds(column, half)], wo_v.at[o], wo_sem.at[o])

    w_c = [load_w(0)]

    def signal(axis, peer):
        pl.semaphore_signal(
            barrier, inc=1, device_id={axis: peer}, device_id_type=pl.DeviceIdType.MESH
        )

    barrier = pltpu.get_barrier_semaphore()
    tp_peers = [lax.rem(tme + o, tp) for o in range(1, tp)]
    for peer in tp_peers:
        signal("tp", peer)

    @pl.when(me > 0)
    def _():
        signal("kv", me - 1)

    @pl.when(me < kv - 1)
    def _():
        signal("kv", me + 1)

    def remote(src, dst, ssem, rsem, axis, peer):
        return pltpu.make_async_remote_copy(
            src_ref=src,
            dst_ref=dst,
            send_sem=ssem,
            recv_sem=rsem,
            device_id={axis: peer},
            device_id_type=pl.DeviceIdType.MESH,
        )

    tok_c.wait()
    gain_c.wait()
    w_c.append(load_w(1))
    for s in range(seqs):
        rows_v[pl.ds(s * props, props), :] = tok_v[s].astype(F32)
    x = rows_v[...]
    my_gain = gain_v[:, pl.ds(pl.multiple_of(me * feat, feat), feat)]
    scaled_v[...] = (x * my_gain).astype(BF16)
    squared = jnp.sum(x * x, axis=1, keepdims=True)
    on_row = lax.broadcasted_iota(jnp.int32, (rows, HEAD), 0)
    on_lane = lax.broadcasted_iota(jnp.int32, (rows, HEAD), 1)
    along = jnp.sum(jnp.where(on_row == on_lane, squared, 0.0), axis=0, keepdims=True)
    ssq_v[...] = jnp.broadcast_to(along, ssq_v.shape)

    def rows_of(device):
        return pl.ds(pl.multiple_of(device * own_rows, own_rows), own_rows)

    def message(c, name):
        _, to, dest, slot = MESSAGES[name]
        return remote(
            send_v.at[c, rows_of(dest)],
            recv_v.at[c, slot],
            rs_ssem.at[c, ORDER[name]],
            rs_rsem.at[c, slot],
            "kv",
            to,
        )

    def pass_on(c, name, onward):
        _, _, dest, slot = MESSAGES[name]
        message(c, name).wait_recv()
        into = rows_of(dest)
        send_v[c, into, :] = (prod_v[c, into, :] + recv_v[c, slot].astype(F32)).astype(BF16)
        message(c, onward).start()

    def ssq_copy(i, slot, to):
        return remote(ssq_s.at[i], ssq_r.at[slot], ssq_ssem.at[i], ssq_rsem.at[slot], "kv", to)

    ssq_s[0] = ssq_v[...]
    partner = me + 1 - 2 * lax.rem(me, 2)
    across = jnp.where(me == 1, 2, 1)
    beyond = jnp.where(me == 1, 3, 0)
    inside = jnp.logical_not(at_end)
    pl.semaphore_wait(barrier, jnp.where(at_end, tp, tp + 1))
    ssq_copy(0, 0, partner).start()

    @pl.when(inside)
    def _():
        pl.semaphore_signal(
            go_sem, inc=1, device_id={"kv": across}, device_id_type=pl.DeviceIdType.MESH
        )

    @pl.when(me == 2)
    def _():
        pl.semaphore_signal(
            go_sem, inc=1, device_id={"kv": 3}, device_id_type=pl.DeviceIdType.MESH
        )

    @pl.when(me != 1)
    def _():
        recv_v[:, 4] = jnp.zeros_like(recv_v[:, 4])

    place = lax.broadcasted_iota(jnp.int32, (own_rows, 1), 0)
    prop = lax.rem(place, props)
    seq = place // props

    def old_terms():
        for copy in small_c:
            copy.wait()
        for s in range(own_seqs):
            lfr_v[pl.ds(s * props, props), :] = lf_v[s]
            lvr_v[pl.ds(s * props, props), :] = lv_v[s].astype(F32)
        limit = jnp.zeros((own_rows, 1), jnp.int32)
        for s in range(own_seqs):
            limit = jnp.where(seq == s, acc_s[s], limit)
        mask = prop < limit
        old = lfr_v[...]
        decay = jnp.where(mask, old, 1.0)
        weight = jnp.where(mask, 1.0 - old, 0.0)
        after = jnp.ones_like(decay)
        for lag in range(1, props):
            after = after * jnp.where(
                prop < props - lag, pltpu.roll(decay, own_rows - lag, 0), 1.0
            )
        return decay * after, weight * after, lvr_v[...].astype(BF16)

    def take(c, ends, old_weight, old_values):
        st_c[c].wait()
        lane_seq = lax.broadcasted_iota(jnp.int32, (1, own_rows), 1) // props
        for h in range(c * LINE_HEADS, (c + 1) * LINE_HEADS):
            cols = slice(h * HEAD, (h + 1) * HEAD)
            end_t = ends[:, cols].T
            weight_t = old_weight[:, cols].T
            for s in range(own_seqs):
                mine = jnp.where(lane_seq == s, weight_t, 0.0).astype(BF16)
                added = jnp.dot(mine, old_values[:, cols], preferred_element_type=F32)
                new = end_t[:, s * props : s * props + 1] * st_v[s, h] + added
                tk_v[s, h] = new
                tkb_v[h, pl.ds(s * HEAD, HEAD), :] = new.astype(BF16)

    for c in range(chunks):
        for copy in w_c[c]:
            copy.wait()
        if c + 2 < chunks:
            w_c.append(load_w(c + 2))
        elif c + 2 == chunks:
            small_c, st_c = load_late()
        else:
            wo_c = [load_out(o) for o in range(tp)]
        product = jnp.dot(scaled_v[...], w_v[c], preferred_element_type=F32)
        prod_v[c] = product
        send_v[c] = product.astype(BF16)

        for device, names in FIRST.items():

            @pl.when(me == device)
            def _():
                for name in names:
                    message(c, name).start()

    for device, names in THEN.items():

        @pl.when(me == device)
        def _():
            if device == 3:
                pl.semaphore_wait(go_sem, 1)
            for name in names:
                for c in range(chunks):
                    message(c, name).start()

    terms = old_terms()
    ssq_copy(0, 0, partner).wait_recv()

    @pl.when(inside)
    def _():
        pl.semaphore_wait(go_sem, 1)
        ssq_s[1] = ssq_v[...] + ssq_r[0]
        ssq_copy(1, 1, across).start()
        ssq_s[2] = ssq_v[...] + ssq_r[0]
        ssq_copy(2, 1, beyond).start()

    for c in range(chunks):
        for device, steps in ONWARD.items():

            @pl.when(me == device)
            def _():
                pass_on(c, *steps[0])

        take(c, *terms)

    @pl.when(me == 1)
    def _():
        for c in range(chunks):
            pass_on(c, *ONWARD[1][1])

    ssq_copy(1, 1, partner).wait_recv()
    whole = ssq_v[...] + ssq_r[0] + ssq_r[1]
    mine_rows = rows_of(me)
    picked = lax.broadcasted_iota(jnp.int32, (own_rows, HEAD), 1) == (
        lax.broadcasted_iota(jnp.int32, (own_rows, HEAD), 0) + me * own_rows
    )
    squares = jnp.sum(jnp.where(picked, whole[:1], 0.0), axis=1, keepdims=True)
    row_scale = lax.rsqrt(squares / width + EPSILON)
    peers = [
        functools.reduce(lambda found, d: jnp.where(me == d, PEERS[d][o], found), range(kv), 0)
        for o in range(kv - 1)
    ]

    def head_copy(c, o):
        return remote(
            gath_v.at[c, mine_rows],
            gath_v.at[c, mine_rows],
            ag_ssem.at[c, o],
            ag_rsem.at[c, me],
            "kv",
            peers[o],
        )

    def recur(c):
        for slot in range(2):
            remote(
                send_v.at[c, mine_rows], recv_v.at[c, slot], rs_ssem.at[c, 0],
                rs_rsem.at[c, slot], "kv", peers[0],
            ).wait_recv()

        @pl.when(me == 1)
        def _():
            message(c, "3 to 1").wait_recv()

        def projected(i):
            cols = pl.ds(i * cw, cw)
            total = prod_v[c, mine_rows, cols]
            for slot in (0, 1, 4):
                total = total + recv_v[c, slot, :, cols].astype(F32)
            return total * row_scale

        column = pl.multiple_of(tme * head_cols + c * cw, cw)
        floor_gate = lb_v[:, pl.ds(column, cw)]
        forget = floor_gate + (1.0 - floor_gate) * jax.nn.sigmoid(projected(1))
        keys = 1.0 - forget
        queries = jax.nn.silu(projected(0)) * HEAD ** (-0.5)
        values = projected(2)
        gate = jax.nn.silu(projected(3)) * hg_v[:, pl.ds(column, cw)]
        start = forget
        for lag in range(1, props):
            start = start * jnp.where(prop >= lag, pltpu.roll(forget, lag, 0), 1.0)
        reading = queries * start
        results = []
        for h in range(LINE_HEADS):
            cols = slice(h * HEAD, (h + 1) * HEAD)
            lhs = jnp.concatenate(
                [jnp.where(seq == s, reading[:, cols], 0.0) for s in range(own_seqs)], axis=1
            ).astype(BF16)
            results.append(
                jnp.dot(lhs, tkb_v[c * LINE_HEADS + h], preferred_element_type=F32)
            )
        decay = queries
        for lag in range(props):
            if lag > 0:
                decay = decay * (forget if lag == 1 else pltpu.roll(forget, lag - 1, 0))
            pair = decay * (keys if lag == 0 else pltpu.roll(keys, lag, 0))
            pair = jnp.where(prop >= lag, pair, 0.0)
            moved = values if lag == 0 else pltpu.roll(values, lag, 0)
            for h in range(LINE_HEADS):
                cols = slice(h * HEAD, (h + 1) * HEAD)
                score = jnp.sum(pair[:, cols], axis=1, keepdims=True)
                results[h] = results[h] + score * moved[:, cols]
        outs = []
        for h in range(LINE_HEADS):
            cols = slice(h * HEAD, (h + 1) * HEAD)
            r = results[h]
            normed = r * lax.rsqrt(jnp.mean(r * r, axis=1, keepdims=True) + EPSILON)
            outs.append((normed * gate[:, cols]).astype(BF16))
        gath_v[c, mine_rows, :] = jnp.concatenate(outs, axis=1)
        for o in range(kv - 1):
            head_copy(c, o).start()

    def product_of(c, o):
        term = jnp.dot(
            gath_v[c], wo_v[o, pl.ds(c * cw, cw), :], preferred_element_type=F32
        )
        return term if c == 0 else acc_v[o] + term

    def gathered(c):
        for peer in peers:
            theirs = gath_v.at[c, rows_of(peer)]
            remote(
                theirs, theirs, ag_ssem.at[c, 0], ag_rsem.at[c, peer], "kv", peer
            ).wait_recv()

    for c in range(chunks):
        recur(c)
    for copy in wo_c:
        copy.wait()
    for c in range(chunks - 1):
        gathered(c)
        for o in range(tp):
            acc_v[o] = product_of(c, o)
    gathered(chunks - 1)
    tp_c = []
    for o in range(1, tp):
        part_v[o - 1] = product_of(chunks - 1, o).astype(BF16)
        copy = remote(
            part_v.at[o - 1],
            peer_v.at[o - 1],
            tp_ssem.at[o - 1],
            tp_rsem.at[o - 1],
            "tp",
            tp_peers[o - 1],
        )
        copy.start()
        tp_c.append(copy)
    own_v[...] = product_of(chunks - 1, 0).astype(BF16)
    for copy in tp_c:
        copy.wait_recv()

    for device in range(kv):

        @pl.when(me == device)
        def _():
            for name, (sender, _, _, _) in MESSAGES.items():
                if sender == device:
                    for c in range(chunks):
                        message(c, name).wait_send()

    ssq_copy(0, 0, partner).wait_send()

    @pl.when(inside)
    def _():
        ssq_copy(1, 1, across).wait_send()
        ssq_copy(2, 1, beyond).wait_send()

    for c in range(chunks):
        for o in range(kv - 1):
            head_copy(c, o).wait_send()
    for copy in tp_c:
        copy.wait_send()


def finish(tk_v, own_v, peer_v, mixed, taken, mix_v, sem):
    tk_c = pltpu.make_async_copy(tk_v, taken, sem.at[0])
    tk_c.start()
    seqs, props, _ = mixed.shape
    total = own_v[...].astype(F32)
    for o in range(peer_v.shape[0]):
        total = total + peer_v[o].astype(F32)
    for s in range(seqs):
        mix_v[s] = total[s * props : (s + 1) * props].astype(BF16)
    mix_c = pltpu.make_async_copy(mix_v, mixed, sem.at[1])
    mix_c.start()
    mix_c.wait()
    tk_c.wait()


def per_device(
    kv,
    tp,
    tokens,
    w_query,
    w_forget,
    w_input,
    w_gate,
    w_out,
    gain,
    head_gain,
    lower_bound,
    state,
    last_forget,
    last_values,
    accepted,
):
    seqs, props, feat = tokens.shape
    own_seqs, heads_dev = state.shape[0], state.shape[1]
    own_rows = own_seqs * props
    rows = seqs * props
    head_cols = heads_dev * HEAD
    on_line = kv == LINE and rows <= HEAD
    per_chunk = LINE_HEADS if on_line else CHUNK_HEADS
    chunks = heads_dev // per_chunk
    cw = per_chunk * HEAD
    half = w_out.shape[1] // tp
    peers = kv - 1
    dma = pltpu.SemaphoreType.DMA
    scratch = [
        pltpu.VMEM(tokens.shape, BF16),
        pltpu.VMEM((1, gain.shape[0]), F32),
        pltpu.VMEM((1, head_gain.shape[0]), F32),
        pltpu.VMEM((1, lower_bound.shape[0]), F32),
        pltpu.VMEM(last_forget.shape, F32),
        pltpu.VMEM(last_values.shape, BF16),
        pltpu.VMEM((rows, feat), F32),
        pltpu.VMEM((rows, feat), BF16),
        pltpu.VMEM((chunks, feat, 4 * cw), BF16),
        pltpu.VMEM((tp, head_cols, half), BF16),
        pltpu.VMEM(state.shape, F32),
        pltpu.VMEM((heads_dev, own_seqs * HEAD, HEAD), BF16),
        pltpu.VMEM((own_rows, head_cols), F32),
        pltpu.VMEM((own_rows, head_cols), F32),
    ]
    if on_line:
        body = functools.partial(kernel_line, tp)
        scratch += [
            pltpu.VMEM((1, HEAD), F32),
            pltpu.VMEM((3, 1, HEAD), F32),
            pltpu.VMEM((2, 1, HEAD), F32),
            pltpu.VMEM((chunks, rows, 4 * cw), F32),
            pltpu.VMEM((chunks, rows, 4 * cw), BF16),
            pltpu.VMEM((chunks, 5, own_rows, 4 * cw), BF16),
            pltpu.VMEM((chunks, rows, cw), BF16),
            pltpu.VMEM((tp, rows, half), F32),
            pltpu.VMEM((tp - 1, rows, half), BF16),
            pltpu.SMEM((own_seqs,), jnp.int32),
            dma((7,)),
            dma((chunks, 4)),
            dma((tp,)),
            dma((chunks,)),
            dma((3,)),
            dma((2,)),
            dma((chunks, 3)),
            dma((chunks, 5)),
            dma((chunks, peers)),
            dma((chunks, kv)),
            dma((tp - 1,)),
            dma((tp - 1,)),
            pltpu.SemaphoreType.REGULAR,
        ]
    else:
        body = functools.partial(kernel_any, kv, tp)
        scratch += [
            pltpu.VMEM((rows, HEAD), F32),
            pltpu.VMEM((peers, own_rows, HEAD), F32),
            pltpu.VMEM((chunks, rows, 4 * cw), F32),
            pltpu.VMEM((chunks, rows, 4 * cw), BF16),
            pltpu.VMEM((chunks, peers, own_rows, 4 * cw), BF16),
            pltpu.VMEM((chunks, rows, cw), BF16),
            pltpu.VMEM((tp, rows, half), F32),
            pltpu.VMEM((tp - 1, rows, half), BF16),
            pltpu.VMEM((chunks, own_rows, 4 * cw), BF16),
            dma((6,)),
            dma((chunks, 4)),
            dma((tp,)),
            dma((chunks,)),
            dma((peers,)),
            dma((peers,)),
            dma((chunks, peers)),
            dma((chunks, peers)),
            dma((chunks,)),
            dma((chunks,)),
            dma((chunks, peers)),
            dma((chunks, peers)),
            dma((tp - 1,)),
            dma((tp - 1,)),
        ]
    anywhere = pl.BlockSpec(memory_space=pl.ANY)
    held = pl.BlockSpec(memory_space=pltpu.VMEM)
    results = pl.pallas_call(
        body,
        out_shape=(
            pltpu.VMEM(state.shape, F32),
            pltpu.VMEM((rows, half), BF16),
            pltpu.VMEM((tp - 1, rows, half), BF16),
        ),
        in_specs=[pl.BlockSpec(memory_space=pltpu.HBM)] * 12
        + [pl.BlockSpec(memory_space=pltpu.HBM if on_line else pltpu.SMEM)],
        out_specs=(held, held, held),
        scratch_shapes=scratch,
        compiler_params=pltpu.CompilerParams(
            collective_id=0, has_side_effects=True, vmem_limit_bytes=VMEM_MIB * 1024 * 1024
        ),
    )(
        tokens,
        w_query,
        w_forget,
        w_input,
        w_gate,
        w_out,
        gain.reshape(1, -1),
        head_gain.reshape(1, -1),
        lower_bound.reshape(1, -1),
        state,
        last_forget,
        last_values,
        accepted,
    )
    return pl.pallas_call(
        finish,
        out_shape=(
            jax.ShapeDtypeStruct((seqs, props, half), BF16),
            jax.ShapeDtypeStruct(state.shape, F32),
        ),
        in_specs=[held] * 3,
        out_specs=(anywhere, anywhere),
        scratch_shapes=[pltpu.VMEM((seqs, props, half), BF16), dma((2,))],
        compiler_params=pltpu.CompilerParams(vmem_limit_bytes=4 * 1024 * 1024),
    )(*results)


def solution(mesh):
    in_specs = (
        P(("grp", "dp"), None, "kv"),
        P("kv", "tp"),
        P("kv", "tp"),
        P("kv", "tp"),
        P("kv", "tp"),
        P("tp", "kv"),
        P(),
        P(),
        P(),
        P(("grp", "dp", "kv"), "tp", None, None),
        P(("grp", "dp", "kv"), None, "tp"),
        P(("grp", "dp", "kv"), None, "tp"),
        P(("grp", "dp", "kv")),
    )
    out_specs = (P(("grp", "dp"), None, ("kv", "tp")), P(("grp", "dp", "kv"), "tp", None, None))
    return jax.shard_map(
        functools.partial(per_device, mesh.shape["kv"], mesh.shape["tp"]),
        mesh=mesh,
        in_specs=in_specs,
        out_specs=out_specs,
        check_vma=False,
    )
```

```python
import functools

import jax
import jax.numpy as jnp
from jax import lax
from jax.experimental import pallas as pl
from jax.experimental.pallas import tpu as pltpu
from jax.sharding import PartitionSpec as P

HEAD = 128
EPSILON = 1e-05
CHUNK_HEADS = 4
LINE = 4
LINE_HEADS = 2
CROSS = 1
VMEM_MIB = 56
F32 = jnp.float32
BF16 = jnp.bfloat16

MESSAGES = {
    "0 for 3": (0, 1, 3, 3),
    "0 for 2": (0, 1, 2, 4),
    "0 to 1": (0, 1, 1, 0),
    "1 to 0": (1, 0, 0, 0),
    "1 to 3": (1, 3, 3, 0),
    "1 to 2": (1, 2, 2, 0),
    "2 to 3": (2, 3, 3, 1),
    "2 to 0": (2, 0, 0, 1),
    "2 to 1": (2, 1, 1, 1),
    "3 for 0": (3, 2, 0, 3),
    "3 to 1": (3, 1, 1, 2),
    "3 to 2": (3, 2, 2, 1),
}
OWN = 3
FIRST = {0: ("0 for 3",), 1: ("1 to 0",), 2: ("2 to 1", "2 to 3"), 3: ("3 for 0",)}
THEN = {0: ("0 for 2", "0 to 1"), 3: ("3 to 1", "3 to 2")}
ONWARD = {
    1: (("0 for 3", "1 to 3"), ("0 for 2", "1 to 2")),
    2: (("3 for 0", "2 to 0"), None),
}
PEERS = ((3, 2, 1), (3, 2, 0), (0, 1, 3), (0, 1, 2))


def kernel_any(
    kv,
    tp,
    tokens,
    w_query,
    w_forget,
    w_input,
    w_gate,
    w_out,
    gain,
    head_gain,
    lower_bound,
    state,
    last_forget,
    last_values,
    accepted,
    tk_v,
    own_v,
    peer_v,
    tok_v,
    gain_v,
    hg_v,
    lb_v,
    lf_v,
    lv_v,
    rows_v,
    scaled_v,
    w_v,
    wo_v,
    st_v,
    tkb_v,
    lfr_v,
    lvr_v,
    ssq_v,
    ssq_r,
    prod_v,
    send_v,
    recv_v,
    gath_v,
    acc_v,
    part_v,
    relay_v,
    load_sem,
    w_sem,
    wo_sem,
    st_sem,
    ssq_ssem,
    ssq_rsem,
    rs_ssem,
    rs_rsem,
    relay_ssem,
    relay_rsem,
    ag_ssem,
    ag_rsem,
    tp_ssem,
    tp_rsem,
):
    me = lax.axis_index("kv")
    tme = lax.axis_index("tp")
    seqs, props, feat = tokens.shape
    own_seqs, heads_dev = state.shape[0], state.shape[1]
    own_rows = own_seqs * props
    rows = seqs * props
    width = gain.shape[1]
    head_cols = heads_dev * HEAD
    chunks = heads_dev // CHUNK_HEADS
    cw = CHUNK_HEADS * HEAD
    half = w_out.shape[1] // tp
    weights = (w_query, w_forget, w_input, w_gate)

    def local(src, dst, sem):
        copy = pltpu.make_async_copy(src, dst, sem)
        copy.start()
        return copy

    tok_c = local(tokens, tok_v, load_sem.at[0])
    gain_c = local(gain, gain_v, load_sem.at[1])

    def load_w(c):
        return [
            local(w.at[:, pl.ds(c * cw, cw)], w_v.at[c, :, pl.ds(i * cw, cw)], w_sem.at[c, i])
            for i, w in enumerate(weights)
        ]

    def load_state(c):
        hs = pl.ds(c * CHUNK_HEADS, CHUNK_HEADS)
        return local(state.at[:, hs], st_v.at[:, hs], st_sem.at[c])

    w_c = [load_w(0)]
    small_c = [
        local(last_forget, lf_v, load_sem.at[2]),
        local(last_values, lv_v, load_sem.at[3]),
        local(head_gain, hg_v, load_sem.at[4]),
        local(lower_bound, lb_v, load_sem.at[5]),
    ]
    st_c = []
    for c in range(chunks):
        st_c.append(load_state(c))
        if c + 1 < chunks:
            w_c.append(load_w(c + 1))
    wo_c = []
    for o in range(tp):
        column = pl.multiple_of(lax.rem(tme + o, tp) * half, half)
        wo_c.append(local(w_out.at[:, pl.ds(column, half)], wo_v.at[o], wo_sem.at[o]))

    barrier = pltpu.get_barrier_semaphore()
    kv_peers = [lax.rem(me + o, kv) for o in range(1, kv)]
    tp_peers = [lax.rem(tme + o, tp) for o in range(1, tp)]
    for peer in kv_peers:
        pl.semaphore_signal(barrier, inc=1, device_id={"kv": peer}, device_id_type=pl.DeviceIdType.MESH)
    for peer in tp_peers:
        pl.semaphore_signal(barrier, inc=1, device_id={"tp": peer}, device_id_type=pl.DeviceIdType.MESH)

    def remote(src, dst, ssem, rsem, axis, peer):
        copy = pltpu.make_async_remote_copy(
            src_ref=src,
            dst_ref=dst,
            send_sem=ssem,
            recv_sem=rsem,
            device_id={axis: peer},
            device_id_type=pl.DeviceIdType.MESH,
        )
        copy.start()
        return copy

    tok_c.wait()
    gain_c.wait()
    for s in range(seqs):
        rows_v[pl.ds(s * props, props), :] = tok_v[s].astype(F32)
    x = rows_v[...]
    my_gain = gain_v[:, pl.ds(pl.multiple_of(me * feat, feat), feat)]
    scaled_v[...] = (x * my_gain).astype(BF16)
    ssq_v[...] = jnp.broadcast_to(jnp.sum(x * x, axis=1, keepdims=True), (rows, HEAD))

    pl.semaphore_wait(barrier, kv - 1 + tp - 1)

    def rows_of(device):
        return pl.ds(pl.multiple_of(device * own_rows, own_rows), own_rows)

    ssq_c = [
        remote(
            ssq_v.at[rows_of(peer)], ssq_r.at[o], ssq_ssem.at[o], ssq_rsem.at[o], "kv", peer
        )
        for o, peer in enumerate(kv_peers)
    ]

    place = lax.broadcasted_iota(jnp.int32, (own_rows, 1), 0)
    prop = lax.rem(place, props)
    seq = place // props

    def old_terms():
        for copy in small_c:
            copy.wait()
        for s in range(own_seqs):
            lfr_v[pl.ds(s * props, props), :] = lf_v[s]
            lvr_v[pl.ds(s * props, props), :] = lv_v[s].astype(F32)
        limit = jnp.zeros((own_rows, 1), jnp.int32)
        for s in range(own_seqs):
            limit = jnp.where(seq == s, accepted[s], limit)
        mask = prop < limit
        old = lfr_v[...]
        decay = jnp.where(mask, old, 1.0)
        weight = jnp.where(mask, 1.0 - old, 0.0)
        after = jnp.ones_like(decay)
        for lag in range(1, props):
            after = after * jnp.where(
                prop < props - lag, pltpu.roll(decay, own_rows - lag, 0), 1.0
            )
        return decay * after, weight * after, lvr_v[...].astype(BF16)

    def take(c, ends, old_weight, old_values):
        st_c[c].wait()
        lane_seq = lax.broadcasted_iota(jnp.int32, (1, own_rows), 1) // props
        for h in range(c * CHUNK_HEADS, (c + 1) * CHUNK_HEADS):
            cols = slice(h * HEAD, (h + 1) * HEAD)
            end_t = ends[:, cols].T
            weight_t = old_weight[:, cols].T
            for s in range(own_seqs):
                mine = jnp.where(lane_seq == s, weight_t, 0.0).astype(BF16)
                added = jnp.dot(mine, old_values[:, cols], preferred_element_type=F32)
                new = end_t[:, s * props : s * props + 1] * st_v[s, h] + added
                tk_v[s, h] = new
                tkb_v[h, pl.ds(s * HEAD, HEAD), :] = new.astype(BF16)

    relayed = kv == 4
    at_end = jnp.logical_or(me == 0, me == kv - 1)
    first = me == 0
    last = me == kv - 1
    if relayed:

        @pl.when(last)
        def _():
            recv_v[:, kv - 2] = jnp.zeros_like(recv_v[:, kv - 2])

        @pl.when(first)
        def _():
            recv_v[:, 0] = jnp.zeros_like(recv_v[:, 0])

    def rs_copy(c, o):
        return pltpu.make_async_remote_copy(
            src_ref=send_v.at[c, rows_of(kv_peers[o])],
            dst_ref=recv_v.at[c, o],
            send_sem=rs_ssem.at[c, o],
            recv_sem=rs_rsem.at[c, o],
            device_id={"kv": kv_peers[o]},
            device_id_type=pl.DeviceIdType.MESH,
        )

    def relay_copy(c, end):
        far, near = (kv - 1, 1) if end == 0 else (0, kv - 2)
        return pltpu.make_async_remote_copy(
            src_ref=send_v.at[c, rows_of(far)],
            dst_ref=relay_v.at[c],
            send_sem=relay_ssem.at[c],
            recv_sem=relay_rsem.at[c],
            device_id={"kv": near},
            device_id_type=pl.DeviceIdType.MESH,
        )

    def send_blocks(c):
        if not relayed:
            for o in range(kv - 1):
                rs_copy(c, o).start()
            return

        @pl.when(first)
        def _():
            relay_copy(c, 0).start()
            rs_copy(c, 1).start()
            if c > 0:
                rs_copy(c - 1, 0).start()
            if c == chunks - 1:
                rs_copy(c, 0).start()

        @pl.when(last)
        def _():
            relay_copy(c, kv - 1).start()
            rs_copy(c, 1).start()
            if c > 0:
                rs_copy(c - 1, 2).start()
            if c == chunks - 1:
                rs_copy(c, 2).start()

        @pl.when(jnp.logical_not(at_end))
        def _():
            rs_copy(c, 0).start()
            rs_copy(c, 2).start()

    def send_on(c):
        if relayed:

            @pl.when(jnp.logical_not(at_end))
            def _():
                relay_copy(c, 0).wait_recv()
                far = rows_of(kv_peers[1])
                send_v[c, far, :] = (prod_v[c, far, :] + relay_v[c].astype(F32)).astype(BF16)
                rs_copy(c, 1).start()

    def wait_blocks(c):
        for o in range(kv - 1):
            if relayed and o == 0:
                pl.when(jnp.logical_not(first))(lambda o=o: rs_copy(c, o).wait_recv())
            elif relayed and o == kv - 2:
                pl.when(jnp.logical_not(last))(lambda o=o: rs_copy(c, o).wait_recv())
            else:
                rs_copy(c, o).wait_recv()

    def wait_sent(c):
        if not relayed:
            for o in range(kv - 1):
                rs_copy(c, o).wait_send()
            return
        rs_copy(c, 1).wait_send()

        @pl.when(first)
        def _():
            relay_copy(c, 0).wait_send()
            rs_copy(c, 0).wait_send()

        @pl.when(last)
        def _():
            relay_copy(c, kv - 1).wait_send()
            rs_copy(c, 2).wait_send()

        @pl.when(jnp.logical_not(at_end))
        def _():
            rs_copy(c, 0).wait_send()
            rs_copy(c, 2).wait_send()

    terms = None
    for c in range(chunks):
        for copy in w_c[c]:
            copy.wait()
        product = jnp.dot(scaled_v[...], w_v[c], preferred_element_type=F32)
        prod_v[c] = product
        send_v[c] = product.astype(BF16)
        send_blocks(c)
        if terms is None:
            terms = old_terms()
        if c > 0:
            send_on(c - 1)
        take(c, *terms)
    send_on(chunks - 1)

    squares = ssq_v[rows_of(me), :]
    for o in range(kv - 1):
        ssq_c[o].wait_recv()
        squares = squares + ssq_r[o]
    row_scale = lax.rsqrt(squares[:, :1] / width + EPSILON)
    mine_rows = rows_of(me)
    ag_c = []

    def recur(c):
        wait_blocks(c)

        def projected(i):
            total = prod_v[c, mine_rows, pl.ds(i * cw, cw)]
            for o in range(kv - 1):
                total = total + recv_v[c, o, :, pl.ds(i * cw, cw)].astype(F32)
            return total * row_scale

        column = pl.multiple_of(tme * head_cols + c * cw, cw)
        floor_gate = lb_v[:, pl.ds(column, cw)]
        forget = floor_gate + (1.0 - floor_gate) * jax.nn.sigmoid(projected(1))
        keys = 1.0 - forget
        queries = jax.nn.silu(projected(0)) * HEAD ** (-0.5)
        values = projected(2)
        gate = jax.nn.silu(projected(3)) * hg_v[:, pl.ds(column, cw)]
        start = forget
        for lag in range(1, props):
            start = start * jnp.where(prop >= lag, pltpu.roll(forget, lag, 0), 1.0)
        reading = queries * start
        results = []
        for h in range(CHUNK_HEADS):
            cols = slice(h * HEAD, (h + 1) * HEAD)
            lhs = jnp.concatenate(
                [jnp.where(seq == s, reading[:, cols], 0.0) for s in range(own_seqs)], axis=1
            ).astype(BF16)
            results.append(
                jnp.dot(lhs, tkb_v[c * CHUNK_HEADS + h], preferred_element_type=F32)
            )
        decay = queries
        for lag in range(props):
            if lag > 0:
                decay = decay * (forget if lag == 1 else pltpu.roll(forget, lag - 1, 0))
            pair = decay * (keys if lag == 0 else pltpu.roll(keys, lag, 0))
            pair = jnp.where(prop >= lag, pair, 0.0)
            moved = values if lag == 0 else pltpu.roll(values, lag, 0)
            for h in range(CHUNK_HEADS):
                cols = slice(h * HEAD, (h + 1) * HEAD)
                score = jnp.sum(pair[:, cols], axis=1, keepdims=True)
                results[h] = results[h] + score * moved[:, cols]
        outs = []
        for h in range(CHUNK_HEADS):
            cols = slice(h * HEAD, (h + 1) * HEAD)
            r = results[h]
            normed = r * lax.rsqrt(jnp.mean(r * r, axis=1, keepdims=True) + EPSILON)
            outs.append((normed * gate[:, cols]).astype(BF16))
        gath_v[c, mine_rows, :] = jnp.concatenate(outs, axis=1)
        ag_c.append(
            [
                remote(
                    gath_v.at[c, mine_rows],
                    gath_v.at[c, mine_rows],
                    ag_ssem.at[c, o],
                    ag_rsem.at[c, o],
                    "kv",
                    peer,
                )
                for o, peer in enumerate(kv_peers)
            ]
        )

    def product_of(c, o):
        term = jnp.dot(
            gath_v[c], wo_v[o, pl.ds(c * cw, cw), :], preferred_element_type=F32
        )
        return term if c == 0 else acc_v[o] + term

    def gathered(c):
        for o in range(kv - 1):
            ag_c[c][o].wait_recv()

    for c in range(chunks):
        recur(c)
    for copy in wo_c:
        copy.wait()
    for c in range(chunks - 1):
        gathered(c)
        for o in range(tp):
            acc_v[o] = product_of(c, o)
    gathered(chunks - 1)
    tp_c = []
    for o in range(1, tp):
        part_v[o - 1] = product_of(chunks - 1, o).astype(BF16)
        tp_c.append(
            remote(
                part_v.at[o - 1],
                peer_v.at[o - 1],
                tp_ssem.at[o - 1],
                tp_rsem.at[o - 1],
                "tp",
                tp_peers[o - 1],
            )
        )
    own_v[...] = product_of(chunks - 1, 0).astype(BF16)
    for copy in tp_c:
        copy.wait_recv()
    for c in range(chunks):
        wait_sent(c)
    for copies in [ssq_c, *ag_c, tp_c]:
        for copy in copies:
            copy.wait_send()


def kernel_line(
    tp,
    tokens,
    w_query,
    w_forget,
    w_input,
    w_gate,
    w_out,
    gain,
    head_gain,
    lower_bound,
    state,
    last_forget,
    last_values,
    accepted,
    tk_v,
    acc_v,
    last_v,
    wl_v,
    tok_v,
    gain_v,
    hg_v,
    lb_v,
    lf_v,
    lv_v,
    rows_v,
    scaled_v,
    w_v,
    wo_v,
    st_v,
    tkb_v,
    lfr_v,
    lvr_v,
    ssq_v,
    ssq_s,
    ssq_r,
    prod_v,
    send_v,
    recv_v,
    gath_v,
    acc_s,
    load_sem,
    w_sem,
    wo_sem,
    st_sem,
    ssq_ssem,
    ssq_rsem,
    rs_ssem,
    rs_rsem,
    ag_ssem,
    ag_rsem,
    cross_rsem,
    fw_ssem,
    fw_rsem,
    wo_ssem,
    wo_rsem,
    go_sem,
):
    kv = LINE
    me = lax.axis_index("kv")
    tme = lax.axis_index("tp")
    seqs, props, feat = tokens.shape
    own_seqs, heads_dev = state.shape[0], state.shape[1]
    own_rows = own_seqs * props
    rows = seqs * props
    width = gain.shape[1]
    head_cols = heads_dev * HEAD
    chunks = heads_dev // LINE_HEADS
    cw = LINE_HEADS * HEAD
    half = w_out.shape[1] // tp
    weights = (w_query, w_forget, w_input, w_gate)

    at_end = jnp.logical_or(me == 0, me == kv - 1)

    def local(src, dst, sem):
        copy = pltpu.make_async_copy(src, dst, sem)
        copy.start()
        return copy

    tok_c = local(tokens, tok_v, load_sem.at[0])
    gain_c = local(gain, gain_v, load_sem.at[1])

    def held(ref, sem):
        pltpu.make_async_copy(ref, ref, sem).wait()

    def load_w(c):
        for i, w in enumerate(weights):
            local(w.at[:, pl.ds(c * cw, cw)], w_v.at[c, :, pl.ds(i * cw, cw)], w_sem.at[c])

    def load_late():
        small = [
            local(last_forget, lf_v, load_sem.at[2]),
            local(last_values, lv_v, load_sem.at[3]),
            local(head_gain, hg_v, load_sem.at[4]),
            local(lower_bound, lb_v, load_sem.at[5]),
            local(accepted, acc_s, load_sem.at[6]),
        ]
        return small, local(state, st_v, st_sem)

    split = (chunks - 1) * cw
    crossed = chunks - CROSS

    def load_out():
        cols = pl.ds(pl.multiple_of(tme * half, half), half)
        local(w_out.at[:split, cols], wo_v.at[0], wo_sem)
        local(w_out.at[split:, cols], wl_v.at[0], wo_sem)

    def out_held(sem):
        held(w_v.at[0, : head_cols * half // (4 * cw)], sem)

    load_w(0)

    def signal(axis, peer):
        pl.semaphore_signal(
            barrier, inc=1, device_id={axis: peer}, device_id_type=pl.DeviceIdType.MESH
        )

    barrier = pltpu.get_barrier_semaphore()
    tp_peers = [lax.rem(tme + o, tp) for o in range(1, tp)]
    for peer in tp_peers:
        signal("tp", peer)

    @pl.when(me > 0)
    def _():
        signal("kv", me - 1)

    @pl.when(me < kv - 1)
    def _():
        signal("kv", me + 1)

    def remote(src, dst, ssem, rsem, axis, peer):
        return pltpu.make_async_remote_copy(
            src_ref=src,
            dst_ref=dst,
            send_sem=ssem,
            recv_sem=rsem,
            device_id={axis: peer},
            device_id_type=pl.DeviceIdType.MESH,
        )

    tok_c.wait()
    gain_c.wait()
    load_w(1)
    load_w(2)
    for s in range(seqs):
        rows_v[pl.ds(s * props, props), :] = tok_v[s].astype(F32)
    x = rows_v[...]
    my_gain = gain_v[:, pl.ds(pl.multiple_of(me * feat, feat), feat)]
    scaled_v[...] = (x * my_gain).astype(BF16)
    squared = jnp.sum(x * x, axis=1, keepdims=True)
    on_row = lax.broadcasted_iota(jnp.int32, (rows, HEAD), 0)
    on_lane = lax.broadcasted_iota(jnp.int32, (rows, HEAD), 1)
    along = jnp.sum(jnp.where(on_row == on_lane, squared, 0.0), axis=0, keepdims=True)
    ssq_v[...] = jnp.broadcast_to(along, ssq_v.shape)

    def rows_of(device):
        return pl.ds(pl.multiple_of(device * own_rows, own_rows), own_rows)

    def message(c, name):
        _, to, dest, slot = MESSAGES[name]
        return remote(
            send_v.at[c, rows_of(dest)],
            recv_v.at[c, slot],
            rs_ssem,
            rs_rsem.at[c, max(slot - OWN + 1, 0)],
            "kv",
            to,
        )

    def pass_on(c, name, onward):
        _, _, dest, slot = MESSAGES[name]
        message(c, name).wait_recv()
        into = rows_of(dest)
        send_v[c, into, :] = (prod_v[c, into, :] + recv_v[c, slot].astype(F32)).astype(BF16)
        message(c, onward).start()

    def ssq_copy(i, slot, to):
        return remote(ssq_s.at[i], ssq_r.at[slot], ssq_ssem.at[i], ssq_rsem.at[slot], "kv", to)

    ssq_s[0] = ssq_v[...]
    partner = me + 1 - 2 * lax.rem(me, 2)
    across = jnp.where(me == 1, 2, 1)
    beyond = jnp.where(me == 1, 3, 0)
    inside = jnp.logical_not(at_end)
    pl.semaphore_wait(barrier, jnp.where(at_end, tp, tp + 1))
    ssq_copy(0, 0, partner).start()

    @pl.when(inside)
    def _():
        pl.semaphore_signal(
            go_sem, inc=1, device_id={"kv": across}, device_id_type=pl.DeviceIdType.MESH
        )

    @pl.when(me == 2)
    def _():
        pl.semaphore_signal(
            go_sem, inc=1, device_id={"kv": 3}, device_id_type=pl.DeviceIdType.MESH
        )

    @pl.when(me != 1)
    def _():
        recv_v[:, OWN - 1] = jnp.zeros_like(recv_v[:, OWN - 1])

    place = lax.broadcasted_iota(jnp.int32, (own_rows, 1), 0)
    prop = lax.rem(place, props)
    seq = place // props

    def old_terms():
        for copy in small_c:
            copy.wait()
        for s in range(own_seqs):
            lfr_v[pl.ds(s * props, props), :] = lf_v[s]
            lvr_v[pl.ds(s * props, props), :] = lv_v[s].astype(F32)
        limit = jnp.zeros((own_rows, 1), jnp.int32)
        for s in range(own_seqs):
            limit = jnp.where(seq == s, acc_s[s], limit)
        mask = prop < limit
        old = lfr_v[...]
        decay = jnp.where(mask, old, 1.0)
        weight = jnp.where(mask, 1.0 - old, 0.0)
        after = jnp.ones_like(decay)
        for lag in range(1, props):
            after = after * jnp.where(
                prop < props - lag, pltpu.roll(decay, own_rows - lag, 0), 1.0
            )
        return decay * after, weight * after, lvr_v[...].astype(BF16)

    def take(c, ends, old_weight, old_values):
        if c == 0:
            st_c.wait()
        lane_seq = lax.broadcasted_iota(jnp.int32, (1, own_rows), 1) // props
        for h in range(c * LINE_HEADS, (c + 1) * LINE_HEADS):
            cols = slice(h * HEAD, (h + 1) * HEAD)
            end_t = ends[:, cols].T
            weight_t = old_weight[:, cols].T
            for s in range(own_seqs):
                mine = jnp.where(lane_seq == s, weight_t, 0.0).astype(BF16)
                added = jnp.dot(mine, old_values[:, cols], preferred_element_type=F32)
                new = end_t[:, s * props : s * props + 1] * st_v[s, h] + added
                tk_v[s, h] = new
                tkb_v[h, pl.ds(s * HEAD, HEAD), :] = new.astype(BF16)

    for c in range(chunks):
        held(w_v.at[c], w_sem.at[c])
        if c + 3 < chunks:
            load_w(c + 3)
        elif c + 3 == chunks:
            small_c, st_c = load_late()
        elif c + 2 == chunks:
            load_out()
        product = jnp.dot(scaled_v[...], w_v[c], preferred_element_type=F32)
        prod_v[c] = product
        send_v[c] = product.astype(BF16)

        for device, names in FIRST.items():

            @pl.when(me == device)
            def _():
                for name in names:
                    message(c, name).start()

    for device, names in THEN.items():

        @pl.when(me == device)
        def _():
            if device == 3:
                pl.semaphore_wait(go_sem, 1)
            for name in names:
                for c in range(chunks):
                    message(c, name).start()

    terms = old_terms()
    ssq_copy(0, 0, partner).wait_recv()

    @pl.when(inside)
    def _():
        pl.semaphore_wait(go_sem, 1)
        ssq_s[1] = ssq_v[...] + ssq_r[0]
        ssq_copy(1, 1, across).start()
        ssq_s[2] = ssq_v[...] + ssq_r[0]
        ssq_copy(2, 1, beyond).start()

    for c in range(chunks):
        for device, steps in ONWARD.items():

            @pl.when(me == device)
            def _():
                pass_on(c, *steps[0])

        take(c, *terms)

    @pl.when(me == 1)
    def _():
        for c in range(chunks):
            pass_on(c, *ONWARD[1][1])

    for o in range(1, tp):
        cols = pl.ds(pl.multiple_of(tp_peers[o - 1] * half, half), half)
        for rows_out, into in ((w_out.at[:split, cols], wo_v), (w_out.at[split:, cols], wl_v)):
            copy = remote(
                rows_out, into.at[tp - o], wo_ssem.at[o - 1], wo_rsem.at[tp - o - 1],
                "tp", tp_peers[o - 1],
            )
            copy.start()

    ssq_copy(1, 1, partner).wait_recv()
    whole = ssq_v[...] + ssq_r[0] + ssq_r[1]
    mine_rows = rows_of(me)
    picked = lax.broadcasted_iota(jnp.int32, (own_rows, HEAD), 1) == (
        lax.broadcasted_iota(jnp.int32, (own_rows, HEAD), 0) + me * own_rows
    )
    squares = jnp.sum(jnp.where(picked, whole[:1], 0.0), axis=1, keepdims=True)
    row_scale = lax.rsqrt(squares / width + EPSILON)
    peers = [
        functools.reduce(lambda found, d: jnp.where(me == d, PEERS[d][o], found), range(kv), 0)
        for o in range(kv - 1)
    ]

    def heads_of(c, slot):
        return gath_v.at[slot, c] if c < chunks - 1 else last_v.at[slot]

    def head_copy(c, o):
        mine = heads_of(c, 0).at[mine_rows]
        return remote(mine, mine, ag_ssem, ag_rsem.at[c], "kv", peers[o])

    def cross_copy(c, o, i):
        ids = {"tp": tp_peers[o - 1]}
        if i < kv - 1:
            ids["kv"] = peers[i]
        return pltpu.make_async_remote_copy(
            src_ref=heads_of(c, 0).at[mine_rows],
            dst_ref=heads_of(c, tp - o).at[mine_rows],
            send_sem=ag_ssem,
            recv_sem=cross_rsem.at[c - crossed, tp - o - 1],
            device_id=ids,
            device_id_type=pl.DeviceIdType.MESH,
        )

    def cross_copies(c):
        return [cross_copy(c, o, i) for o in range(1, tp) for i in range(kv)]

    def forward(c, o):
        return remote(
            gath_v.at[0, c], gath_v.at[tp - o, c], fw_ssem.at[c, o - 1],
            fw_rsem.at[c, tp - o - 1], "tp", tp_peers[o - 1],
        )

    def recur(c):
        @pl.when(me == 1)
        def _():
            held(recv_v.at[c, :OWN], rs_rsem.at[c, 0])

        @pl.when(me != 1)
        def _():
            held(recv_v.at[c, : OWN - 1], rs_rsem.at[c, 0])

        def projected(i):
            cols = pl.ds(i * cw, cw)
            total = prod_v[c, mine_rows, cols]
            for slot in range(OWN):
                total = total + recv_v[c, slot, :, cols].astype(F32)
            return total * row_scale

        column = pl.multiple_of(tme * head_cols + c * cw, cw)
        floor_gate = lb_v[:, pl.ds(column, cw)]
        forget = floor_gate + (1.0 - floor_gate) * jax.nn.sigmoid(projected(1))
        keys = 1.0 - forget
        queries = jax.nn.silu(projected(0)) * HEAD ** (-0.5)
        values = projected(2)
        gate = jax.nn.silu(projected(3)) * hg_v[:, pl.ds(column, cw)]
        start = forget
        for lag in range(1, props):
            start = start * jnp.where(prop >= lag, pltpu.roll(forget, lag, 0), 1.0)
        reading = queries * start
        results = []
        for h in range(LINE_HEADS):
            cols = slice(h * HEAD, (h + 1) * HEAD)
            lhs = jnp.concatenate(
                [jnp.where(seq == s, reading[:, cols], 0.0) for s in range(own_seqs)], axis=1
            ).astype(BF16)
            results.append(
                jnp.dot(lhs, tkb_v[c * LINE_HEADS + h], preferred_element_type=F32)
            )
        decay = queries
        for lag in range(props):
            if lag > 0:
                decay = decay * (forget if lag == 1 else pltpu.roll(forget, lag - 1, 0))
            pair = decay * (keys if lag == 0 else pltpu.roll(keys, lag, 0))
            pair = jnp.where(prop >= lag, pair, 0.0)
            moved = values if lag == 0 else pltpu.roll(values, lag, 0)
            for h in range(LINE_HEADS):
                cols = slice(h * HEAD, (h + 1) * HEAD)
                score = jnp.sum(pair[:, cols], axis=1, keepdims=True)
                results[h] = results[h] + score * moved[:, cols]
        outs = []
        for h in range(LINE_HEADS):
            cols = slice(h * HEAD, (h + 1) * HEAD)
            r = results[h]
            normed = r * lax.rsqrt(jnp.mean(r * r, axis=1, keepdims=True) + EPSILON)
            outs.append((normed * gate[:, cols]).astype(BF16))
        heads_of(c, 0)[mine_rows, :] = jnp.concatenate(outs, axis=1)
        for o in range(kv - 1):
            head_copy(c, o).start()
        if c >= crossed:
            for copy in cross_copies(c):
                copy.start()

    def gathered(c):
        held(heads_of(c, 0).at[: (kv - 1) * own_rows], ag_rsem.at[c])

    def product_of(c, slot):
        term = jnp.dot(
            gath_v[slot, c], wo_v[slot, pl.ds(c * cw, cw), :], preferred_element_type=F32
        )
        acc_v[slot] = term if c == 0 else acc_v[slot] + term

    def from_tp(c):
        for o in range(1, tp):
            if c < crossed:
                forward(c, tp - o).wait_recv()
                continue
            held(heads_of(c, o), cross_rsem.at[c - crossed, o - 1])

    for c in range(chunks):
        recur(c)
    out_held(wo_sem)
    for o in range(1, tp):
        out_held(wo_rsem.at[o - 1])
    for c in range(chunks):
        gathered(c)
        if c < crossed:
            for o in range(1, tp):
                forward(c, o).start()
        if c < chunks - 1:
            product_of(c, 0)
        if c > 0:
            from_tp(c - 1)
            for o in range(1, tp):
                product_of(c - 1, o)
    from_tp(chunks - 1)

    held(send_v.at[:, : (kv - 1) * own_rows], rs_ssem)
    ssq_copy(0, 0, partner).wait_send()

    @pl.when(inside)
    def _():
        ssq_copy(1, 1, across).wait_send()
        ssq_copy(2, 1, beyond).wait_send()

    blocks = chunks * (kv - 1) + CROSS * (tp - 1) * kv
    held(w_v.at[0, : blocks * own_rows // 4], ag_ssem)
    for o in range(1, tp):
        out_held(wo_ssem.at[o - 1])
    for c in range(crossed):
        for o in range(1, tp):
            forward(c, o).wait_send()


def finish_line(tk_v, acc_v, last_v, wl_v, mixed, taken, mix_v, sem):
    tk_c = pltpu.make_async_copy(tk_v, taken, sem.at[0])
    tk_c.start()
    seqs, props, _ = mixed.shape
    total = 0.0
    for slot in range(acc_v.shape[0]):
        term = jnp.dot(last_v[slot], wl_v[slot], preferred_element_type=F32)
        total = total + (acc_v[slot] + term).astype(BF16).astype(F32)
    for s in range(seqs):
        mix_v[s] = total[s * props : (s + 1) * props].astype(BF16)
    mix_c = pltpu.make_async_copy(mix_v, mixed, sem.at[1])
    mix_c.start()
    mix_c.wait()
    tk_c.wait()


def finish(tk_v, own_v, peer_v, mixed, taken, mix_v, sem):
    tk_c = pltpu.make_async_copy(tk_v, taken, sem.at[0])
    tk_c.start()
    seqs, props, _ = mixed.shape
    total = own_v[...].astype(F32)
    for o in range(peer_v.shape[0]):
        total = total + peer_v[o].astype(F32)
    for s in range(seqs):
        mix_v[s] = total[s * props : (s + 1) * props].astype(BF16)
    mix_c = pltpu.make_async_copy(mix_v, mixed, sem.at[1])
    mix_c.start()
    mix_c.wait()
    tk_c.wait()


def per_device(
    kv,
    tp,
    tokens,
    w_query,
    w_forget,
    w_input,
    w_gate,
    w_out,
    gain,
    head_gain,
    lower_bound,
    state,
    last_forget,
    last_values,
    accepted,
):
    seqs, props, feat = tokens.shape
    own_seqs, heads_dev = state.shape[0], state.shape[1]
    own_rows = own_seqs * props
    rows = seqs * props
    head_cols = heads_dev * HEAD
    on_line = kv == LINE and rows <= HEAD
    per_chunk = LINE_HEADS if on_line else CHUNK_HEADS
    chunks = heads_dev // per_chunk
    cw = per_chunk * HEAD
    half = w_out.shape[1] // tp
    peers = kv - 1
    dma = pltpu.SemaphoreType.DMA
    scratch = [
        pltpu.VMEM(tokens.shape, BF16),
        pltpu.VMEM((1, gain.shape[0]), F32),
        pltpu.VMEM((1, head_gain.shape[0]), F32),
        pltpu.VMEM((1, lower_bound.shape[0]), F32),
        pltpu.VMEM(last_forget.shape, F32),
        pltpu.VMEM(last_values.shape, BF16),
        pltpu.VMEM((rows, feat), F32),
        pltpu.VMEM((rows, feat), BF16),
        pltpu.VMEM((chunks, feat, 4 * cw), BF16),
        pltpu.VMEM((tp, head_cols, half), BF16),
        pltpu.VMEM(state.shape, F32),
        pltpu.VMEM((heads_dev, own_seqs * HEAD, HEAD), BF16),
        pltpu.VMEM((own_rows, head_cols), F32),
        pltpu.VMEM((own_rows, head_cols), F32),
    ]
    if on_line:
        body, last = functools.partial(kernel_line, tp), finish_line
        scratch[9] = pltpu.VMEM((tp, head_cols - cw, half), BF16)
        outs = (
            pltpu.VMEM(state.shape, F32),
            pltpu.VMEM((tp, rows, half), F32),
            pltpu.VMEM((tp, rows, cw), BF16),
            pltpu.VMEM((tp, cw, half), BF16),
        )
        scratch += [
            pltpu.VMEM((1, HEAD), F32),
            pltpu.VMEM((3, 1, HEAD), F32),
            pltpu.VMEM((2, 1, HEAD), F32),
            pltpu.VMEM((chunks, rows, 4 * cw), F32),
            pltpu.VMEM((chunks, rows, 4 * cw), BF16),
            pltpu.VMEM((chunks, 5, own_rows, 4 * cw), BF16),
            pltpu.VMEM((tp, chunks - 1, rows, cw), BF16),
            pltpu.SMEM((own_seqs,), jnp.int32),
            dma((7,)),
            dma((chunks,)),
            dma,
            dma,
            dma((3,)),
            dma((2,)),
            dma,
            dma((chunks, 3)),
            dma,
            dma((chunks,)),
            dma((CROSS, tp - 1)),
            dma((chunks - CROSS, tp - 1)),
            dma((chunks - CROSS, tp - 1)),
            dma((tp - 1,)),
            dma((tp - 1,)),
            pltpu.SemaphoreType.REGULAR,
        ]
    else:
        body, last = functools.partial(kernel_any, kv, tp), finish
        outs = (
            pltpu.VMEM(state.shape, F32),
            pltpu.VMEM((rows, half), BF16),
            pltpu.VMEM((tp - 1, rows, half), BF16),
        )
        scratch += [
            pltpu.VMEM((rows, HEAD), F32),
            pltpu.VMEM((peers, own_rows, HEAD), F32),
            pltpu.VMEM((chunks, rows, 4 * cw), F32),
            pltpu.VMEM((chunks, rows, 4 * cw), BF16),
            pltpu.VMEM((chunks, peers, own_rows, 4 * cw), BF16),
            pltpu.VMEM((chunks, rows, cw), BF16),
            pltpu.VMEM((tp, rows, half), F32),
            pltpu.VMEM((tp - 1, rows, half), BF16),
            pltpu.VMEM((chunks, own_rows, 4 * cw), BF16),
            dma((6,)),
            dma((chunks, 4)),
            dma((tp,)),
            dma((chunks,)),
            dma((peers,)),
            dma((peers,)),
            dma((chunks, peers)),
            dma((chunks, peers)),
            dma((chunks,)),
            dma((chunks,)),
            dma((chunks, peers)),
            dma((chunks, peers)),
            dma((tp - 1,)),
            dma((tp - 1,)),
        ]
    anywhere = pl.BlockSpec(memory_space=pl.ANY)
    held = pl.BlockSpec(memory_space=pltpu.VMEM)
    results = pl.pallas_call(
        body,
        out_shape=outs,
        in_specs=[pl.BlockSpec(memory_space=pltpu.HBM)] * 12
        + [pl.BlockSpec(memory_space=pltpu.HBM if on_line else pltpu.SMEM)],
        out_specs=(held,) * len(outs),
        scratch_shapes=scratch,
        compiler_params=pltpu.CompilerParams(
            collective_id=0, has_side_effects=True, vmem_limit_bytes=VMEM_MIB * 1024 * 1024
        ),
    )(
        tokens,
        w_query,
        w_forget,
        w_input,
        w_gate,
        w_out,
        gain.reshape(1, -1),
        head_gain.reshape(1, -1),
        lower_bound.reshape(1, -1),
        state,
        last_forget,
        last_values,
        accepted,
    )
    return pl.pallas_call(
        last,
        out_shape=(
            jax.ShapeDtypeStruct((seqs, props, half), BF16),
            jax.ShapeDtypeStruct(state.shape, F32),
        ),
        in_specs=[held] * len(outs),
        out_specs=(anywhere, anywhere),
        scratch_shapes=[pltpu.VMEM((seqs, props, half), BF16), dma((2,))],
        compiler_params=pltpu.CompilerParams(vmem_limit_bytes=4 * 1024 * 1024),
    )(*results)


def solution(mesh):
    in_specs = (
        P(("grp", "dp"), None, "kv"),
        P("kv", "tp"),
        P("kv", "tp"),
        P("kv", "tp"),
        P("kv", "tp"),
        P("tp", "kv"),
        P(),
        P(),
        P(),
        P(("grp", "dp", "kv"), "tp", None, None),
        P(("grp", "dp", "kv"), None, "tp"),
        P(("grp", "dp", "kv"), None, "tp"),
        P(("grp", "dp", "kv")),
    )
    out_specs = (P(("grp", "dp"), None, ("kv", "tp")), P(("grp", "dp", "kv"), "tp", None, None))
    return jax.shard_map(
        functools.partial(per_device, mesh.shape["kv"], mesh.shape["tp"]),
        mesh=mesh,
        in_specs=in_specs,
        out_specs=out_specs,
        check_vma=False,
    )
```

```python
import functools

import jax
import jax.numpy as jnp
from jax import lax
from jax.experimental import pallas as pl
from jax.experimental.pallas import tpu as pltpu
from jax.sharding import PartitionSpec as P

HEAD = 128
EPSILON = 1e-05
CHUNK_HEADS = 4
LINE = 4
LINE_HEADS = 2
CROSS = 1
VMEM_MIB = 56
F32 = jnp.float32
BF16 = jnp.bfloat16

MESSAGES = {
    "0 for 3": (0, 1, 3, 3),
    "0 for 2": (0, 1, 2, 4),
    "0 to 1": (0, 1, 1, 0),
    "1 to 0": (1, 0, 0, 0),
    "1 to 3": (1, 3, 3, 0),
    "1 to 2": (1, 2, 2, 0),
    "2 to 3": (2, 3, 3, 1),
    "2 to 0": (2, 0, 0, 1),
    "2 to 1": (2, 1, 1, 1),
    "3 for 1": (3, 2, 1, 3),
    "3 to 1": (3, 1, 1, 2),
    "3 to 2": (3, 2, 2, 1),
    "3 to 0": (3, 0, 0, 2),
}
OWN = 3
DIRECT = 1
PEERS = ((3, 2, 1), (3, 2, 0), (0, 1, 3), (0, 1, 2))


def kernel_any(
    kv,
    tp,
    tokens,
    w_query,
    w_forget,
    w_input,
    w_gate,
    w_out,
    gain,
    head_gain,
    lower_bound,
    state,
    last_forget,
    last_values,
    accepted,
    tk_v,
    own_v,
    peer_v,
    tok_v,
    gain_v,
    hg_v,
    lb_v,
    lf_v,
    lv_v,
    rows_v,
    scaled_v,
    w_v,
    wo_v,
    st_v,
    tkb_v,
    lfr_v,
    lvr_v,
    ssq_v,
    ssq_r,
    prod_v,
    send_v,
    recv_v,
    gath_v,
    acc_v,
    part_v,
    relay_v,
    load_sem,
    w_sem,
    wo_sem,
    st_sem,
    ssq_ssem,
    ssq_rsem,
    rs_ssem,
    rs_rsem,
    relay_ssem,
    relay_rsem,
    ag_ssem,
    ag_rsem,
    tp_ssem,
    tp_rsem,
):
    me = lax.axis_index("kv")
    tme = lax.axis_index("tp")
    seqs, props, feat = tokens.shape
    own_seqs, heads_dev = state.shape[0], state.shape[1]
    own_rows = own_seqs * props
    rows = seqs * props
    width = gain.shape[1]
    head_cols = heads_dev * HEAD
    chunks = heads_dev // CHUNK_HEADS
    cw = CHUNK_HEADS * HEAD
    half = w_out.shape[1] // tp
    weights = (w_query, w_forget, w_input, w_gate)

    def local(src, dst, sem):
        copy = pltpu.make_async_copy(src, dst, sem)
        copy.start()
        return copy

    tok_c = local(tokens, tok_v, load_sem.at[0])
    gain_c = local(gain, gain_v, load_sem.at[1])

    def load_w(c):
        return [
            local(w.at[:, pl.ds(c * cw, cw)], w_v.at[c, :, pl.ds(i * cw, cw)], w_sem.at[c, i])
            for i, w in enumerate(weights)
        ]

    def load_state(c):
        hs = pl.ds(c * CHUNK_HEADS, CHUNK_HEADS)
        return local(state.at[:, hs], st_v.at[:, hs], st_sem.at[c])

    w_c = [load_w(0)]
    small_c = [
        local(last_forget, lf_v, load_sem.at[2]),
        local(last_values, lv_v, load_sem.at[3]),
        local(head_gain, hg_v, load_sem.at[4]),
        local(lower_bound, lb_v, load_sem.at[5]),
    ]
    st_c = []
    for c in range(chunks):
        st_c.append(load_state(c))
        if c + 1 < chunks:
            w_c.append(load_w(c + 1))
    wo_c = []
    for o in range(tp):
        column = pl.multiple_of(lax.rem(tme + o, tp) * half, half)
        wo_c.append(local(w_out.at[:, pl.ds(column, half)], wo_v.at[o], wo_sem.at[o]))

    barrier = pltpu.get_barrier_semaphore()
    kv_peers = [lax.rem(me + o, kv) for o in range(1, kv)]
    tp_peers = [lax.rem(tme + o, tp) for o in range(1, tp)]
    for peer in kv_peers:
        pl.semaphore_signal(barrier, inc=1, device_id={"kv": peer}, device_id_type=pl.DeviceIdType.MESH)
    for peer in tp_peers:
        pl.semaphore_signal(barrier, inc=1, device_id={"tp": peer}, device_id_type=pl.DeviceIdType.MESH)

    def remote(src, dst, ssem, rsem, axis, peer):
        copy = pltpu.make_async_remote_copy(
            src_ref=src,
            dst_ref=dst,
            send_sem=ssem,
            recv_sem=rsem,
            device_id={axis: peer},
            device_id_type=pl.DeviceIdType.MESH,
        )
        copy.start()
        return copy

    tok_c.wait()
    gain_c.wait()
    for s in range(seqs):
        rows_v[pl.ds(s * props, props), :] = tok_v[s].astype(F32)
    x = rows_v[...]
    my_gain = gain_v[:, pl.ds(pl.multiple_of(me * feat, feat), feat)]
    scaled_v[...] = (x * my_gain).astype(BF16)
    ssq_v[...] = jnp.broadcast_to(jnp.sum(x * x, axis=1, keepdims=True), (rows, HEAD))

    pl.semaphore_wait(barrier, kv - 1 + tp - 1)

    def rows_of(device):
        return pl.ds(pl.multiple_of(device * own_rows, own_rows), own_rows)

    ssq_c = [
        remote(
            ssq_v.at[rows_of(peer)], ssq_r.at[o], ssq_ssem.at[o], ssq_rsem.at[o], "kv", peer
        )
        for o, peer in enumerate(kv_peers)
    ]

    place = lax.broadcasted_iota(jnp.int32, (own_rows, 1), 0)
    prop = lax.rem(place, props)
    seq = place // props

    def old_terms():
        for copy in small_c:
            copy.wait()
        for s in range(own_seqs):
            lfr_v[pl.ds(s * props, props), :] = lf_v[s]
            lvr_v[pl.ds(s * props, props), :] = lv_v[s].astype(F32)
        limit = jnp.zeros((own_rows, 1), jnp.int32)
        for s in range(own_seqs):
            limit = jnp.where(seq == s, accepted[s], limit)
        mask = prop < limit
        old = lfr_v[...]
        decay = jnp.where(mask, old, 1.0)
        weight = jnp.where(mask, 1.0 - old, 0.0)
        after = jnp.ones_like(decay)
        for lag in range(1, props):
            after = after * jnp.where(
                prop < props - lag, pltpu.roll(decay, own_rows - lag, 0), 1.0
            )
        return decay * after, weight * after, lvr_v[...].astype(BF16)

    def take(c, ends, old_weight, old_values):
        st_c[c].wait()
        lane_seq = lax.broadcasted_iota(jnp.int32, (1, own_rows), 1) // props
        for h in range(c * CHUNK_HEADS, (c + 1) * CHUNK_HEADS):
            cols = slice(h * HEAD, (h + 1) * HEAD)
            end_t = ends[:, cols].T
            weight_t = old_weight[:, cols].T
            for s in range(own_seqs):
                mine = jnp.where(lane_seq == s, weight_t, 0.0).astype(BF16)
                added = jnp.dot(mine, old_values[:, cols], preferred_element_type=F32)
                new = end_t[:, s * props : s * props + 1] * st_v[s, h] + added
                tk_v[s, h] = new
                tkb_v[h, pl.ds(s * HEAD, HEAD), :] = new.astype(BF16)

    relayed = kv == 4
    at_end = jnp.logical_or(me == 0, me == kv - 1)
    first = me == 0
    last = me == kv - 1
    if relayed:

        @pl.when(last)
        def _():
            recv_v[:, kv - 2] = jnp.zeros_like(recv_v[:, kv - 2])

        @pl.when(first)
        def _():
            recv_v[:, 0] = jnp.zeros_like(recv_v[:, 0])

    def rs_copy(c, o):
        return pltpu.make_async_remote_copy(
            src_ref=send_v.at[c, rows_of(kv_peers[o])],
            dst_ref=recv_v.at[c, o],
            send_sem=rs_ssem.at[c, o],
            recv_sem=rs_rsem.at[c, o],
            device_id={"kv": kv_peers[o]},
            device_id_type=pl.DeviceIdType.MESH,
        )

    def relay_copy(c, end):
        far, near = (kv - 1, 1) if end == 0 else (0, kv - 2)
        return pltpu.make_async_remote_copy(
            src_ref=send_v.at[c, rows_of(far)],
            dst_ref=relay_v.at[c],
            send_sem=relay_ssem.at[c],
            recv_sem=relay_rsem.at[c],
            device_id={"kv": near},
            device_id_type=pl.DeviceIdType.MESH,
        )

    def send_blocks(c):
        if not relayed:
            for o in range(kv - 1):
                rs_copy(c, o).start()
            return

        @pl.when(first)
        def _():
            relay_copy(c, 0).start()
            rs_copy(c, 1).start()
            if c > 0:
                rs_copy(c - 1, 0).start()
            if c == chunks - 1:
                rs_copy(c, 0).start()

        @pl.when(last)
        def _():
            relay_copy(c, kv - 1).start()
            rs_copy(c, 1).start()
            if c > 0:
                rs_copy(c - 1, 2).start()
            if c == chunks - 1:
                rs_copy(c, 2).start()

        @pl.when(jnp.logical_not(at_end))
        def _():
            rs_copy(c, 0).start()
            rs_copy(c, 2).start()

    def send_on(c):
        if relayed:

            @pl.when(jnp.logical_not(at_end))
            def _():
                relay_copy(c, 0).wait_recv()
                far = rows_of(kv_peers[1])
                send_v[c, far, :] = (prod_v[c, far, :] + relay_v[c].astype(F32)).astype(BF16)
                rs_copy(c, 1).start()

    def wait_blocks(c):
        for o in range(kv - 1):
            if relayed and o == 0:
                pl.when(jnp.logical_not(first))(lambda o=o: rs_copy(c, o).wait_recv())
            elif relayed and o == kv - 2:
                pl.when(jnp.logical_not(last))(lambda o=o: rs_copy(c, o).wait_recv())
            else:
                rs_copy(c, o).wait_recv()

    def wait_sent(c):
        if not relayed:
            for o in range(kv - 1):
                rs_copy(c, o).wait_send()
            return
        rs_copy(c, 1).wait_send()

        @pl.when(first)
        def _():
            relay_copy(c, 0).wait_send()
            rs_copy(c, 0).wait_send()

        @pl.when(last)
        def _():
            relay_copy(c, kv - 1).wait_send()
            rs_copy(c, 2).wait_send()

        @pl.when(jnp.logical_not(at_end))
        def _():
            rs_copy(c, 0).wait_send()
            rs_copy(c, 2).wait_send()

    terms = None
    for c in range(chunks):
        for copy in w_c[c]:
            copy.wait()
        product = jnp.dot(scaled_v[...], w_v[c], preferred_element_type=F32)
        prod_v[c] = product
        send_v[c] = product.astype(BF16)
        send_blocks(c)
        if terms is None:
            terms = old_terms()
        if c > 0:
            send_on(c - 1)
        take(c, *terms)
    send_on(chunks - 1)

    squares = ssq_v[rows_of(me), :]
    for o in range(kv - 1):
        ssq_c[o].wait_recv()
        squares = squares + ssq_r[o]
    row_scale = lax.rsqrt(squares[:, :1] / width + EPSILON)
    mine_rows = rows_of(me)
    ag_c = []

    def recur(c):
        wait_blocks(c)

        def projected(i):
            total = prod_v[c, mine_rows, pl.ds(i * cw, cw)]
            for o in range(kv - 1):
                total = total + recv_v[c, o, :, pl.ds(i * cw, cw)].astype(F32)
            return total * row_scale

        column = pl.multiple_of(tme * head_cols + c * cw, cw)
        floor_gate = lb_v[:, pl.ds(column, cw)]
        forget = floor_gate + (1.0 - floor_gate) * jax.nn.sigmoid(projected(1))
        keys = 1.0 - forget
        queries = jax.nn.silu(projected(0)) * HEAD ** (-0.5)
        values = projected(2)
        gate = jax.nn.silu(projected(3)) * hg_v[:, pl.ds(column, cw)]
        start = forget
        for lag in range(1, props):
            start = start * jnp.where(prop >= lag, pltpu.roll(forget, lag, 0), 1.0)
        reading = queries * start
        results = []
        for h in range(CHUNK_HEADS):
            cols = slice(h * HEAD, (h + 1) * HEAD)
            lhs = jnp.concatenate(
                [jnp.where(seq == s, reading[:, cols], 0.0) for s in range(own_seqs)], axis=1
            ).astype(BF16)
            results.append(
                jnp.dot(lhs, tkb_v[c * CHUNK_HEADS + h], preferred_element_type=F32)
            )
        decay = queries
        for lag in range(props):
            if lag > 0:
                decay = decay * (forget if lag == 1 else pltpu.roll(forget, lag - 1, 0))
            pair = decay * (keys if lag == 0 else pltpu.roll(keys, lag, 0))
            pair = jnp.where(prop >= lag, pair, 0.0)
            moved = values if lag == 0 else pltpu.roll(values, lag, 0)
            for h in range(CHUNK_HEADS):
                cols = slice(h * HEAD, (h + 1) * HEAD)
                score = jnp.sum(pair[:, cols], axis=1, keepdims=True)
                results[h] = results[h] + score * moved[:, cols]
        outs = []
        for h in range(CHUNK_HEADS):
            cols = slice(h * HEAD, (h + 1) * HEAD)
            r = results[h]
            normed = r * lax.rsqrt(jnp.mean(r * r, axis=1, keepdims=True) + EPSILON)
            outs.append((normed * gate[:, cols]).astype(BF16))
        gath_v[c, mine_rows, :] = jnp.concatenate(outs, axis=1)
        ag_c.append(
            [
                remote(
                    gath_v.at[c, mine_rows],
                    gath_v.at[c, mine_rows],
                    ag_ssem.at[c, o],
                    ag_rsem.at[c, o],
                    "kv",
                    peer,
                )
                for o, peer in enumerate(kv_peers)
            ]
        )

    def product_of(c, o):
        term = jnp.dot(
            gath_v[c], wo_v[o, pl.ds(c * cw, cw), :], preferred_element_type=F32
        )
        return term if c == 0 else acc_v[o] + term

    def gathered(c):
        for o in range(kv - 1):
            ag_c[c][o].wait_recv()

    for c in range(chunks):
        recur(c)
    for copy in wo_c:
        copy.wait()
    for c in range(chunks - 1):
        gathered(c)
        for o in range(tp):
            acc_v[o] = product_of(c, o)
    gathered(chunks - 1)
    tp_c = []
    for o in range(1, tp):
        part_v[o - 1] = product_of(chunks - 1, o).astype(BF16)
        tp_c.append(
            remote(
                part_v.at[o - 1],
                peer_v.at[o - 1],
                tp_ssem.at[o - 1],
                tp_rsem.at[o - 1],
                "tp",
                tp_peers[o - 1],
            )
        )
    own_v[...] = product_of(chunks - 1, 0).astype(BF16)
    for copy in tp_c:
        copy.wait_recv()
    for c in range(chunks):
        wait_sent(c)
    for copies in [ssq_c, *ag_c, tp_c]:
        for copy in copies:
            copy.wait_send()


def kernel_line(
    tp,
    tokens,
    w_query,
    w_forget,
    w_input,
    w_gate,
    w_out,
    gain,
    head_gain,
    lower_bound,
    state,
    last_forget,
    last_values,
    accepted,
    tk_v,
    acc_v,
    last_v,
    wl_v,
    tok_v,
    gain_v,
    hg_v,
    lb_v,
    lf_v,
    lv_v,
    rows_v,
    scaled_v,
    w_v,
    wo_v,
    st_v,
    tkb_v,
    lfr_v,
    lvr_v,
    ssq_v,
    ssq_s,
    ssq_r,
    prod_v,
    send_v,
    recv_v,
    gath_v,
    acc_s,
    load_sem,
    w_sem,
    wo_sem,
    st_sem,
    ssq_ssem,
    ssq_rsem,
    rs_ssem,
    rs_rsem,
    ag_ssem,
    ag_rsem,
    cross_rsem,
    fw_ssem,
    fw_rsem,
    wo_ssem,
    wo_rsem,
    go_sem,
):
    kv = LINE
    me = lax.axis_index("kv")
    tme = lax.axis_index("tp")
    seqs, props, feat = tokens.shape
    own_seqs, heads_dev = state.shape[0], state.shape[1]
    own_rows = own_seqs * props
    rows = seqs * props
    width = gain.shape[1]
    head_cols = heads_dev * HEAD
    chunks = heads_dev // LINE_HEADS
    cw = LINE_HEADS * HEAD
    half = w_out.shape[1] // tp
    weights = (w_query, w_forget, w_input, w_gate)

    at_end = jnp.logical_or(me == 0, me == kv - 1)

    def local(src, dst, sem):
        copy = pltpu.make_async_copy(src, dst, sem)
        copy.start()
        return copy

    tok_c = local(tokens, tok_v, load_sem.at[0])
    gain_c = local(gain, gain_v, load_sem.at[1])

    def held(ref, sem):
        pltpu.make_async_copy(ref, ref, sem).wait()

    def load_w(c):
        for i, w in enumerate(weights):
            local(w.at[:, pl.ds(c * cw, cw)], w_v.at[c, :, pl.ds(i * cw, cw)], w_sem.at[c])

    def load_late():
        small = [
            local(last_forget, lf_v, load_sem.at[2]),
            local(last_values, lv_v, load_sem.at[3]),
            local(head_gain, hg_v, load_sem.at[4]),
            local(lower_bound, lb_v, load_sem.at[5]),
            local(accepted, acc_s, load_sem.at[6]),
        ]
        return small, local(state, st_v, st_sem)

    split = (chunks - 1) * cw
    crossed = chunks - CROSS

    def load_out():
        cols = pl.ds(pl.multiple_of(tme * half, half), half)
        local(w_out.at[:split, cols], wo_v.at[0], wo_sem)
        local(w_out.at[split:, cols], wl_v.at[0], wo_sem)

    def out_held(sem):
        held(w_v.at[0, : head_cols * half // (4 * cw)], sem)

    load_w(0)

    def signal(axis, peer):
        pl.semaphore_signal(
            barrier, inc=1, device_id={axis: peer}, device_id_type=pl.DeviceIdType.MESH
        )

    barrier = pltpu.get_barrier_semaphore()
    tp_peers = [lax.rem(tme + o, tp) for o in range(1, tp)]
    for peer in tp_peers:
        signal("tp", peer)

    @pl.when(me > 0)
    def _():
        signal("kv", me - 1)

    @pl.when(me < kv - 1)
    def _():
        signal("kv", me + 1)

    def remote(src, dst, ssem, rsem, axis, peer):
        return pltpu.make_async_remote_copy(
            src_ref=src,
            dst_ref=dst,
            send_sem=ssem,
            recv_sem=rsem,
            device_id={axis: peer},
            device_id_type=pl.DeviceIdType.MESH,
        )

    tok_c.wait()
    gain_c.wait()
    load_w(1)
    load_w(2)
    for s in range(seqs):
        rows_v[pl.ds(s * props, props), :] = tok_v[s].astype(F32)
    x = rows_v[...]
    my_gain = gain_v[:, pl.ds(pl.multiple_of(me * feat, feat), feat)]
    scaled_v[...] = (x * my_gain).astype(BF16)
    squared = jnp.sum(x * x, axis=1, keepdims=True)
    on_row = lax.broadcasted_iota(jnp.int32, (rows, HEAD), 0)
    on_lane = lax.broadcasted_iota(jnp.int32, (rows, HEAD), 1)
    along = jnp.sum(jnp.where(on_row == on_lane, squared, 0.0), axis=0, keepdims=True)
    ssq_v[...] = jnp.broadcast_to(along, ssq_v.shape)

    def rows_of(device):
        return pl.ds(pl.multiple_of(device * own_rows, own_rows), own_rows)

    def message(c, name):
        _, to, dest, slot = MESSAGES[name]
        return remote(
            send_v.at[c, rows_of(dest)],
            recv_v.at[c, slot],
            rs_ssem,
            rs_rsem.at[c, max(slot - OWN + 1, 0)],
            "kv",
            to,
        )

    def pass_on(c, name, onward):
        _, _, dest, slot = MESSAGES[name]
        message(c, name).wait_recv()
        into = rows_of(dest)
        send_v[c, into, :] = (prod_v[c, into, :] + recv_v[c, slot].astype(F32)).astype(BF16)
        message(c, onward).start()

    def ssq_copy(i, slot, to):
        return remote(ssq_s.at[i], ssq_r.at[slot], ssq_ssem.at[i], ssq_rsem.at[slot], "kv", to)

    ssq_s[0] = ssq_v[...]
    partner = me + 1 - 2 * lax.rem(me, 2)
    across = jnp.where(me == 1, 2, 1)
    beyond = jnp.where(me == 1, 3, 0)
    inside = jnp.logical_not(at_end)
    pl.semaphore_wait(barrier, jnp.where(at_end, tp, tp + 1))
    ssq_copy(0, 0, partner).start()

    def go(to):
        pl.semaphore_signal(
            go_sem, inc=1, device_id={"kv": to}, device_id_type=pl.DeviceIdType.MESH
        )

    @pl.when(inside)
    def _():
        go(across)

    direct = chunks - DIRECT

    def terms_of(c):
        return (me == 0) if c < direct else (me < 2)

    for c in range(chunks):

        @pl.when(jnp.logical_not(terms_of(c)))
        def _():
            recv_v[c, OWN - 1] = jnp.zeros_like(recv_v[c, OWN - 1])

    place = lax.broadcasted_iota(jnp.int32, (own_rows, 1), 0)
    prop = lax.rem(place, props)
    seq = place // props

    def old_terms():
        for copy in small_c:
            copy.wait()
        for s in range(own_seqs):
            lfr_v[pl.ds(s * props, props), :] = lf_v[s]
            lvr_v[pl.ds(s * props, props), :] = lv_v[s].astype(F32)
        limit = jnp.zeros((own_rows, 1), jnp.int32)
        for s in range(own_seqs):
            limit = jnp.where(seq == s, acc_s[s], limit)
        mask = prop < limit
        old = lfr_v[...]
        decay = jnp.where(mask, old, 1.0)
        weight = jnp.where(mask, 1.0 - old, 0.0)
        after = jnp.ones_like(decay)
        for lag in range(1, props):
            after = after * jnp.where(
                prop < props - lag, pltpu.roll(decay, own_rows - lag, 0), 1.0
            )
        return decay * after, weight * after, lvr_v[...].astype(BF16)

    def take(c, ends, old_weight, old_values):
        if c == 0:
            st_c.wait()
        lane_seq = lax.broadcasted_iota(jnp.int32, (1, own_rows), 1) // props
        for h in range(c * LINE_HEADS, (c + 1) * LINE_HEADS):
            cols = slice(h * HEAD, (h + 1) * HEAD)
            end_t = ends[:, cols].T
            weight_t = old_weight[:, cols].T
            for s in range(own_seqs):
                mine = jnp.where(lane_seq == s, weight_t, 0.0).astype(BF16)
                added = jnp.dot(mine, old_values[:, cols], preferred_element_type=F32)
                new = end_t[:, s * props : s * props + 1] * st_v[s, h] + added
                tk_v[s, h] = new
                tkb_v[h, pl.ds(s * HEAD, HEAD), :] = new.astype(BF16)

    for c in range(chunks):
        held(w_v.at[c], w_sem.at[c])
        if c + 3 < chunks:
            load_w(c + 3)
        elif c + 3 == chunks:
            small_c, st_c = load_late()
        elif c + 2 == chunks:
            load_out()
        product = jnp.dot(scaled_v[...], w_v[c], preferred_element_type=F32)
        prod_v[c] = product
        send_v[c] = product.astype(BF16)

        @pl.when(me == 0)
        def _():
            message(c, "0 for 3").start()

        @pl.when(me == 1)
        def _():
            message(c, "1 to 0").start()

        @pl.when(me == 2)
        def _():
            message(c, "2 to 3").start()
            if c == 0:
                pl.semaphore_wait(go_sem, 1)
                go(3)
            message(c, "2 to 0").start()
            if c >= direct:
                message(c, "2 to 1").start()

        @pl.when(me == 3)
        def _():
            if c == direct:
                pl.semaphore_wait(go_sem, 1)
            message(c, "3 to 1" if c >= direct else "3 for 1").start()

    @pl.when(me == 0)
    def _():
        for name in ("0 for 2", "0 to 1"):
            for c in range(chunks):
                message(c, name).start()

    @pl.when(me == 3)
    def _():
        for name in ("3 to 2", "3 to 0"):
            for c in range(chunks):
                message(c, name).start()

    terms = old_terms()
    ssq_copy(0, 0, partner).wait_recv()

    @pl.when(me == 1)
    def _():
        pl.semaphore_wait(go_sem, 1)

    @pl.when(inside)
    def _():
        ssq_s[1] = ssq_v[...] + ssq_r[0]
        ssq_copy(1, 1, across).start()
        ssq_s[2] = ssq_v[...] + ssq_r[0]
        ssq_copy(2, 1, beyond).start()

    for c in range(chunks):
        @pl.when(me == 1)
        def _():
            pass_on(c, "0 for 3", "1 to 3")

        if c < direct:

            @pl.when(me == 2)
            def _():
                pass_on(c, "3 for 1", "2 to 1")

        take(c, *terms)

    @pl.when(me == 1)
    def _():
        for c in range(chunks):
            pass_on(c, "0 for 2", "1 to 2")

    for o in range(1, tp):
        cols = pl.ds(pl.multiple_of(tp_peers[o - 1] * half, half), half)
        for rows_out, into in ((w_out.at[:split, cols], wo_v), (w_out.at[split:, cols], wl_v)):
            copy = remote(
                rows_out, into.at[tp - o], wo_ssem.at[o - 1], wo_rsem.at[tp - o - 1],
                "tp", tp_peers[o - 1],
            )
            copy.start()

    ssq_copy(1, 1, partner).wait_recv()
    whole = ssq_v[...] + ssq_r[0] + ssq_r[1]
    mine_rows = rows_of(me)
    picked = lax.broadcasted_iota(jnp.int32, (own_rows, HEAD), 1) == (
        lax.broadcasted_iota(jnp.int32, (own_rows, HEAD), 0) + me * own_rows
    )
    squares = jnp.sum(jnp.where(picked, whole[:1], 0.0), axis=1, keepdims=True)
    row_scale = lax.rsqrt(squares / width + EPSILON)
    peers = [
        functools.reduce(lambda found, d: jnp.where(me == d, PEERS[d][o], found), range(kv), 0)
        for o in range(kv - 1)
    ]

    def heads_of(c, slot):
        return gath_v.at[slot, c] if c < chunks - 1 else last_v.at[slot]

    def head_copy(c, o):
        mine = heads_of(c, 0).at[mine_rows]
        return remote(mine, mine, ag_ssem, ag_rsem.at[c], "kv", peers[o])

    def cross_copy(c, o, i):
        ids = {"tp": tp_peers[o - 1]}
        if i < kv - 1:
            ids["kv"] = peers[i]
        return pltpu.make_async_remote_copy(
            src_ref=heads_of(c, 0).at[mine_rows],
            dst_ref=heads_of(c, tp - o).at[mine_rows],
            send_sem=ag_ssem,
            recv_sem=cross_rsem.at[c - crossed, tp - o - 1],
            device_id=ids,
            device_id_type=pl.DeviceIdType.MESH,
        )

    def cross_copies(c):
        return [cross_copy(c, o, i) for o in range(1, tp) for i in range(kv)]

    def forward(c, o):
        return remote(
            gath_v.at[0, c], gath_v.at[tp - o, c], fw_ssem.at[c, o - 1],
            fw_rsem.at[c, tp - o - 1], "tp", tp_peers[o - 1],
        )

    def recur(c):
        @pl.when(terms_of(c))
        def _():
            held(recv_v.at[c, :OWN], rs_rsem.at[c, 0])

        @pl.when(jnp.logical_not(terms_of(c)))
        def _():
            held(recv_v.at[c, : OWN - 1], rs_rsem.at[c, 0])

        def projected(i):
            cols = pl.ds(i * cw, cw)
            total = prod_v[c, mine_rows, cols]
            for slot in range(OWN):
                total = total + recv_v[c, slot, :, cols].astype(F32)
            return total * row_scale

        column = pl.multiple_of(tme * head_cols + c * cw, cw)
        floor_gate = lb_v[:, pl.ds(column, cw)]
        forget = floor_gate + (1.0 - floor_gate) * jax.nn.sigmoid(projected(1))
        keys = 1.0 - forget
        queries = jax.nn.silu(projected(0)) * HEAD ** (-0.5)
        values = projected(2)
        gate = jax.nn.silu(projected(3)) * hg_v[:, pl.ds(column, cw)]
        start = forget
        for lag in range(1, props):
            start = start * jnp.where(prop >= lag, pltpu.roll(forget, lag, 0), 1.0)
        reading = queries * start
        results = []
        for h in range(LINE_HEADS):
            cols = slice(h * HEAD, (h + 1) * HEAD)
            lhs = jnp.concatenate(
                [jnp.where(seq == s, reading[:, cols], 0.0) for s in range(own_seqs)], axis=1
            ).astype(BF16)
            results.append(
                jnp.dot(lhs, tkb_v[c * LINE_HEADS + h], preferred_element_type=F32)
            )
        decay = queries
        for lag in range(props):
            if lag > 0:
                decay = decay * (forget if lag == 1 else pltpu.roll(forget, lag - 1, 0))
            pair = decay * (keys if lag == 0 else pltpu.roll(keys, lag, 0))
            pair = jnp.where(prop >= lag, pair, 0.0)
            moved = values if lag == 0 else pltpu.roll(values, lag, 0)
            for h in range(LINE_HEADS):
                cols = slice(h * HEAD, (h + 1) * HEAD)
                score = jnp.sum(pair[:, cols], axis=1, keepdims=True)
                results[h] = results[h] + score * moved[:, cols]
        outs = []
        for h in range(LINE_HEADS):
            cols = slice(h * HEAD, (h + 1) * HEAD)
            r = results[h]
            normed = r * lax.rsqrt(jnp.mean(r * r, axis=1, keepdims=True) + EPSILON)
            outs.append((normed * gate[:, cols]).astype(BF16))
        heads_of(c, 0)[mine_rows, :] = jnp.concatenate(outs, axis=1)
        for o in range(kv - 1):
            head_copy(c, o).start()
        if c >= crossed:
            for copy in cross_copies(c):
                copy.start()

    def gathered(c):
        held(heads_of(c, 0).at[: (kv - 1) * own_rows], ag_rsem.at[c])

    def product_of(c, slot):
        term = jnp.dot(
            gath_v[slot, c], wo_v[slot, pl.ds(c * cw, cw), :], preferred_element_type=F32
        )
        acc_v[slot] = term if c == 0 else acc_v[slot] + term

    def from_tp(c):
        for o in range(1, tp):
            if c < crossed:
                forward(c, tp - o).wait_recv()
                continue
            held(heads_of(c, o), cross_rsem.at[c - crossed, o - 1])

    for c in range(chunks):
        recur(c)
    out_held(wo_sem)
    for o in range(1, tp):
        out_held(wo_rsem.at[o - 1])
    for c in range(chunks):
        gathered(c)
        if c < crossed:
            for o in range(1, tp):
                forward(c, o).start()
        if c < chunks - 1:
            product_of(c, 0)
        if c > 0:
            from_tp(c - 1)
            for o in range(1, tp):
                product_of(c - 1, o)
    from_tp(chunks - 1)

    held(send_v.at[:, : (kv - 1) * own_rows], rs_ssem)
    ssq_copy(0, 0, partner).wait_send()

    @pl.when(inside)
    def _():
        ssq_copy(1, 1, across).wait_send()
        ssq_copy(2, 1, beyond).wait_send()

    blocks = chunks * (kv - 1) + CROSS * (tp - 1) * kv
    held(w_v.at[0, : blocks * own_rows // 4], ag_ssem)
    for o in range(1, tp):
        out_held(wo_ssem.at[o - 1])
    for c in range(crossed):
        for o in range(1, tp):
            forward(c, o).wait_send()


def finish_line(tk_v, acc_v, last_v, wl_v, mixed, taken, mix_v, sem):
    tk_c = pltpu.make_async_copy(tk_v, taken, sem.at[0])
    tk_c.start()
    seqs, props, _ = mixed.shape
    total = 0.0
    for slot in range(acc_v.shape[0]):
        term = jnp.dot(last_v[slot], wl_v[slot], preferred_element_type=F32)
        total = total + (acc_v[slot] + term).astype(BF16).astype(F32)
    for s in range(seqs):
        mix_v[s] = total[s * props : (s + 1) * props].astype(BF16)
    mix_c = pltpu.make_async_copy(mix_v, mixed, sem.at[1])
    mix_c.start()
    mix_c.wait()
    tk_c.wait()


def finish(tk_v, own_v, peer_v, mixed, taken, mix_v, sem):
    tk_c = pltpu.make_async_copy(tk_v, taken, sem.at[0])
    tk_c.start()
    seqs, props, _ = mixed.shape
    total = own_v[...].astype(F32)
    for o in range(peer_v.shape[0]):
        total = total + peer_v[o].astype(F32)
    for s in range(seqs):
        mix_v[s] = total[s * props : (s + 1) * props].astype(BF16)
    mix_c = pltpu.make_async_copy(mix_v, mixed, sem.at[1])
    mix_c.start()
    mix_c.wait()
    tk_c.wait()


def per_device(
    kv,
    tp,
    tokens,
    w_query,
    w_forget,
    w_input,
    w_gate,
    w_out,
    gain,
    head_gain,
    lower_bound,
    state,
    last_forget,
    last_values,
    accepted,
):
    seqs, props, feat = tokens.shape
    own_seqs, heads_dev = state.shape[0], state.shape[1]
    own_rows = own_seqs * props
    rows = seqs * props
    head_cols = heads_dev * HEAD
    on_line = kv == LINE and rows <= HEAD
    per_chunk = LINE_HEADS if on_line else CHUNK_HEADS
    chunks = heads_dev // per_chunk
    cw = per_chunk * HEAD
    half = w_out.shape[1] // tp
    peers = kv - 1
    dma = pltpu.SemaphoreType.DMA
    scratch = [
        pltpu.VMEM(tokens.shape, BF16),
        pltpu.VMEM((1, gain.shape[0]), F32),
        pltpu.VMEM((1, head_gain.shape[0]), F32),
        pltpu.VMEM((1, lower_bound.shape[0]), F32),
        pltpu.VMEM(last_forget.shape, F32),
        pltpu.VMEM(last_values.shape, BF16),
        pltpu.VMEM((rows, feat), F32),
        pltpu.VMEM((rows, feat), BF16),
        pltpu.VMEM((chunks, feat, 4 * cw), BF16),
        pltpu.VMEM((tp, head_cols, half), BF16),
        pltpu.VMEM(state.shape, F32),
        pltpu.VMEM((heads_dev, own_seqs * HEAD, HEAD), BF16),
        pltpu.VMEM((own_rows, head_cols), F32),
        pltpu.VMEM((own_rows, head_cols), F32),
    ]
    if on_line:
        body, last = functools.partial(kernel_line, tp), finish_line
        scratch[9] = pltpu.VMEM((tp, head_cols - cw, half), BF16)
        outs = (
            pltpu.VMEM(state.shape, F32),
            pltpu.VMEM((tp, rows, half), F32),
            pltpu.VMEM((tp, rows, cw), BF16),
            pltpu.VMEM((tp, cw, half), BF16),
        )
        scratch += [
            pltpu.VMEM((1, HEAD), F32),
            pltpu.VMEM((3, 1, HEAD), F32),
            pltpu.VMEM((2, 1, HEAD), F32),
            pltpu.VMEM((chunks, rows, 4 * cw), F32),
            pltpu.VMEM((chunks, rows, 4 * cw), BF16),
            pltpu.VMEM((chunks, 5, own_rows, 4 * cw), BF16),
            pltpu.VMEM((tp, chunks - 1, rows, cw), BF16),
            pltpu.SMEM((own_seqs,), jnp.int32),
            dma((7,)),
            dma((chunks,)),
            dma,
            dma,
            dma((3,)),
            dma((2,)),
            dma,
            dma((chunks, 3)),
            dma,
            dma((chunks,)),
            dma((CROSS, tp - 1)),
            dma((chunks - CROSS, tp - 1)),
            dma((chunks - CROSS, tp - 1)),
            dma((tp - 1,)),
            dma((tp - 1,)),
            pltpu.SemaphoreType.REGULAR,
        ]
    else:
        body, last = functools.partial(kernel_any, kv, tp), finish
        outs = (
            pltpu.VMEM(state.shape, F32),
            pltpu.VMEM((rows, half), BF16),
            pltpu.VMEM((tp - 1, rows, half), BF16),
        )
        scratch += [
            pltpu.VMEM((rows, HEAD), F32),
            pltpu.VMEM((peers, own_rows, HEAD), F32),
            pltpu.VMEM((chunks, rows, 4 * cw), F32),
            pltpu.VMEM((chunks, rows, 4 * cw), BF16),
            pltpu.VMEM((chunks, peers, own_rows, 4 * cw), BF16),
            pltpu.VMEM((chunks, rows, cw), BF16),
            pltpu.VMEM((tp, rows, half), F32),
            pltpu.VMEM((tp - 1, rows, half), BF16),
            pltpu.VMEM((chunks, own_rows, 4 * cw), BF16),
            dma((6,)),
            dma((chunks, 4)),
            dma((tp,)),
            dma((chunks,)),
            dma((peers,)),
            dma((peers,)),
            dma((chunks, peers)),
            dma((chunks, peers)),
            dma((chunks,)),
            dma((chunks,)),
            dma((chunks, peers)),
            dma((chunks, peers)),
            dma((tp - 1,)),
            dma((tp - 1,)),
        ]
    anywhere = pl.BlockSpec(memory_space=pl.ANY)
    held = pl.BlockSpec(memory_space=pltpu.VMEM)
    results = pl.pallas_call(
        body,
        out_shape=outs,
        in_specs=[pl.BlockSpec(memory_space=pltpu.HBM)] * 12
        + [pl.BlockSpec(memory_space=pltpu.HBM if on_line else pltpu.SMEM)],
        out_specs=(held,) * len(outs),
        scratch_shapes=scratch,
        compiler_params=pltpu.CompilerParams(
            collective_id=0, has_side_effects=True, vmem_limit_bytes=VMEM_MIB * 1024 * 1024
        ),
    )(
        tokens,
        w_query,
        w_forget,
        w_input,
        w_gate,
        w_out,
        gain.reshape(1, -1),
        head_gain.reshape(1, -1),
        lower_bound.reshape(1, -1),
        state,
        last_forget,
        last_values,
        accepted,
    )
    return pl.pallas_call(
        last,
        out_shape=(
            jax.ShapeDtypeStruct((seqs, props, half), BF16),
            jax.ShapeDtypeStruct(state.shape, F32),
        ),
        in_specs=[held] * len(outs),
        out_specs=(anywhere, anywhere),
        scratch_shapes=[pltpu.VMEM((seqs, props, half), BF16), dma((2,))],
        compiler_params=pltpu.CompilerParams(vmem_limit_bytes=4 * 1024 * 1024),
    )(*results)


def solution(mesh):
    in_specs = (
        P(("grp", "dp"), None, "kv"),
        P("kv", "tp"),
        P("kv", "tp"),
        P("kv", "tp"),
        P("kv", "tp"),
        P("tp", "kv"),
        P(),
        P(),
        P(),
        P(("grp", "dp", "kv"), "tp", None, None),
        P(("grp", "dp", "kv"), None, "tp"),
        P(("grp", "dp", "kv"), None, "tp"),
        P(("grp", "dp", "kv")),
    )
    out_specs = (P(("grp", "dp"), None, ("kv", "tp")), P(("grp", "dp", "kv"), "tp", None, None))
    return jax.shard_map(
        functools.partial(per_device, mesh.shape["kv"], mesh.shape["tp"]),
        mesh=mesh,
        in_specs=in_specs,
        out_specs=out_specs,
        check_vma=False,
    )
```

```python
import functools

import jax
import jax.numpy as jnp
from jax import lax
from jax.experimental import pallas as pl
from jax.experimental.pallas import tpu as pltpu
from jax.sharding import PartitionSpec as P

HEAD = 128
EPSILON = 1e-05
CHUNK_HEADS = 4
LINE = 4
LINE_HEADS = 2
CROSS = 1
VMEM_MIB = 56
F32 = jnp.float32
BF16 = jnp.bfloat16

MESSAGES = {
    "0 for 3": (0, 1, 3, 3),
    "0 for 2": (0, 1, 2, 4),
    "0 to 1": (0, 1, 1, 0),
    "1 to 0": (1, 0, 0, 0),
    "1 to 3": (1, 3, 3, 0),
    "1 to 2": (1, 2, 2, 0),
    "2 to 3": (2, 3, 3, 1),
    "2 to 0": (2, 0, 0, 1),
    "2 to 1": (2, 1, 1, 1),
    "3 for 1": (3, 2, 1, 3),
    "3 to 1": (3, 1, 1, 2),
    "3 to 2": (3, 2, 2, 1),
    "3 to 0": (3, 0, 0, 2),
}
OWN = 3
DIRECT = 1
PEERS = ((3, 2, 1), (3, 2, 0), (0, 3, 1), (0, 1, 2))


def kernel_any(
    kv,
    tp,
    tokens,
    w_query,
    w_forget,
    w_input,
    w_gate,
    w_out,
    gain,
    head_gain,
    lower_bound,
    state,
    last_forget,
    last_values,
    accepted,
    tk_v,
    own_v,
    peer_v,
    tok_v,
    gain_v,
    hg_v,
    lb_v,
    lf_v,
    lv_v,
    rows_v,
    scaled_v,
    w_v,
    wo_v,
    st_v,
    tkb_v,
    lfr_v,
    lvr_v,
    ssq_v,
    ssq_r,
    prod_v,
    send_v,
    recv_v,
    gath_v,
    acc_v,
    part_v,
    relay_v,
    load_sem,
    w_sem,
    wo_sem,
    st_sem,
    ssq_ssem,
    ssq_rsem,
    rs_ssem,
    rs_rsem,
    relay_ssem,
    relay_rsem,
    ag_ssem,
    ag_rsem,
    tp_ssem,
    tp_rsem,
):
    me = lax.axis_index("kv")
    tme = lax.axis_index("tp")
    seqs, props, feat = tokens.shape
    own_seqs, heads_dev = state.shape[0], state.shape[1]
    own_rows = own_seqs * props
    rows = seqs * props
    width = gain.shape[1]
    head_cols = heads_dev * HEAD
    chunks = heads_dev // CHUNK_HEADS
    cw = CHUNK_HEADS * HEAD
    half = w_out.shape[1] // tp
    weights = (w_query, w_forget, w_input, w_gate)

    def local(src, dst, sem):
        copy = pltpu.make_async_copy(src, dst, sem)
        copy.start()
        return copy

    tok_c = local(tokens, tok_v, load_sem.at[0])
    gain_c = local(gain, gain_v, load_sem.at[1])

    def load_w(c):
        return [
            local(w.at[:, pl.ds(c * cw, cw)], w_v.at[c, :, pl.ds(i * cw, cw)], w_sem.at[c, i])
            for i, w in enumerate(weights)
        ]

    def load_state(c):
        hs = pl.ds(c * CHUNK_HEADS, CHUNK_HEADS)
        return local(state.at[:, hs], st_v.at[:, hs], st_sem.at[c])

    w_c = [load_w(0)]
    small_c = [
        local(last_forget, lf_v, load_sem.at[2]),
        local(last_values, lv_v, load_sem.at[3]),
        local(head_gain, hg_v, load_sem.at[4]),
        local(lower_bound, lb_v, load_sem.at[5]),
    ]
    st_c = []
    for c in range(chunks):
        st_c.append(load_state(c))
        if c + 1 < chunks:
            w_c.append(load_w(c + 1))
    wo_c = []
    for o in range(tp):
        column = pl.multiple_of(lax.rem(tme + o, tp) * half, half)
        wo_c.append(local(w_out.at[:, pl.ds(column, half)], wo_v.at[o], wo_sem.at[o]))

    barrier = pltpu.get_barrier_semaphore()
    kv_peers = [lax.rem(me + o, kv) for o in range(1, kv)]
    tp_peers = [lax.rem(tme + o, tp) for o in range(1, tp)]
    for peer in kv_peers:
        pl.semaphore_signal(barrier, inc=1, device_id={"kv": peer}, device_id_type=pl.DeviceIdType.MESH)
    for peer in tp_peers:
        pl.semaphore_signal(barrier, inc=1, device_id={"tp": peer}, device_id_type=pl.DeviceIdType.MESH)

    def remote(src, dst, ssem, rsem, axis, peer):
        copy = pltpu.make_async_remote_copy(
            src_ref=src,
            dst_ref=dst,
            send_sem=ssem,
            recv_sem=rsem,
            device_id={axis: peer},
            device_id_type=pl.DeviceIdType.MESH,
        )
        copy.start()
        return copy

    tok_c.wait()
    gain_c.wait()
    for s in range(seqs):
        rows_v[pl.ds(s * props, props), :] = tok_v[s].astype(F32)
    x = rows_v[...]
    my_gain = gain_v[:, pl.ds(pl.multiple_of(me * feat, feat), feat)]
    scaled_v[...] = (x * my_gain).astype(BF16)
    ssq_v[...] = jnp.broadcast_to(jnp.sum(x * x, axis=1, keepdims=True), (rows, HEAD))

    pl.semaphore_wait(barrier, kv - 1 + tp - 1)

    def rows_of(device):
        return pl.ds(pl.multiple_of(device * own_rows, own_rows), own_rows)

    ssq_c = [
        remote(
            ssq_v.at[rows_of(peer)], ssq_r.at[o], ssq_ssem.at[o], ssq_rsem.at[o], "kv", peer
        )
        for o, peer in enumerate(kv_peers)
    ]

    place = lax.broadcasted_iota(jnp.int32, (own_rows, 1), 0)
    prop = lax.rem(place, props)
    seq = place // props

    def old_terms():
        for copy in small_c:
            copy.wait()
        for s in range(own_seqs):
            lfr_v[pl.ds(s * props, props), :] = lf_v[s]
            lvr_v[pl.ds(s * props, props), :] = lv_v[s].astype(F32)
        limit = jnp.zeros((own_rows, 1), jnp.int32)
        for s in range(own_seqs):
            limit = jnp.where(seq == s, accepted[s], limit)
        mask = prop < limit
        old = lfr_v[...]
        decay = jnp.where(mask, old, 1.0)
        weight = jnp.where(mask, 1.0 - old, 0.0)
        after = jnp.ones_like(decay)
        for lag in range(1, props):
            after = after * jnp.where(
                prop < props - lag, pltpu.roll(decay, own_rows - lag, 0), 1.0
            )
        return decay * after, weight * after, lvr_v[...].astype(BF16)

    def take(c, ends, old_weight, old_values):
        st_c[c].wait()
        lane_seq = lax.broadcasted_iota(jnp.int32, (1, own_rows), 1) // props
        for h in range(c * CHUNK_HEADS, (c + 1) * CHUNK_HEADS):
            cols = slice(h * HEAD, (h + 1) * HEAD)
            end_t = ends[:, cols].T
            weight_t = old_weight[:, cols].T
            for s in range(own_seqs):
                mine = jnp.where(lane_seq == s, weight_t, 0.0).astype(BF16)
                added = jnp.dot(mine, old_values[:, cols], preferred_element_type=F32)
                new = end_t[:, s * props : s * props + 1] * st_v[s, h] + added
                tk_v[s, h] = new
                tkb_v[h, pl.ds(s * HEAD, HEAD), :] = new.astype(BF16)

    relayed = kv == 4
    at_end = jnp.logical_or(me == 0, me == kv - 1)
    first = me == 0
    last = me == kv - 1
    if relayed:

        @pl.when(last)
        def _():
            recv_v[:, kv - 2] = jnp.zeros_like(recv_v[:, kv - 2])

        @pl.when(first)
        def _():
            recv_v[:, 0] = jnp.zeros_like(recv_v[:, 0])

    def rs_copy(c, o):
        return pltpu.make_async_remote_copy(
            src_ref=send_v.at[c, rows_of(kv_peers[o])],
            dst_ref=recv_v.at[c, o],
            send_sem=rs_ssem.at[c, o],
            recv_sem=rs_rsem.at[c, o],
            device_id={"kv": kv_peers[o]},
            device_id_type=pl.DeviceIdType.MESH,
        )

    def relay_copy(c, end):
        far, near = (kv - 1, 1) if end == 0 else (0, kv - 2)
        return pltpu.make_async_remote_copy(
            src_ref=send_v.at[c, rows_of(far)],
            dst_ref=relay_v.at[c],
            send_sem=relay_ssem.at[c],
            recv_sem=relay_rsem.at[c],
            device_id={"kv": near},
            device_id_type=pl.DeviceIdType.MESH,
        )

    def send_blocks(c):
        if not relayed:
            for o in range(kv - 1):
                rs_copy(c, o).start()
            return

        @pl.when(first)
        def _():
            relay_copy(c, 0).start()
            rs_copy(c, 1).start()
            if c > 0:
                rs_copy(c - 1, 0).start()
            if c == chunks - 1:
                rs_copy(c, 0).start()

        @pl.when(last)
        def _():
            relay_copy(c, kv - 1).start()
            rs_copy(c, 1).start()
            if c > 0:
                rs_copy(c - 1, 2).start()
            if c == chunks - 1:
                rs_copy(c, 2).start()

        @pl.when(jnp.logical_not(at_end))
        def _():
            rs_copy(c, 0).start()
            rs_copy(c, 2).start()

    def send_on(c):
        if relayed:

            @pl.when(jnp.logical_not(at_end))
            def _():
                relay_copy(c, 0).wait_recv()
                far = rows_of(kv_peers[1])
                send_v[c, far, :] = (prod_v[c, far, :] + relay_v[c].astype(F32)).astype(BF16)
                rs_copy(c, 1).start()

    def wait_blocks(c):
        for o in range(kv - 1):
            if relayed and o == 0:
                pl.when(jnp.logical_not(first))(lambda o=o: rs_copy(c, o).wait_recv())
            elif relayed and o == kv - 2:
                pl.when(jnp.logical_not(last))(lambda o=o: rs_copy(c, o).wait_recv())
            else:
                rs_copy(c, o).wait_recv()

    def wait_sent(c):
        if not relayed:
            for o in range(kv - 1):
                rs_copy(c, o).wait_send()
            return
        rs_copy(c, 1).wait_send()

        @pl.when(first)
        def _():
            relay_copy(c, 0).wait_send()
            rs_copy(c, 0).wait_send()

        @pl.when(last)
        def _():
            relay_copy(c, kv - 1).wait_send()
            rs_copy(c, 2).wait_send()

        @pl.when(jnp.logical_not(at_end))
        def _():
            rs_copy(c, 0).wait_send()
            rs_copy(c, 2).wait_send()

    terms = None
    for c in range(chunks):
        for copy in w_c[c]:
            copy.wait()
        product = jnp.dot(scaled_v[...], w_v[c], preferred_element_type=F32)
        prod_v[c] = product
        send_v[c] = product.astype(BF16)
        send_blocks(c)
        if terms is None:
            terms = old_terms()
        if c > 0:
            send_on(c - 1)
        take(c, *terms)
    send_on(chunks - 1)

    squares = ssq_v[rows_of(me), :]
    for o in range(kv - 1):
        ssq_c[o].wait_recv()
        squares = squares + ssq_r[o]
    row_scale = lax.rsqrt(squares[:, :1] / width + EPSILON)
    mine_rows = rows_of(me)
    ag_c = []

    def recur(c):
        wait_blocks(c)

        def projected(i):
            total = prod_v[c, mine_rows, pl.ds(i * cw, cw)]
            for o in range(kv - 1):
                total = total + recv_v[c, o, :, pl.ds(i * cw, cw)].astype(F32)
            return total * row_scale

        column = pl.multiple_of(tme * head_cols + c * cw, cw)
        floor_gate = lb_v[:, pl.ds(column, cw)]
        forget = floor_gate + (1.0 - floor_gate) * jax.nn.sigmoid(projected(1))
        keys = 1.0 - forget
        queries = jax.nn.silu(projected(0)) * HEAD ** (-0.5)
        values = projected(2)
        gate = jax.nn.silu(projected(3)) * hg_v[:, pl.ds(column, cw)]
        start = forget
        for lag in range(1, props):
            start = start * jnp.where(prop >= lag, pltpu.roll(forget, lag, 0), 1.0)
        reading = queries * start
        results = []
        for h in range(CHUNK_HEADS):
            cols = slice(h * HEAD, (h + 1) * HEAD)
            lhs = jnp.concatenate(
                [jnp.where(seq == s, reading[:, cols], 0.0) for s in range(own_seqs)], axis=1
            ).astype(BF16)
            results.append(
                jnp.dot(lhs, tkb_v[c * CHUNK_HEADS + h], preferred_element_type=F32)
            )
        decay = queries
        for lag in range(props):
            if lag > 0:
                decay = decay * (forget if lag == 1 else pltpu.roll(forget, lag - 1, 0))
            pair = decay * (keys if lag == 0 else pltpu.roll(keys, lag, 0))
            pair = jnp.where(prop >= lag, pair, 0.0)
            moved = values if lag == 0 else pltpu.roll(values, lag, 0)
            for h in range(CHUNK_HEADS):
                cols = slice(h * HEAD, (h + 1) * HEAD)
                score = jnp.sum(pair[:, cols], axis=1, keepdims=True)
                results[h] = results[h] + score * moved[:, cols]
        outs = []
        for h in range(CHUNK_HEADS):
            cols = slice(h * HEAD, (h + 1) * HEAD)
            r = results[h]
            normed = r * lax.rsqrt(jnp.mean(r * r, axis=1, keepdims=True) + EPSILON)
            outs.append((normed * gate[:, cols]).astype(BF16))
        gath_v[c, mine_rows, :] = jnp.concatenate(outs, axis=1)
        ag_c.append(
            [
                remote(
                    gath_v.at[c, mine_rows],
                    gath_v.at[c, mine_rows],
                    ag_ssem.at[c, o],
                    ag_rsem.at[c, o],
                    "kv",
                    peer,
                )
                for o, peer in enumerate(kv_peers)
            ]
        )

    def product_of(c, o):
        term = jnp.dot(
            gath_v[c], wo_v[o, pl.ds(c * cw, cw), :], preferred_element_type=F32
        )
        return term if c == 0 else acc_v[o] + term

    def gathered(c):
        for o in range(kv - 1):
            ag_c[c][o].wait_recv()

    for c in range(chunks):
        recur(c)
    for copy in wo_c:
        copy.wait()
    for c in range(chunks - 1):
        gathered(c)
        for o in range(tp):
            acc_v[o] = product_of(c, o)
    gathered(chunks - 1)
    tp_c = []
    for o in range(1, tp):
        part_v[o - 1] = product_of(chunks - 1, o).astype(BF16)
        tp_c.append(
            remote(
                part_v.at[o - 1],
                peer_v.at[o - 1],
                tp_ssem.at[o - 1],
                tp_rsem.at[o - 1],
                "tp",
                tp_peers[o - 1],
            )
        )
    own_v[...] = product_of(chunks - 1, 0).astype(BF16)
    for copy in tp_c:
        copy.wait_recv()
    for c in range(chunks):
        wait_sent(c)
    for copies in [ssq_c, *ag_c, tp_c]:
        for copy in copies:
            copy.wait_send()


def kernel_line(
    tp,
    tokens,
    w_query,
    w_forget,
    w_input,
    w_gate,
    w_out,
    gain,
    head_gain,
    lower_bound,
    state,
    last_forget,
    last_values,
    accepted,
    tk_v,
    acc_v,
    last_v,
    wl_v,
    tok_v,
    gain_v,
    hg_v,
    lb_v,
    lf_v,
    lv_v,
    rows_v,
    scaled_v,
    w_v,
    wo_v,
    st_v,
    tkb_v,
    lfr_v,
    lvr_v,
    ssq_v,
    ssq_s,
    ssq_r,
    prod_v,
    send_v,
    recv_v,
    gath_v,
    acc_s,
    load_sem,
    w_sem,
    wo_sem,
    st_sem,
    ssq_ssem,
    ssq_rsem,
    rs_ssem,
    rs_rsem,
    ag_ssem,
    ag_rsem,
    cross_rsem,
    fw_ssem,
    fw_rsem,
    wo_ssem,
    wo_rsem,
    go_sem,
):
    kv = LINE
    me = lax.axis_index("kv")
    tme = lax.axis_index("tp")
    seqs, props, feat = tokens.shape
    own_seqs, heads_dev = state.shape[0], state.shape[1]
    own_rows = own_seqs * props
    rows = seqs * props
    width = gain.shape[1]
    head_cols = heads_dev * HEAD
    chunks = heads_dev // LINE_HEADS
    cw = LINE_HEADS * HEAD
    half = w_out.shape[1] // tp
    weights = (w_query, w_forget, w_input, w_gate)

    at_end = jnp.logical_or(me == 0, me == kv - 1)

    def local(src, dst, sem):
        copy = pltpu.make_async_copy(src, dst, sem)
        copy.start()
        return copy

    tok_c = local(tokens, tok_v, load_sem.at[0])
    gain_c = local(gain, gain_v, load_sem.at[1])

    def held(ref, sem):
        pltpu.make_async_copy(ref, ref, sem).wait()

    def load_w(c):
        for i, w in enumerate(weights):
            local(w.at[:, pl.ds(c * cw, cw)], w_v.at[c, :, pl.ds(i * cw, cw)], w_sem.at[c])

    def load_late():
        small = [
            local(last_forget, lf_v, load_sem.at[2]),
            local(last_values, lv_v, load_sem.at[3]),
            local(head_gain, hg_v, load_sem.at[4]),
            local(lower_bound, lb_v, load_sem.at[5]),
            local(accepted, acc_s, load_sem.at[6]),
        ]
        return small, local(state, st_v, st_sem)

    split = (chunks - 1) * cw
    crossed = chunks - CROSS

    def load_out():
        cols = pl.ds(pl.multiple_of(tme * half, half), half)
        local(w_out.at[:split, cols], wo_v.at[0], wo_sem)
        local(w_out.at[split:, cols], wl_v.at[0], wo_sem)

    def out_held(sem):
        held(w_v.at[0, : head_cols * half // (4 * cw)], sem)

    load_w(0)

    def signal(axis, peer):
        pl.semaphore_signal(
            barrier, inc=1, device_id={axis: peer}, device_id_type=pl.DeviceIdType.MESH
        )

    barrier = pltpu.get_barrier_semaphore()
    tp_peers = [lax.rem(tme + o, tp) for o in range(1, tp)]
    for peer in tp_peers:
        signal("tp", peer)

    @pl.when(me > 0)
    def _():
        signal("kv", me - 1)

    @pl.when(me < kv - 1)
    def _():
        signal("kv", me + 1)

    def remote(src, dst, ssem, rsem, axis, peer):
        return pltpu.make_async_remote_copy(
            src_ref=src,
            dst_ref=dst,
            send_sem=ssem,
            recv_sem=rsem,
            device_id={axis: peer},
            device_id_type=pl.DeviceIdType.MESH,
        )

    gain_c.wait()
    load_w(1)
    tok_c.wait()
    load_w(2)
    for s in range(seqs):
        rows_v[pl.ds(s * props, props), :] = tok_v[s].astype(F32)
    x = rows_v[...]
    my_gain = gain_v[:, pl.ds(pl.multiple_of(me * feat, feat), feat)]
    scaled_v[...] = (x * my_gain).astype(BF16)

    def rows_of(device):
        return pl.ds(pl.multiple_of(device * own_rows, own_rows), own_rows)

    def message(c, name):
        _, to, dest, slot = MESSAGES[name]
        return remote(
            send_v.at[c, rows_of(dest)],
            recv_v.at[c, slot],
            rs_ssem,
            rs_rsem.at[c, max(slot - OWN + 1, 0)],
            "kv",
            to,
        )

    def pass_on(c, name, onward):
        _, _, dest, slot = MESSAGES[name]
        message(c, name).wait_recv()
        into = rows_of(dest)
        send_v[c, into, :] = (prod_v[c, into, :] + recv_v[c, slot].astype(F32)).astype(BF16)
        message(c, onward).start()

    def ssq_copy(i, slot, to):
        return remote(ssq_s.at[i], ssq_r.at[slot], ssq_ssem.at[i], ssq_rsem.at[slot], "kv", to)

    partner = me + 1 - 2 * lax.rem(me, 2)
    across = jnp.where(me == 1, 2, 1)
    beyond = jnp.where(me == 1, 3, 0)
    inside = jnp.logical_not(at_end)
    pl.semaphore_wait(barrier, jnp.where(at_end, tp, tp + 1))
    def go(to):
        pl.semaphore_signal(
            go_sem, inc=1, device_id={"kv": to}, device_id_type=pl.DeviceIdType.MESH
        )

    @pl.when(inside)
    def _():
        go(across)

    direct = chunks - DIRECT

    def terms_of(c):
        return (me == 0) if c < direct else (me < 2)


    place = lax.broadcasted_iota(jnp.int32, (own_rows, 1), 0)
    prop = lax.rem(place, props)
    seq = place // props

    def old_terms():
        for copy in small_c:
            copy.wait()
        for s in range(own_seqs):
            lfr_v[pl.ds(s * props, props), :] = lf_v[s]
            lvr_v[pl.ds(s * props, props), :] = lv_v[s].astype(F32)
        limit = jnp.zeros((own_rows, 1), jnp.int32)
        for s in range(own_seqs):
            limit = jnp.where(seq == s, acc_s[s], limit)
        mask = prop < limit
        old = lfr_v[...]
        decay = jnp.where(mask, old, 1.0)
        weight = jnp.where(mask, 1.0 - old, 0.0)
        after = jnp.ones_like(decay)
        for lag in range(1, props):
            after = after * jnp.where(
                prop < props - lag, pltpu.roll(decay, own_rows - lag, 0), 1.0
            )
        return decay * after, weight * after, lvr_v[...].astype(BF16)

    def take(c, ends, old_weight, old_values):
        if c == 0:
            st_c.wait()
        lane_seq = lax.broadcasted_iota(jnp.int32, (1, own_rows), 1) // props
        for h in range(c * LINE_HEADS, (c + 1) * LINE_HEADS):
            cols = slice(h * HEAD, (h + 1) * HEAD)
            end_t = ends[:, cols].T
            weight_t = old_weight[:, cols].T
            for s in range(own_seqs):
                mine = jnp.where(lane_seq == s, weight_t, 0.0).astype(BF16)
                added = jnp.dot(mine, old_values[:, cols], preferred_element_type=F32)
                new = end_t[:, s * props : s * props + 1] * st_v[s, h] + added
                tk_v[s, h] = new
                tkb_v[h, pl.ds(s * HEAD, HEAD), :] = new.astype(BF16)

    for c in range(chunks):
        held(w_v.at[c], w_sem.at[c])
        if c + 3 < chunks:
            load_w(c + 3)
        elif c + 3 == chunks:
            small_c, st_c = load_late()
        elif c + 2 == chunks:
            load_out()
        product = jnp.dot(scaled_v[...], w_v[c], preferred_element_type=F32)
        prod_v[c] = product
        send_v[c] = product.astype(BF16)

        @pl.when(me == 0)
        def _():
            message(c, "0 for 3").start()

        @pl.when(me == 1)
        def _():
            message(c, "1 to 0").start()

        @pl.when(me == 2)
        def _():
            message(c, "2 to 3").start()
            if c == 0:
                pl.semaphore_wait(go_sem, 1)
                go(3)
            message(c, "2 to 0").start()
            if c >= direct:
                message(c, "2 to 1").start()

        @pl.when(me == 3)
        def _():
            if c == direct:
                pl.semaphore_wait(go_sem, 1)
            message(c, "3 to 1" if c >= direct else "3 for 1").start()

        if c == 0:
            x = rows_v[...]
            squared = jnp.sum(x * x, axis=1, keepdims=True)
            on_row = lax.broadcasted_iota(jnp.int32, (rows, HEAD), 0)
            on_lane = lax.broadcasted_iota(jnp.int32, (rows, HEAD), 1)
            along = jnp.sum(jnp.where(on_row == on_lane, squared, 0.0), axis=0, keepdims=True)
            ssq_v[...] = along
            ssq_s[0] = along
            ssq_copy(0, 0, partner).start()

    @pl.when(me == 0)
    def _():
        for name in ("0 for 2", "0 to 1"):
            for c in range(chunks):
                message(c, name).start()

    @pl.when(me == 3)
    def _():
        for name in ("3 to 2", "3 to 0"):
            for c in range(chunks):
                message(c, name).start()

    for c in range(chunks):

        @pl.when(jnp.logical_not(terms_of(c)))
        def _():
            recv_v[c, OWN - 1] = jnp.zeros_like(recv_v[c, OWN - 1])

    terms = old_terms()
    ssq_copy(0, 0, partner).wait_recv()

    @pl.when(me == 1)
    def _():
        pl.semaphore_wait(go_sem, 1)

    @pl.when(inside)
    def _():
        ssq_s[1] = ssq_v[...] + ssq_r[0]
        ssq_copy(1, 1, across).start()
        ssq_s[2] = ssq_v[...] + ssq_r[0]
        ssq_copy(2, 1, beyond).start()

    for c in range(chunks):
        @pl.when(me == 1)
        def _():
            pass_on(c, "0 for 3", "1 to 3")

        if c < direct:

            @pl.when(me == 2)
            def _():
                pass_on(c, "3 for 1", "2 to 1")

        take(c, *terms)

    @pl.when(me == 1)
    def _():
        for c in range(chunks):
            pass_on(c, "0 for 2", "1 to 2")

    for o in range(1, tp):
        cols = pl.ds(pl.multiple_of(tp_peers[o - 1] * half, half), half)
        for rows_out, into in ((w_out.at[:split, cols], wo_v), (w_out.at[split:, cols], wl_v)):
            copy = remote(
                rows_out, into.at[tp - o], wo_ssem.at[o - 1], wo_rsem.at[tp - o - 1],
                "tp", tp_peers[o - 1],
            )
            copy.start()

    ssq_copy(1, 1, partner).wait_recv()
    whole = ssq_v[...] + ssq_r[0] + ssq_r[1]
    mine_rows = rows_of(me)
    picked = lax.broadcasted_iota(jnp.int32, (own_rows, HEAD), 1) == (
        lax.broadcasted_iota(jnp.int32, (own_rows, HEAD), 0) + me * own_rows
    )
    squares = jnp.sum(jnp.where(picked, whole[:1], 0.0), axis=1, keepdims=True)
    row_scale = lax.rsqrt(squares / width + EPSILON)
    peers = [
        functools.reduce(lambda found, d: jnp.where(me == d, PEERS[d][o], found), range(kv), 0)
        for o in range(kv - 1)
    ]

    def heads_of(c, slot):
        return gath_v.at[slot, c] if c < chunks - 1 else last_v.at[slot]

    def head_copy(c, o):
        mine = heads_of(c, 0).at[mine_rows]
        return remote(mine, mine, ag_ssem, ag_rsem.at[c], "kv", peers[o])

    def cross_copy(c, o, i):
        ids = {"tp": tp_peers[o - 1]}
        if i < kv - 1:
            ids["kv"] = peers[i]
        return pltpu.make_async_remote_copy(
            src_ref=heads_of(c, 0).at[mine_rows],
            dst_ref=heads_of(c, tp - o).at[mine_rows],
            send_sem=ag_ssem,
            recv_sem=cross_rsem.at[c - crossed, tp - o - 1],
            device_id=ids,
            device_id_type=pl.DeviceIdType.MESH,
        )

    def cross_copies(c):
        return [cross_copy(c, o, i) for o in range(1, tp) for i in range(kv)]

    def forward(c, o):
        return remote(
            gath_v.at[0, c], gath_v.at[tp - o, c], fw_ssem.at[c, o - 1],
            fw_rsem.at[c, tp - o - 1], "tp", tp_peers[o - 1],
        )

    def send_heads(c, o):
        if o < kv - 1:
            head_copy(c, o).start()
        if c >= crossed:
            for away in range(1, tp):
                cross_copy(c, away, o).start()

    def recur(c):
        @pl.when(terms_of(c))
        def _():
            held(recv_v.at[c, :OWN], rs_rsem.at[c, 0])

        @pl.when(jnp.logical_not(terms_of(c)))
        def _():
            held(recv_v.at[c, : OWN - 1], rs_rsem.at[c, 0])

        def projected(i):
            cols = pl.ds(i * cw, cw)
            total = prod_v[c, mine_rows, cols]
            for slot in range(OWN):
                total = total + recv_v[c, slot, :, cols].astype(F32)
            return total * row_scale

        column = pl.multiple_of(tme * head_cols + c * cw, cw)
        floor_gate = lb_v[:, pl.ds(column, cw)]
        forget = floor_gate + (1.0 - floor_gate) * jax.nn.sigmoid(projected(1))
        keys = 1.0 - forget
        queries = jax.nn.silu(projected(0)) * HEAD ** (-0.5)
        values = projected(2)
        gate = jax.nn.silu(projected(3)) * hg_v[:, pl.ds(column, cw)]
        start = forget
        for lag in range(1, props):
            start = start * jnp.where(prop >= lag, pltpu.roll(forget, lag, 0), 1.0)
        reading = queries * start
        results = []
        for h in range(LINE_HEADS):
            cols = slice(h * HEAD, (h + 1) * HEAD)
            lhs = jnp.concatenate(
                [jnp.where(seq == s, reading[:, cols], 0.0) for s in range(own_seqs)], axis=1
            ).astype(BF16)
            results.append(
                jnp.dot(lhs, tkb_v[c * LINE_HEADS + h], preferred_element_type=F32)
            )
        decay = queries
        for lag in range(props):
            if lag > 0:
                decay = decay * (forget if lag == 1 else pltpu.roll(forget, lag - 1, 0))
            pair = decay * (keys if lag == 0 else pltpu.roll(keys, lag, 0))
            pair = jnp.where(prop >= lag, pair, 0.0)
            moved = values if lag == 0 else pltpu.roll(values, lag, 0)
            for h in range(LINE_HEADS):
                cols = slice(h * HEAD, (h + 1) * HEAD)
                score = jnp.sum(pair[:, cols], axis=1, keepdims=True)
                results[h] = results[h] + score * moved[:, cols]
        outs = []
        for h in range(LINE_HEADS):
            cols = slice(h * HEAD, (h + 1) * HEAD)
            r = results[h]
            normed = r * lax.rsqrt(jnp.mean(r * r, axis=1, keepdims=True) + EPSILON)
            outs.append((normed * gate[:, cols]).astype(BF16))
        heads_of(c, 0)[mine_rows, :] = jnp.concatenate(outs, axis=1)
        for o in (0, 1, kv - 1):
            send_heads(c, o)

        @pl.when(me != 2)
        def _():
            send_heads(c, 2)

    def gathered(c):
        held(heads_of(c, 0).at[: (kv - 1) * own_rows], ag_rsem.at[c])

    def product_of(c, slot):
        term = jnp.dot(
            gath_v[slot, c], wo_v[slot, pl.ds(c * cw, cw), :], preferred_element_type=F32
        )
        acc_v[slot] = term if c == 0 else acc_v[slot] + term

    def from_tp(c):
        for o in range(1, tp):
            if c < crossed:
                forward(c, tp - o).wait_recv()
                continue
            held(heads_of(c, o), cross_rsem.at[c - crossed, o - 1])

    for c in range(chunks):
        recur(c)

    @pl.when(me == 2)
    def _():
        for c in range(chunks):
            send_heads(c, 2)

    out_held(wo_sem)
    for o in range(1, tp):
        out_held(wo_rsem.at[o - 1])
    for c in range(chunks):
        gathered(c)
        if c < crossed:
            for o in range(1, tp):
                forward(c, o).start()
        if c < chunks - 1:
            product_of(c, 0)
        if c > 0:
            from_tp(c - 1)
            for o in range(1, tp):
                product_of(c - 1, o)
    from_tp(chunks - 1)

    held(send_v.at[:, : (kv - 1) * own_rows], rs_ssem)
    ssq_copy(0, 0, partner).wait_send()

    @pl.when(inside)
    def _():
        ssq_copy(1, 1, across).wait_send()
        ssq_copy(2, 1, beyond).wait_send()

    blocks = chunks * (kv - 1) + CROSS * (tp - 1) * kv
    held(w_v.at[0, : blocks * own_rows // 4], ag_ssem)
    for o in range(1, tp):
        out_held(wo_ssem.at[o - 1])
    for c in range(crossed):
        for o in range(1, tp):
            forward(c, o).wait_send()


def finish_line(tk_v, acc_v, last_v, wl_v, mixed, taken, mix_v, sem):
    tk_c = pltpu.make_async_copy(tk_v, taken, sem.at[0])
    tk_c.start()
    seqs, props, _ = mixed.shape
    total = 0.0
    for slot in range(acc_v.shape[0]):
        term = jnp.dot(last_v[slot], wl_v[slot], preferred_element_type=F32)
        total = total + (acc_v[slot] + term).astype(BF16).astype(F32)
    for s in range(seqs):
        mix_v[s] = total[s * props : (s + 1) * props].astype(BF16)
    mix_c = pltpu.make_async_copy(mix_v, mixed, sem.at[1])
    mix_c.start()
    mix_c.wait()
    tk_c.wait()


def finish(tk_v, own_v, peer_v, mixed, taken, mix_v, sem):
    tk_c = pltpu.make_async_copy(tk_v, taken, sem.at[0])
    tk_c.start()
    seqs, props, _ = mixed.shape
    total = own_v[...].astype(F32)
    for o in range(peer_v.shape[0]):
        total = total + peer_v[o].astype(F32)
    for s in range(seqs):
        mix_v[s] = total[s * props : (s + 1) * props].astype(BF16)
    mix_c = pltpu.make_async_copy(mix_v, mixed, sem.at[1])
    mix_c.start()
    mix_c.wait()
    tk_c.wait()


def per_device(
    kv,
    tp,
    tokens,
    w_query,
    w_forget,
    w_input,
    w_gate,
    w_out,
    gain,
    head_gain,
    lower_bound,
    state,
    last_forget,
    last_values,
    accepted,
):
    seqs, props, feat = tokens.shape
    own_seqs, heads_dev = state.shape[0], state.shape[1]
    own_rows = own_seqs * props
    rows = seqs * props
    head_cols = heads_dev * HEAD
    on_line = kv == LINE and rows <= HEAD
    per_chunk = LINE_HEADS if on_line else CHUNK_HEADS
    chunks = heads_dev // per_chunk
    cw = per_chunk * HEAD
    half = w_out.shape[1] // tp
    peers = kv - 1
    dma = pltpu.SemaphoreType.DMA
    scratch = [
        pltpu.VMEM(tokens.shape, BF16),
        pltpu.VMEM((1, gain.shape[0]), F32),
        pltpu.VMEM((1, head_gain.shape[0]), F32),
        pltpu.VMEM((1, lower_bound.shape[0]), F32),
        pltpu.VMEM(last_forget.shape, F32),
        pltpu.VMEM(last_values.shape, BF16),
        pltpu.VMEM((rows, feat), F32),
        pltpu.VMEM((rows, feat), BF16),
        pltpu.VMEM((chunks, feat, 4 * cw), BF16),
        pltpu.VMEM((tp, head_cols, half), BF16),
        pltpu.VMEM(state.shape, F32),
        pltpu.VMEM((heads_dev, own_seqs * HEAD, HEAD), BF16),
        pltpu.VMEM((own_rows, head_cols), F32),
        pltpu.VMEM((own_rows, head_cols), F32),
    ]
    if on_line:
        body, last = functools.partial(kernel_line, tp), finish_line
        scratch[9] = pltpu.VMEM((tp, head_cols - cw, half), BF16)
        outs = (
            pltpu.VMEM(state.shape, F32),
            pltpu.VMEM((tp, rows, half), F32),
            pltpu.VMEM((tp, rows, cw), BF16),
            pltpu.VMEM((tp, cw, half), BF16),
        )
        scratch += [
            pltpu.VMEM((1, HEAD), F32),
            pltpu.VMEM((3, 1, HEAD), F32),
            pltpu.VMEM((2, 1, HEAD), F32),
            pltpu.VMEM((chunks, rows, 4 * cw), F32),
            pltpu.VMEM((chunks, rows, 4 * cw), BF16),
            pltpu.VMEM((chunks, 5, own_rows, 4 * cw), BF16),
            pltpu.VMEM((tp, chunks - 1, rows, cw), BF16),
            pltpu.SMEM((own_seqs,), jnp.int32),
            dma((7,)),
            dma((chunks,)),
            dma,
            dma,
            dma((3,)),
            dma((2,)),
            dma,
            dma((chunks, 3)),
            dma,
            dma((chunks,)),
            dma((CROSS, tp - 1)),
            dma((chunks - CROSS, tp - 1)),
            dma((chunks - CROSS, tp - 1)),
            dma((tp - 1,)),
            dma((tp - 1,)),
            pltpu.SemaphoreType.REGULAR,
        ]
    else:
        body, last = functools.partial(kernel_any, kv, tp), finish
        outs = (
            pltpu.VMEM(state.shape, F32),
            pltpu.VMEM((rows, half), BF16),
            pltpu.VMEM((tp - 1, rows, half), BF16),
        )
        scratch += [
            pltpu.VMEM((rows, HEAD), F32),
            pltpu.VMEM((peers, own_rows, HEAD), F32),
            pltpu.VMEM((chunks, rows, 4 * cw), F32),
            pltpu.VMEM((chunks, rows, 4 * cw), BF16),
            pltpu.VMEM((chunks, peers, own_rows, 4 * cw), BF16),
            pltpu.VMEM((chunks, rows, cw), BF16),
            pltpu.VMEM((tp, rows, half), F32),
            pltpu.VMEM((tp - 1, rows, half), BF16),
            pltpu.VMEM((chunks, own_rows, 4 * cw), BF16),
            dma((6,)),
            dma((chunks, 4)),
            dma((tp,)),
            dma((chunks,)),
            dma((peers,)),
            dma((peers,)),
            dma((chunks, peers)),
            dma((chunks, peers)),
            dma((chunks,)),
            dma((chunks,)),
            dma((chunks, peers)),
            dma((chunks, peers)),
            dma((tp - 1,)),
            dma((tp - 1,)),
        ]
    anywhere = pl.BlockSpec(memory_space=pl.ANY)
    held = pl.BlockSpec(memory_space=pltpu.VMEM)
    results = pl.pallas_call(
        body,
        out_shape=outs,
        in_specs=[pl.BlockSpec(memory_space=pltpu.HBM)] * 12
        + [pl.BlockSpec(memory_space=pltpu.HBM if on_line else pltpu.SMEM)],
        out_specs=(held,) * len(outs),
        scratch_shapes=scratch,
        compiler_params=pltpu.CompilerParams(
            collective_id=0, has_side_effects=True, vmem_limit_bytes=VMEM_MIB * 1024 * 1024
        ),
    )(
        tokens,
        w_query,
        w_forget,
        w_input,
        w_gate,
        w_out,
        gain.reshape(1, -1),
        head_gain.reshape(1, -1),
        lower_bound.reshape(1, -1),
        state,
        last_forget,
        last_values,
        accepted,
    )
    return pl.pallas_call(
        last,
        out_shape=(
            jax.ShapeDtypeStruct((seqs, props, half), BF16),
            jax.ShapeDtypeStruct(state.shape, F32),
        ),
        in_specs=[held] * len(outs),
        out_specs=(anywhere, anywhere),
        scratch_shapes=[pltpu.VMEM((seqs, props, half), BF16), dma((2,))],
        compiler_params=pltpu.CompilerParams(vmem_limit_bytes=4 * 1024 * 1024),
    )(*results)


def solution(mesh):
    in_specs = (
        P(("grp", "dp"), None, "kv"),
        P("kv", "tp"),
        P("kv", "tp"),
        P("kv", "tp"),
        P("kv", "tp"),
        P("tp", "kv"),
        P(),
        P(),
        P(),
        P(("grp", "dp", "kv"), "tp", None, None),
        P(("grp", "dp", "kv"), None, "tp"),
        P(("grp", "dp", "kv"), None, "tp"),
        P(("grp", "dp", "kv")),
    )
    out_specs = (P(("grp", "dp"), None, ("kv", "tp")), P(("grp", "dp", "kv"), "tp", None, None))
    return jax.shard_map(
        functools.partial(per_device, mesh.shape["kv"], mesh.shape["tp"]),
        mesh=mesh,
        in_specs=in_specs,
        out_specs=out_specs,
        check_vma=False,
    )
```

```python
import functools

import jax
import jax.numpy as jnp
from jax import lax
from jax.experimental import pallas as pl
from jax.experimental.pallas import tpu as pltpu
from jax.sharding import PartitionSpec as P

HEAD = 128
EPSILON = 1e-05
CHUNK_HEADS = 4
LINE = 4
LINE_HEADS = 2
CROSS = 1
VMEM_MIB = 56
F32 = jnp.float32
BF16 = jnp.bfloat16

MESSAGES = {
    "0 for 3": (0, 1, 3, 3),
    "0 for 2": (0, 1, 2, 4),
    "0 to 1": (0, 1, 1, 0),
    "1 to 0": (1, 0, 0, 0),
    "1 to 3": (1, 3, 3, 0),
    "1 to 2": (1, 2, 2, 0),
    "2 to 3": (2, 3, 3, 1),
    "2 to 0": (2, 0, 0, 1),
    "2 to 1": (2, 1, 1, 1),
    "3 for 1": (3, 2, 1, 3),
    "3 to 1": (3, 1, 1, 2),
    "3 to 2": (3, 2, 2, 1),
    "3 to 0": (3, 0, 0, 2),
}
OWN = 3
DIRECT = 1
PEERS = ((3, 2, 1), (3, 2, 0), (0, 3, 1), (0, 1, 2))


def kernel_any(
    kv,
    tp,
    tokens,
    w_query,
    w_forget,
    w_input,
    w_gate,
    w_out,
    gain,
    head_gain,
    lower_bound,
    state,
    last_forget,
    last_values,
    accepted,
    tk_v,
    own_v,
    peer_v,
    tok_v,
    gain_v,
    hg_v,
    lb_v,
    lf_v,
    lv_v,
    rows_v,
    scaled_v,
    w_v,
    wo_v,
    st_v,
    tkb_v,
    lfr_v,
    lvr_v,
    ssq_v,
    ssq_r,
    prod_v,
    send_v,
    recv_v,
    gath_v,
    acc_v,
    part_v,
    relay_v,
    load_sem,
    w_sem,
    wo_sem,
    st_sem,
    ssq_ssem,
    ssq_rsem,
    rs_ssem,
    rs_rsem,
    relay_ssem,
    relay_rsem,
    ag_ssem,
    ag_rsem,
    tp_ssem,
    tp_rsem,
):
    me = lax.axis_index("kv")
    tme = lax.axis_index("tp")
    seqs, props, feat = tokens.shape
    own_seqs, heads_dev = state.shape[0], state.shape[1]
    own_rows = own_seqs * props
    rows = seqs * props
    width = gain.shape[1]
    head_cols = heads_dev * HEAD
    chunks = heads_dev // CHUNK_HEADS
    cw = CHUNK_HEADS * HEAD
    half = w_out.shape[1] // tp
    weights = (w_query, w_forget, w_input, w_gate)

    def local(src, dst, sem):
        copy = pltpu.make_async_copy(src, dst, sem)
        copy.start()
        return copy

    tok_c = local(tokens, tok_v, load_sem.at[0])
    gain_c = local(gain, gain_v, load_sem.at[1])

    def load_w(c):
        return [
            local(w.at[:, pl.ds(c * cw, cw)], w_v.at[c, :, pl.ds(i * cw, cw)], w_sem.at[c, i])
            for i, w in enumerate(weights)
        ]

    def load_state(c):
        hs = pl.ds(c * CHUNK_HEADS, CHUNK_HEADS)
        return local(state.at[:, hs], st_v.at[:, hs], st_sem.at[c])

    w_c = [load_w(0)]
    small_c = [
        local(last_forget, lf_v, load_sem.at[2]),
        local(last_values, lv_v, load_sem.at[3]),
        local(head_gain, hg_v, load_sem.at[4]),
        local(lower_bound, lb_v, load_sem.at[5]),
    ]
    st_c = []
    for c in range(chunks):
        st_c.append(load_state(c))
        if c + 1 < chunks:
            w_c.append(load_w(c + 1))
    wo_c = []
    for o in range(tp):
        column = pl.multiple_of(lax.rem(tme + o, tp) * half, half)
        wo_c.append(local(w_out.at[:, pl.ds(column, half)], wo_v.at[o], wo_sem.at[o]))

    barrier = pltpu.get_barrier_semaphore()
    kv_peers = [lax.rem(me + o, kv) for o in range(1, kv)]
    tp_peers = [lax.rem(tme + o, tp) for o in range(1, tp)]
    for peer in kv_peers:
        pl.semaphore_signal(barrier, inc=1, device_id={"kv": peer}, device_id_type=pl.DeviceIdType.MESH)
    for peer in tp_peers:
        pl.semaphore_signal(barrier, inc=1, device_id={"tp": peer}, device_id_type=pl.DeviceIdType.MESH)

    def remote(src, dst, ssem, rsem, axis, peer):
        copy = pltpu.make_async_remote_copy(
            src_ref=src,
            dst_ref=dst,
            send_sem=ssem,
            recv_sem=rsem,
            device_id={axis: peer},
            device_id_type=pl.DeviceIdType.MESH,
        )
        copy.start()
        return copy

    tok_c.wait()
    gain_c.wait()
    for s in range(seqs):
        rows_v[pl.ds(s * props, props), :] = tok_v[s].astype(F32)
    x = rows_v[...]
    my_gain = gain_v[:, pl.ds(pl.multiple_of(me * feat, feat), feat)]
    scaled_v[...] = (x * my_gain).astype(BF16)
    ssq_v[...] = jnp.broadcast_to(jnp.sum(x * x, axis=1, keepdims=True), (rows, HEAD))

    pl.semaphore_wait(barrier, kv - 1 + tp - 1)

    def rows_of(device):
        return pl.ds(pl.multiple_of(device * own_rows, own_rows), own_rows)

    ssq_c = [
        remote(
            ssq_v.at[rows_of(peer)], ssq_r.at[o], ssq_ssem.at[o], ssq_rsem.at[o], "kv", peer
        )
        for o, peer in enumerate(kv_peers)
    ]

    place = lax.broadcasted_iota(jnp.int32, (own_rows, 1), 0)
    prop = lax.rem(place, props)
    seq = place // props

    def old_terms():
        for copy in small_c:
            copy.wait()
        for s in range(own_seqs):
            lfr_v[pl.ds(s * props, props), :] = lf_v[s]
            lvr_v[pl.ds(s * props, props), :] = lv_v[s].astype(F32)
        limit = jnp.zeros((own_rows, 1), jnp.int32)
        for s in range(own_seqs):
            limit = jnp.where(seq == s, accepted[s], limit)
        mask = prop < limit
        old = lfr_v[...]
        decay = jnp.where(mask, old, 1.0)
        weight = jnp.where(mask, 1.0 - old, 0.0)
        after = jnp.ones_like(decay)
        for lag in range(1, props):
            after = after * jnp.where(
                prop < props - lag, pltpu.roll(decay, own_rows - lag, 0), 1.0
            )
        return decay * after, weight * after, lvr_v[...].astype(BF16)

    def take(c, ends, old_weight, old_values):
        st_c[c].wait()
        lane_seq = lax.broadcasted_iota(jnp.int32, (1, own_rows), 1) // props
        for h in range(c * CHUNK_HEADS, (c + 1) * CHUNK_HEADS):
            cols = slice(h * HEAD, (h + 1) * HEAD)
            end_t = ends[:, cols].T
            weight_t = old_weight[:, cols].T
            for s in range(own_seqs):
                mine = jnp.where(lane_seq == s, weight_t, 0.0).astype(BF16)
                added = jnp.dot(mine, old_values[:, cols], preferred_element_type=F32)
                new = end_t[:, s * props : s * props + 1] * st_v[s, h] + added
                tk_v[s, h] = new
                tkb_v[h, pl.ds(s * HEAD, HEAD), :] = new.astype(BF16)

    relayed = kv == 4
    at_end = jnp.logical_or(me == 0, me == kv - 1)
    first = me == 0
    last = me == kv - 1
    if relayed:

        @pl.when(last)
        def _():
            recv_v[:, kv - 2] = jnp.zeros_like(recv_v[:, kv - 2])

        @pl.when(first)
        def _():
            recv_v[:, 0] = jnp.zeros_like(recv_v[:, 0])

    def rs_copy(c, o):
        return pltpu.make_async_remote_copy(
            src_ref=send_v.at[c, rows_of(kv_peers[o])],
            dst_ref=recv_v.at[c, o],
            send_sem=rs_ssem.at[c, o],
            recv_sem=rs_rsem.at[c, o],
            device_id={"kv": kv_peers[o]},
            device_id_type=pl.DeviceIdType.MESH,
        )

    def relay_copy(c, end):
        far, near = (kv - 1, 1) if end == 0 else (0, kv - 2)
        return pltpu.make_async_remote_copy(
            src_ref=send_v.at[c, rows_of(far)],
            dst_ref=relay_v.at[c],
            send_sem=relay_ssem.at[c],
            recv_sem=relay_rsem.at[c],
            device_id={"kv": near},
            device_id_type=pl.DeviceIdType.MESH,
        )

    def send_blocks(c):
        if not relayed:
            for o in range(kv - 1):
                rs_copy(c, o).start()
            return

        @pl.when(first)
        def _():
            relay_copy(c, 0).start()
            rs_copy(c, 1).start()
            if c > 0:
                rs_copy(c - 1, 0).start()
            if c == chunks - 1:
                rs_copy(c, 0).start()

        @pl.when(last)
        def _():
            relay_copy(c, kv - 1).start()
            rs_copy(c, 1).start()
            if c > 0:
                rs_copy(c - 1, 2).start()
            if c == chunks - 1:
                rs_copy(c, 2).start()

        @pl.when(jnp.logical_not(at_end))
        def _():
            rs_copy(c, 0).start()
            rs_copy(c, 2).start()

    def send_on(c):
        if relayed:

            @pl.when(jnp.logical_not(at_end))
            def _():
                relay_copy(c, 0).wait_recv()
                far = rows_of(kv_peers[1])
                send_v[c, far, :] = (prod_v[c, far, :] + relay_v[c].astype(F32)).astype(BF16)
                rs_copy(c, 1).start()

    def wait_blocks(c):
        for o in range(kv - 1):
            if relayed and o == 0:
                pl.when(jnp.logical_not(first))(lambda o=o: rs_copy(c, o).wait_recv())
            elif relayed and o == kv - 2:
                pl.when(jnp.logical_not(last))(lambda o=o: rs_copy(c, o).wait_recv())
            else:
                rs_copy(c, o).wait_recv()

    def wait_sent(c):
        if not relayed:
            for o in range(kv - 1):
                rs_copy(c, o).wait_send()
            return
        rs_copy(c, 1).wait_send()

        @pl.when(first)
        def _():
            relay_copy(c, 0).wait_send()
            rs_copy(c, 0).wait_send()

        @pl.when(last)
        def _():
            relay_copy(c, kv - 1).wait_send()
            rs_copy(c, 2).wait_send()

        @pl.when(jnp.logical_not(at_end))
        def _():
            rs_copy(c, 0).wait_send()
            rs_copy(c, 2).wait_send()

    terms = None
    for c in range(chunks):
        for copy in w_c[c]:
            copy.wait()
        product = jnp.dot(scaled_v[...], w_v[c], preferred_element_type=F32)
        prod_v[c] = product
        send_v[c] = product.astype(BF16)
        send_blocks(c)
        if terms is None:
            terms = old_terms()
        if c > 0:
            send_on(c - 1)
        take(c, *terms)
    send_on(chunks - 1)

    squares = ssq_v[rows_of(me), :]
    for o in range(kv - 1):
        ssq_c[o].wait_recv()
        squares = squares + ssq_r[o]
    row_scale = lax.rsqrt(squares[:, :1] / width + EPSILON)
    mine_rows = rows_of(me)
    ag_c = []

    def recur(c):
        wait_blocks(c)

        def projected(i):
            total = prod_v[c, mine_rows, pl.ds(i * cw, cw)]
            for o in range(kv - 1):
                total = total + recv_v[c, o, :, pl.ds(i * cw, cw)].astype(F32)
            return total * row_scale

        column = pl.multiple_of(tme * head_cols + c * cw, cw)
        floor_gate = lb_v[:, pl.ds(column, cw)]
        forget = floor_gate + (1.0 - floor_gate) * jax.nn.sigmoid(projected(1))
        keys = 1.0 - forget
        queries = jax.nn.silu(projected(0)) * HEAD ** (-0.5)
        values = projected(2)
        gate = jax.nn.silu(projected(3)) * hg_v[:, pl.ds(column, cw)]
        start = forget
        for lag in range(1, props):
            start = start * jnp.where(prop >= lag, pltpu.roll(forget, lag, 0), 1.0)
        reading = queries * start
        results = []
        for h in range(CHUNK_HEADS):
            cols = slice(h * HEAD, (h + 1) * HEAD)
            lhs = jnp.concatenate(
                [jnp.where(seq == s, reading[:, cols], 0.0) for s in range(own_seqs)], axis=1
            ).astype(BF16)
            results.append(
                jnp.dot(lhs, tkb_v[c * CHUNK_HEADS + h], preferred_element_type=F32)
            )
        decay = queries
        for lag in range(props):
            if lag > 0:
                decay = decay * (forget if lag == 1 else pltpu.roll(forget, lag - 1, 0))
            pair = decay * (keys if lag == 0 else pltpu.roll(keys, lag, 0))
            pair = jnp.where(prop >= lag, pair, 0.0)
            moved = values if lag == 0 else pltpu.roll(values, lag, 0)
            for h in range(CHUNK_HEADS):
                cols = slice(h * HEAD, (h + 1) * HEAD)
                score = jnp.sum(pair[:, cols], axis=1, keepdims=True)
                results[h] = results[h] + score * moved[:, cols]
        outs = []
        for h in range(CHUNK_HEADS):
            cols = slice(h * HEAD, (h + 1) * HEAD)
            r = results[h]
            normed = r * lax.rsqrt(jnp.mean(r * r, axis=1, keepdims=True) + EPSILON)
            outs.append((normed * gate[:, cols]).astype(BF16))
        gath_v[c, mine_rows, :] = jnp.concatenate(outs, axis=1)
        ag_c.append(
            [
                remote(
                    gath_v.at[c, mine_rows],
                    gath_v.at[c, mine_rows],
                    ag_ssem.at[c, o],
                    ag_rsem.at[c, o],
                    "kv",
                    peer,
                )
                for o, peer in enumerate(kv_peers)
            ]
        )

    def product_of(c, o):
        term = jnp.dot(
            gath_v[c], wo_v[o, pl.ds(c * cw, cw), :], preferred_element_type=F32
        )
        return term if c == 0 else acc_v[o] + term

    def gathered(c):
        for o in range(kv - 1):
            ag_c[c][o].wait_recv()

    for c in range(chunks):
        recur(c)
    for copy in wo_c:
        copy.wait()
    for c in range(chunks - 1):
        gathered(c)
        for o in range(tp):
            acc_v[o] = product_of(c, o)
    gathered(chunks - 1)
    tp_c = []
    for o in range(1, tp):
        part_v[o - 1] = product_of(chunks - 1, o).astype(BF16)
        tp_c.append(
            remote(
                part_v.at[o - 1],
                peer_v.at[o - 1],
                tp_ssem.at[o - 1],
                tp_rsem.at[o - 1],
                "tp",
                tp_peers[o - 1],
            )
        )
    own_v[...] = product_of(chunks - 1, 0).astype(BF16)
    for copy in tp_c:
        copy.wait_recv()
    for c in range(chunks):
        wait_sent(c)
    for copies in [ssq_c, *ag_c, tp_c]:
        for copy in copies:
            copy.wait_send()


def kernel_line(
    tp,
    tokens,
    w_query,
    w_forget,
    w_input,
    w_gate,
    w_out,
    gain,
    head_gain,
    lower_bound,
    state,
    last_forget,
    last_values,
    accepted,
    tk_v,
    acc_v,
    last_v,
    wl_v,
    tok_v,
    gain_v,
    hg_v,
    lb_v,
    lf_v,
    lv_v,
    rows_v,
    scaled_v,
    w_v,
    wo_v,
    st_v,
    tkb_v,
    lfr_v,
    lvr_v,
    ssq_v,
    ssq_s,
    ssq_r,
    prod_v,
    send_v,
    recv_v,
    gath_v,
    acc_s,
    load_sem,
    w_sem,
    wo_sem,
    st_sem,
    ssq_ssem,
    ssq_rsem,
    rs_ssem,
    rs_rsem,
    ag_ssem,
    ag_rsem,
    cross_rsem,
    fw_ssem,
    fw_rsem,
    wo_ssem,
    wo_rsem,
    go_sem,
):
    kv = LINE
    me = lax.axis_index("kv")
    tme = lax.axis_index("tp")
    seqs, props, feat = tokens.shape
    own_seqs, heads_dev = state.shape[0], state.shape[1]
    own_rows = own_seqs * props
    rows = seqs * props
    width = gain.shape[1]
    head_cols = heads_dev * HEAD
    chunks = heads_dev // LINE_HEADS
    cw = LINE_HEADS * HEAD
    half = w_out.shape[1] // tp
    weights = (w_query, w_forget, w_input, w_gate)

    at_end = jnp.logical_or(me == 0, me == kv - 1)

    def local(src, dst, sem):
        copy = pltpu.make_async_copy(src, dst, sem)
        copy.start()
        return copy

    tok_c = local(tokens, tok_v, load_sem.at[0])
    gain_c = local(gain, gain_v, load_sem.at[1])

    def held(ref, sem):
        pltpu.make_async_copy(ref, ref, sem).wait()

    def load_w(c):
        for i, w in enumerate(weights):
            local(w.at[:, pl.ds(c * cw, cw)], w_v.at[c, :, pl.ds(i * cw, cw)], w_sem.at[c])

    def load_late():
        small = [
            local(last_forget, lf_v, load_sem.at[2]),
            local(last_values, lv_v, load_sem.at[3]),
            local(head_gain, hg_v, load_sem.at[4]),
            local(lower_bound, lb_v, load_sem.at[5]),
            local(accepted, acc_s, load_sem.at[6]),
        ]
        return small, local(state, st_v, st_sem)

    split = (chunks - 1) * cw
    crossed = chunks - CROSS

    def load_out():
        cols = pl.ds(pl.multiple_of(tme * half, half), half)
        local(w_out.at[:split, cols], wo_v.at[0], wo_sem)
        local(w_out.at[split:, cols], wl_v.at[0], wo_sem)

    def out_held(sem):
        held(w_v.at[0, : head_cols * half // (4 * cw)], sem)

    load_w(0)

    def signal(axis, peer):
        pl.semaphore_signal(
            barrier, inc=1, device_id={axis: peer}, device_id_type=pl.DeviceIdType.MESH
        )

    barrier = pltpu.get_barrier_semaphore()
    tp_peers = [lax.rem(tme + o, tp) for o in range(1, tp)]
    for peer in tp_peers:
        signal("tp", peer)

    @pl.when(me > 0)
    def _():
        signal("kv", me - 1)

    @pl.when(me < kv - 1)
    def _():
        signal("kv", me + 1)

    def remote(src, dst, ssem, rsem, axis, peer):
        return pltpu.make_async_remote_copy(
            src_ref=src,
            dst_ref=dst,
            send_sem=ssem,
            recv_sem=rsem,
            device_id={axis: peer},
            device_id_type=pl.DeviceIdType.MESH,
        )

    gain_c.wait()
    load_w(1)
    tok_c.wait()
    load_w(2)
    for s in range(seqs):
        rows_v[pl.ds(s * props, props), :] = tok_v[s].astype(F32)
    x = rows_v[...]
    my_gain = gain_v[:, pl.ds(pl.multiple_of(me * feat, feat), feat)]
    scaled_v[...] = (x * my_gain).astype(BF16)

    def rows_of(device):
        return pl.ds(pl.multiple_of(device * own_rows, own_rows), own_rows)

    def message(c, name):
        _, to, dest, slot = MESSAGES[name]
        return remote(
            send_v.at[c, rows_of(dest)],
            recv_v.at[c, slot],
            rs_ssem,
            rs_rsem.at[c, max(slot - OWN + 1, 0)],
            "kv",
            to,
        )

    def pass_on(c, name, onward):
        _, _, dest, slot = MESSAGES[name]
        message(c, name).wait_recv()
        into = rows_of(dest)
        send_v[c, into, :] = (prod_v[c, into, :] + recv_v[c, slot].astype(F32)).astype(BF16)
        message(c, onward).start()

    def ssq_copy(i, slot, to):
        return remote(ssq_s.at[i], ssq_r.at[slot], ssq_ssem.at[i], ssq_rsem.at[slot], "kv", to)

    partner = me + 1 - 2 * lax.rem(me, 2)
    across = jnp.where(me == 1, 2, 1)
    beyond = jnp.where(me == 1, 3, 0)
    inside = jnp.logical_not(at_end)
    pl.semaphore_wait(barrier, jnp.where(at_end, tp, tp + 1))
    def go(to):
        pl.semaphore_signal(
            go_sem, inc=1, device_id={"kv": to}, device_id_type=pl.DeviceIdType.MESH
        )

    @pl.when(inside)
    def _():
        go(across)

    direct = chunks - DIRECT

    def terms_of(c):
        return (me == 0) if c < direct else (me < 2)


    place = lax.broadcasted_iota(jnp.int32, (own_rows, 1), 0)
    prop = lax.rem(place, props)
    seq = place // props

    def old_terms():
        for copy in small_c:
            copy.wait()
        for s in range(own_seqs):
            lfr_v[pl.ds(s * props, props), :] = lf_v[s]
            lvr_v[pl.ds(s * props, props), :] = lv_v[s].astype(F32)
        limit = jnp.zeros((own_rows, 1), jnp.int32)
        for s in range(own_seqs):
            limit = jnp.where(seq == s, acc_s[s], limit)
        mask = prop < limit
        old = lfr_v[...]
        decay = jnp.where(mask, old, 1.0)
        weight = jnp.where(mask, 1.0 - old, 0.0)
        after = jnp.ones_like(decay)
        for lag in range(1, props):
            after = after * jnp.where(
                prop < props - lag, pltpu.roll(decay, own_rows - lag, 0), 1.0
            )
        return decay * after, weight * after, lvr_v[...].astype(BF16)

    def take(c, ends, old_weight, old_values):
        if c == 0:
            st_c.wait()
        lane_seq = lax.broadcasted_iota(jnp.int32, (1, own_rows), 1) // props
        for h in range(c * LINE_HEADS, (c + 1) * LINE_HEADS):
            cols = slice(h * HEAD, (h + 1) * HEAD)
            end_t = ends[:, cols].T
            weight_t = old_weight[:, cols].T
            for s in range(own_seqs):
                mine = jnp.where(lane_seq == s, weight_t, 0.0).astype(BF16)
                added = jnp.dot(mine, old_values[:, cols], preferred_element_type=F32)
                new = end_t[:, s * props : s * props + 1] * st_v[s, h] + added
                tk_v[s, h] = new
                tkb_v[h, pl.ds(s * HEAD, HEAD), :] = new.astype(BF16)

    for c in range(chunks):
        held(w_v.at[c], w_sem.at[c])
        if c + 3 < chunks:
            load_w(c + 3)
        elif c + 3 == chunks:
            small_c, st_c = load_late()
        elif c + 2 == chunks:
            load_out()
        product = jnp.dot(scaled_v[...], w_v[c], preferred_element_type=F32)
        prod_v[c] = product
        send_v[c] = product.astype(BF16)

        @pl.when(me == 0)
        def _():
            message(c, "0 for 3").start()

        @pl.when(me == 1)
        def _():
            message(c, "1 to 0").start()

        @pl.when(me == 2)
        def _():
            message(c, "2 to 3").start()
            if c == 0:
                pl.semaphore_wait(go_sem, 1)
                go(3)
            message(c, "2 to 0").start()
            if c >= direct:
                message(c, "2 to 1").start()

        @pl.when(me == 3)
        def _():
            if c == direct:
                pl.semaphore_wait(go_sem, 1)
            message(c, "3 to 1" if c >= direct else "3 for 1").start()

        if c == 0:
            x = rows_v[...]
            squared = jnp.sum(x * x, axis=1, keepdims=True)
            on_row = lax.broadcasted_iota(jnp.int32, (rows, HEAD), 0)
            on_lane = lax.broadcasted_iota(jnp.int32, (rows, HEAD), 1)
            along = jnp.sum(jnp.where(on_row == on_lane, squared, 0.0), axis=0, keepdims=True)
            ssq_v[...] = along
            ssq_s[0] = along
            ssq_copy(0, 0, partner).start()

    @pl.when(me == 0)
    def _():
        for name in ("0 for 2", "0 to 1"):
            for c in range(chunks):
                message(c, name).start()

    @pl.when(me == 3)
    def _():
        for name in ("3 to 2", "3 to 0"):
            for c in range(chunks):
                message(c, name).start()

    for c in range(chunks):

        @pl.when(jnp.logical_not(terms_of(c)))
        def _():
            recv_v[c, OWN - 1] = jnp.zeros_like(recv_v[c, OWN - 1])

    terms = old_terms()
    ssq_copy(0, 0, partner).wait_recv()

    @pl.when(me == 1)
    def _():
        pl.semaphore_wait(go_sem, 1)

    @pl.when(inside)
    def _():
        ssq_s[1] = ssq_v[...] + ssq_r[0]
        ssq_copy(1, 1, across).start()
        ssq_s[2] = ssq_v[...] + ssq_r[0]
        ssq_copy(2, 1, beyond).start()

    for c in range(chunks):
        @pl.when(me == 1)
        def _():
            pass_on(c, "0 for 3", "1 to 3")

        if c < direct:

            @pl.when(me == 2)
            def _():
                pass_on(c, "3 for 1", "2 to 1")

        take(c, *terms)

    @pl.when(me == 1)
    def _():
        for c in range(chunks):
            pass_on(c, "0 for 2", "1 to 2")

    for o in range(1, tp):
        cols = pl.ds(pl.multiple_of(tp_peers[o - 1] * half, half), half)
        for rows_out, into in ((w_out.at[:split, cols], wo_v), (w_out.at[split:, cols], wl_v)):
            copy = remote(
                rows_out, into.at[tp - o], wo_ssem.at[o - 1], wo_rsem.at[tp - o - 1],
                "tp", tp_peers[o - 1],
            )
            copy.start()

    ssq_copy(1, 1, partner).wait_recv()
    whole = ssq_v[...] + ssq_r[0] + ssq_r[1]
    mine_rows = rows_of(me)
    picked = lax.broadcasted_iota(jnp.int32, (own_rows, HEAD), 1) == (
        lax.broadcasted_iota(jnp.int32, (own_rows, HEAD), 0) + me * own_rows
    )
    squares = jnp.sum(jnp.where(picked, whole[:1], 0.0), axis=1, keepdims=True)
    row_scale = lax.rsqrt(squares / width + EPSILON)
    peers = [
        functools.reduce(lambda found, d: jnp.where(me == d, PEERS[d][o], found), range(kv), 0)
        for o in range(kv - 1)
    ]

    def heads_of(c, slot):
        return gath_v.at[slot, c] if c < chunks - 1 else last_v.at[slot]

    def head_copy(c, o):
        mine = heads_of(c, 0).at[mine_rows]
        return remote(mine, mine, ag_ssem, ag_rsem.at[c], "kv", peers[o])

    def cross_copy(c, o, i):
        ids = {"tp": tp_peers[o - 1]}
        if i < kv - 1:
            ids["kv"] = peers[i]
        return pltpu.make_async_remote_copy(
            src_ref=heads_of(c, 0).at[mine_rows],
            dst_ref=heads_of(c, tp - o).at[mine_rows],
            send_sem=ag_ssem,
            recv_sem=cross_rsem.at[c - crossed, tp - o - 1],
            device_id=ids,
            device_id_type=pl.DeviceIdType.MESH,
        )

    def cross_copies(c):
        return [cross_copy(c, o, i) for o in range(1, tp) for i in range(kv)]

    def forward(c, o):
        return remote(
            gath_v.at[0, c], gath_v.at[tp - o, c], fw_ssem.at[c, o - 1],
            fw_rsem.at[c, tp - o - 1], "tp", tp_peers[o - 1],
        )

    def send_heads(c, o):
        if o < kv - 1:
            head_copy(c, o).start()
        if c >= crossed:
            for away in range(1, tp):
                cross_copy(c, away, o).start()

    def recur(c):
        @pl.when(terms_of(c))
        def _():
            held(recv_v.at[c, :OWN], rs_rsem.at[c, 0])

        @pl.when(jnp.logical_not(terms_of(c)))
        def _():
            held(recv_v.at[c, : OWN - 1], rs_rsem.at[c, 0])

        def projected(i):
            cols = pl.ds(i * cw, cw)
            total = prod_v[c, mine_rows, cols]
            for slot in range(OWN):
                total = total + recv_v[c, slot, :, cols].astype(F32)
            return total * row_scale

        column = pl.multiple_of(tme * head_cols + c * cw, cw)
        floor_gate = lb_v[:, pl.ds(column, cw)]
        forget = floor_gate + (1.0 - floor_gate) * jax.nn.sigmoid(projected(1))
        keys = 1.0 - forget
        queries = jax.nn.silu(projected(0)) * HEAD ** (-0.5)
        values = projected(2)
        gate = jax.nn.silu(projected(3)) * hg_v[:, pl.ds(column, cw)]
        start = forget
        for lag in range(1, props):
            start = start * jnp.where(prop >= lag, pltpu.roll(forget, lag, 0), 1.0)
        reading = queries * start
        results = []
        for h in range(LINE_HEADS):
            cols = slice(h * HEAD, (h + 1) * HEAD)
            lhs = jnp.concatenate(
                [jnp.where(seq == s, reading[:, cols], 0.0) for s in range(own_seqs)], axis=1
            ).astype(BF16)
            results.append(
                jnp.dot(lhs, tkb_v[c * LINE_HEADS + h], preferred_element_type=F32)
            )
        decay = queries
        for lag in range(props):
            if lag > 0:
                decay = decay * (forget if lag == 1 else pltpu.roll(forget, lag - 1, 0))
            pair = decay * (keys if lag == 0 else pltpu.roll(keys, lag, 0))
            pair = jnp.where(prop >= lag, pair, 0.0)
            moved = values if lag == 0 else pltpu.roll(values, lag, 0)
            for h in range(LINE_HEADS):
                cols = slice(h * HEAD, (h + 1) * HEAD)
                score = jnp.sum(pair[:, cols], axis=1, keepdims=True)
                results[h] = results[h] + score * moved[:, cols]
        outs = []
        for h in range(LINE_HEADS):
            cols = slice(h * HEAD, (h + 1) * HEAD)
            r = results[h]
            normed = r * lax.rsqrt(jnp.mean(r * r, axis=1, keepdims=True) + EPSILON)
            outs.append((normed * gate[:, cols]).astype(BF16))
        heads_of(c, 0)[mine_rows, :] = jnp.concatenate(outs, axis=1)
        for o in (0, 1, kv - 1):
            send_heads(c, o)

        @pl.when(me != 2)
        def _():
            send_heads(c, 2)

        if c >= 2:

            @pl.when(me == 2)
            def _():
                send_heads(c - 2, 2)

    def gathered(c):
        held(heads_of(c, 0).at[: (kv - 1) * own_rows], ag_rsem.at[c])

    def product_of(c, slot):
        term = jnp.dot(
            gath_v[slot, c], wo_v[slot, pl.ds(c * cw, cw), :], preferred_element_type=F32
        )
        acc_v[slot] = term if c == 0 else acc_v[slot] + term

    def from_tp(c):
        for o in range(1, tp):
            if c < crossed:
                forward(c, tp - o).wait_recv()
                continue
            held(heads_of(c, o), cross_rsem.at[c - crossed, o - 1])

    for c in range(chunks):
        recur(c)

    @pl.when(me == 2)
    def _():
        for c in range(chunks - 2, chunks):
            send_heads(c, 2)

    out_held(wo_sem)
    for o in range(1, tp):
        out_held(wo_rsem.at[o - 1])
    for c in range(chunks):
        gathered(c)
        if c < crossed:
            for o in range(1, tp):
                forward(c, o).start()
        if c < chunks - 1:
            product_of(c, 0)
        if c == chunks - 2:
            for early in range(chunks - 2):
                from_tp(early)
                for o in range(1, tp):
                    product_of(early, o)
    for c in range(chunks - 2, chunks):
        from_tp(c)
        if c < chunks - 1:
            for o in range(1, tp):
                product_of(c, o)

    held(send_v.at[:, : (kv - 1) * own_rows], rs_ssem)
    ssq_copy(0, 0, partner).wait_send()

    @pl.when(inside)
    def _():
        ssq_copy(1, 1, across).wait_send()
        ssq_copy(2, 1, beyond).wait_send()

    blocks = chunks * (kv - 1) + CROSS * (tp - 1) * kv
    held(w_v.at[0, : blocks * own_rows // 4], ag_ssem)
    for o in range(1, tp):
        out_held(wo_ssem.at[o - 1])
    for c in range(crossed):
        for o in range(1, tp):
            forward(c, o).wait_send()


def finish_line(tk_v, acc_v, last_v, wl_v, mixed, taken, mix_v, sem):
    tk_c = pltpu.make_async_copy(tk_v, taken, sem.at[0])
    tk_c.start()
    seqs, props, _ = mixed.shape
    total = 0.0
    for slot in range(acc_v.shape[0]):
        term = jnp.dot(last_v[slot], wl_v[slot], preferred_element_type=F32)
        total = total + (acc_v[slot] + term).astype(BF16).astype(F32)
    for s in range(seqs):
        mix_v[s] = total[s * props : (s + 1) * props].astype(BF16)
    mix_c = pltpu.make_async_copy(mix_v, mixed, sem.at[1])
    mix_c.start()
    mix_c.wait()
    tk_c.wait()


def finish(tk_v, own_v, peer_v, mixed, taken, mix_v, sem):
    tk_c = pltpu.make_async_copy(tk_v, taken, sem.at[0])
    tk_c.start()
    seqs, props, _ = mixed.shape
    total = own_v[...].astype(F32)
    for o in range(peer_v.shape[0]):
        total = total + peer_v[o].astype(F32)
    for s in range(seqs):
        mix_v[s] = total[s * props : (s + 1) * props].astype(BF16)
    mix_c = pltpu.make_async_copy(mix_v, mixed, sem.at[1])
    mix_c.start()
    mix_c.wait()
    tk_c.wait()


def per_device(
    kv,
    tp,
    tokens,
    w_query,
    w_forget,
    w_input,
    w_gate,
    w_out,
    gain,
    head_gain,
    lower_bound,
    state,
    last_forget,
    last_values,
    accepted,
):
    seqs, props, feat = tokens.shape
    own_seqs, heads_dev = state.shape[0], state.shape[1]
    own_rows = own_seqs * props
    rows = seqs * props
    head_cols = heads_dev * HEAD
    on_line = kv == LINE and rows <= HEAD
    per_chunk = LINE_HEADS if on_line else CHUNK_HEADS
    chunks = heads_dev // per_chunk
    cw = per_chunk * HEAD
    half = w_out.shape[1] // tp
    peers = kv - 1
    dma = pltpu.SemaphoreType.DMA
    scratch = [
        pltpu.VMEM(tokens.shape, BF16),
        pltpu.VMEM((1, gain.shape[0]), F32),
        pltpu.VMEM((1, head_gain.shape[0]), F32),
        pltpu.VMEM((1, lower_bound.shape[0]), F32),
        pltpu.VMEM(last_forget.shape, F32),
        pltpu.VMEM(last_values.shape, BF16),
        pltpu.VMEM((rows, feat), F32),
        pltpu.VMEM((rows, feat), BF16),
        pltpu.VMEM((chunks, feat, 4 * cw), BF16),
        pltpu.VMEM((tp, head_cols, half), BF16),
        pltpu.VMEM(state.shape, F32),
        pltpu.VMEM((heads_dev, own_seqs * HEAD, HEAD), BF16),
        pltpu.VMEM((own_rows, head_cols), F32),
        pltpu.VMEM((own_rows, head_cols), F32),
    ]
    if on_line:
        body, last = functools.partial(kernel_line, tp), finish_line
        scratch[9] = pltpu.VMEM((tp, head_cols - cw, half), BF16)
        outs = (
            pltpu.VMEM(state.shape, F32),
            pltpu.VMEM((tp, rows, half), F32),
            pltpu.VMEM((tp, rows, cw), BF16),
            pltpu.VMEM((tp, cw, half), BF16),
        )
        scratch += [
            pltpu.VMEM((1, HEAD), F32),
            pltpu.VMEM((3, 1, HEAD), F32),
            pltpu.VMEM((2, 1, HEAD), F32),
            pltpu.VMEM((chunks, rows, 4 * cw), F32),
            pltpu.VMEM((chunks, rows, 4 * cw), BF16),
            pltpu.VMEM((chunks, 5, own_rows, 4 * cw), BF16),
            pltpu.VMEM((tp, chunks - 1, rows, cw), BF16),
            pltpu.SMEM((own_seqs,), jnp.int32),
            dma((7,)),
            dma((chunks,)),
            dma,
            dma,
            dma((3,)),
            dma((2,)),
            dma,
            dma((chunks, 3)),
            dma,
            dma((chunks,)),
            dma((CROSS, tp - 1)),
            dma((chunks - CROSS, tp - 1)),
            dma((chunks - CROSS, tp - 1)),
            dma((tp - 1,)),
            dma((tp - 1,)),
            pltpu.SemaphoreType.REGULAR,
        ]
    else:
        body, last = functools.partial(kernel_any, kv, tp), finish
        outs = (
            pltpu.VMEM(state.shape, F32),
            pltpu.VMEM((rows, half), BF16),
            pltpu.VMEM((tp - 1, rows, half), BF16),
        )
        scratch += [
            pltpu.VMEM((rows, HEAD), F32),
            pltpu.VMEM((peers, own_rows, HEAD), F32),
            pltpu.VMEM((chunks, rows, 4 * cw), F32),
            pltpu.VMEM((chunks, rows, 4 * cw), BF16),
            pltpu.VMEM((chunks, peers, own_rows, 4 * cw), BF16),
            pltpu.VMEM((chunks, rows, cw), BF16),
            pltpu.VMEM((tp, rows, half), F32),
            pltpu.VMEM((tp - 1, rows, half), BF16),
            pltpu.VMEM((chunks, own_rows, 4 * cw), BF16),
            dma((6,)),
            dma((chunks, 4)),
            dma((tp,)),
            dma((chunks,)),
            dma((peers,)),
            dma((peers,)),
            dma((chunks, peers)),
            dma((chunks, peers)),
            dma((chunks,)),
            dma((chunks,)),
            dma((chunks, peers)),
            dma((chunks, peers)),
            dma((tp - 1,)),
            dma((tp - 1,)),
        ]
    anywhere = pl.BlockSpec(memory_space=pl.ANY)
    held = pl.BlockSpec(memory_space=pltpu.VMEM)
    results = pl.pallas_call(
        body,
        out_shape=outs,
        in_specs=[pl.BlockSpec(memory_space=pltpu.HBM)] * 12
        + [pl.BlockSpec(memory_space=pltpu.HBM if on_line else pltpu.SMEM)],
        out_specs=(held,) * len(outs),
        scratch_shapes=scratch,
        compiler_params=pltpu.CompilerParams(
            collective_id=0, has_side_effects=True, vmem_limit_bytes=VMEM_MIB * 1024 * 1024
        ),
    )(
        tokens,
        w_query,
        w_forget,
        w_input,
        w_gate,
        w_out,
        gain.reshape(1, -1),
        head_gain.reshape(1, -1),
        lower_bound.reshape(1, -1),
        state,
        last_forget,
        last_values,
        accepted,
    )
    return pl.pallas_call(
        last,
        out_shape=(
            jax.ShapeDtypeStruct((seqs, props, half), BF16),
            jax.ShapeDtypeStruct(state.shape, F32),
        ),
        in_specs=[held] * len(outs),
        out_specs=(anywhere, anywhere),
        scratch_shapes=[pltpu.VMEM((seqs, props, half), BF16), dma((2,))],
        compiler_params=pltpu.CompilerParams(vmem_limit_bytes=4 * 1024 * 1024),
    )(*results)


def solution(mesh):
    in_specs = (
        P(("grp", "dp"), None, "kv"),
        P("kv", "tp"),
        P("kv", "tp"),
        P("kv", "tp"),
        P("kv", "tp"),
        P("tp", "kv"),
        P(),
        P(),
        P(),
        P(("grp", "dp", "kv"), "tp", None, None),
        P(("grp", "dp", "kv"), None, "tp"),
        P(("grp", "dp", "kv"), None, "tp"),
        P(("grp", "dp", "kv")),
    )
    out_specs = (P(("grp", "dp"), None, ("kv", "tp")), P(("grp", "dp", "kv"), "tp", None, None))
    return jax.shard_map(
        functools.partial(per_device, mesh.shape["kv"], mesh.shape["tp"]),
        mesh=mesh,
        in_specs=in_specs,
        out_specs=out_specs,
        check_vma=False,
    )
```

```python
import functools

import jax
import jax.numpy as jnp
from jax import lax
from jax.experimental import pallas as pl
from jax.experimental.pallas import tpu as pltpu
from jax.sharding import PartitionSpec as P

HEAD = 128
EPSILON = 1e-05
CHUNK_HEADS = 4
LINE = 4
LINE_HEADS = 2
CROSS = 1
VMEM_MIB = 56
F32 = jnp.float32
BF16 = jnp.bfloat16

MESSAGES = {
    "0 for 3": (0, 1, 3, 3),
    "0 for 2": (0, 1, 2, 4),
    "0 to 1": (0, 1, 1, 0),
    "1 to 0": (1, 0, 0, 0),
    "1 to 3": (1, 3, 3, 0),
    "1 to 2": (1, 2, 2, 0),
    "2 to 3": (2, 3, 3, 1),
    "2 to 0": (2, 0, 0, 1),
    "2 to 1": (2, 1, 1, 1),
    "3 for 1": (3, 2, 1, 3),
    "3 to 1": (3, 1, 1, 2),
    "3 to 2": (3, 2, 2, 1),
    "3 to 0": (3, 0, 0, 2),
}
OWN = 3
DIRECT = 1
PEERS = ((3, 2, 1), (0, 3, 2), (0, 3, 1), (0, 1, 2))


def kernel_any(
    kv,
    tp,
    tokens,
    w_query,
    w_forget,
    w_input,
    w_gate,
    w_out,
    gain,
    head_gain,
    lower_bound,
    state,
    last_forget,
    last_values,
    accepted,
    tk_v,
    own_v,
    peer_v,
    tok_v,
    gain_v,
    hg_v,
    lb_v,
    lf_v,
    lv_v,
    rows_v,
    scaled_v,
    w_v,
    wo_v,
    st_v,
    tkb_v,
    lfr_v,
    lvr_v,
    ssq_v,
    ssq_r,
    prod_v,
    send_v,
    recv_v,
    gath_v,
    acc_v,
    part_v,
    relay_v,
    load_sem,
    w_sem,
    wo_sem,
    st_sem,
    ssq_ssem,
    ssq_rsem,
    rs_ssem,
    rs_rsem,
    relay_ssem,
    relay_rsem,
    ag_ssem,
    ag_rsem,
    tp_ssem,
    tp_rsem,
):
    me = lax.axis_index("kv")
    tme = lax.axis_index("tp")
    seqs, props, feat = tokens.shape
    own_seqs, heads_dev = state.shape[0], state.shape[1]
    own_rows = own_seqs * props
    rows = seqs * props
    width = gain.shape[1]
    head_cols = heads_dev * HEAD
    chunks = heads_dev // CHUNK_HEADS
    cw = CHUNK_HEADS * HEAD
    half = w_out.shape[1] // tp
    weights = (w_query, w_forget, w_input, w_gate)

    def local(src, dst, sem):
        copy = pltpu.make_async_copy(src, dst, sem)
        copy.start()
        return copy

    tok_c = local(tokens, tok_v, load_sem.at[0])
    gain_c = local(gain, gain_v, load_sem.at[1])

    def load_w(c):
        return [
            local(w.at[:, pl.ds(c * cw, cw)], w_v.at[c, :, pl.ds(i * cw, cw)], w_sem.at[c, i])
            for i, w in enumerate(weights)
        ]

    def load_state(c):
        hs = pl.ds(c * CHUNK_HEADS, CHUNK_HEADS)
        return local(state.at[:, hs], st_v.at[:, hs], st_sem.at[c])

    w_c = [load_w(0)]
    small_c = [
        local(last_forget, lf_v, load_sem.at[2]),
        local(last_values, lv_v, load_sem.at[3]),
        local(head_gain, hg_v, load_sem.at[4]),
        local(lower_bound, lb_v, load_sem.at[5]),
    ]
    st_c = []
    for c in range(chunks):
        st_c.append(load_state(c))
        if c + 1 < chunks:
            w_c.append(load_w(c + 1))
    wo_c = []
    for o in range(tp):
        column = pl.multiple_of(lax.rem(tme + o, tp) * half, half)
        wo_c.append(local(w_out.at[:, pl.ds(column, half)], wo_v.at[o], wo_sem.at[o]))

    barrier = pltpu.get_barrier_semaphore()
    kv_peers = [lax.rem(me + o, kv) for o in range(1, kv)]
    tp_peers = [lax.rem(tme + o, tp) for o in range(1, tp)]
    for peer in kv_peers:
        pl.semaphore_signal(barrier, inc=1, device_id={"kv": peer}, device_id_type=pl.DeviceIdType.MESH)
    for peer in tp_peers:
        pl.semaphore_signal(barrier, inc=1, device_id={"tp": peer}, device_id_type=pl.DeviceIdType.MESH)

    def remote(src, dst, ssem, rsem, axis, peer):
        copy = pltpu.make_async_remote_copy(
            src_ref=src,
            dst_ref=dst,
            send_sem=ssem,
            recv_sem=rsem,
            device_id={axis: peer},
            device_id_type=pl.DeviceIdType.MESH,
        )
        copy.start()
        return copy

    tok_c.wait()
    gain_c.wait()
    for s in range(seqs):
        rows_v[pl.ds(s * props, props), :] = tok_v[s].astype(F32)
    x = rows_v[...]
    my_gain = gain_v[:, pl.ds(pl.multiple_of(me * feat, feat), feat)]
    scaled_v[...] = (x * my_gain).astype(BF16)
    ssq_v[...] = jnp.broadcast_to(jnp.sum(x * x, axis=1, keepdims=True), (rows, HEAD))

    pl.semaphore_wait(barrier, kv - 1 + tp - 1)

    def rows_of(device):
        return pl.ds(pl.multiple_of(device * own_rows, own_rows), own_rows)

    ssq_c = [
        remote(
            ssq_v.at[rows_of(peer)], ssq_r.at[o], ssq_ssem.at[o], ssq_rsem.at[o], "kv", peer
        )
        for o, peer in enumerate(kv_peers)
    ]

    place = lax.broadcasted_iota(jnp.int32, (own_rows, 1), 0)
    prop = lax.rem(place, props)
    seq = place // props

    def old_terms():
        for copy in small_c:
            copy.wait()
        for s in range(own_seqs):
            lfr_v[pl.ds(s * props, props), :] = lf_v[s]
            lvr_v[pl.ds(s * props, props), :] = lv_v[s].astype(F32)
        limit = jnp.zeros((own_rows, 1), jnp.int32)
        for s in range(own_seqs):
            limit = jnp.where(seq == s, accepted[s], limit)
        mask = prop < limit
        old = lfr_v[...]
        decay = jnp.where(mask, old, 1.0)
        weight = jnp.where(mask, 1.0 - old, 0.0)
        after = jnp.ones_like(decay)
        for lag in range(1, props):
            after = after * jnp.where(
                prop < props - lag, pltpu.roll(decay, own_rows - lag, 0), 1.0
            )
        return decay * after, weight * after, lvr_v[...].astype(BF16)

    def take(c, ends, old_weight, old_values):
        st_c[c].wait()
        lane_seq = lax.broadcasted_iota(jnp.int32, (1, own_rows), 1) // props
        for h in range(c * CHUNK_HEADS, (c + 1) * CHUNK_HEADS):
            cols = slice(h * HEAD, (h + 1) * HEAD)
            end_t = ends[:, cols].T
            weight_t = old_weight[:, cols].T
            for s in range(own_seqs):
                mine = jnp.where(lane_seq == s, weight_t, 0.0).astype(BF16)
                added = jnp.dot(mine, old_values[:, cols], preferred_element_type=F32)
                new = end_t[:, s * props : s * props + 1] * st_v[s, h] + added
                tk_v[s, h] = new
                tkb_v[h, pl.ds(s * HEAD, HEAD), :] = new.astype(BF16)

    relayed = kv == 4
    at_end = jnp.logical_or(me == 0, me == kv - 1)
    first = me == 0
    last = me == kv - 1
    if relayed:

        @pl.when(last)
        def _():
            recv_v[:, kv - 2] = jnp.zeros_like(recv_v[:, kv - 2])

        @pl.when(first)
        def _():
            recv_v[:, 0] = jnp.zeros_like(recv_v[:, 0])

    def rs_copy(c, o):
        return pltpu.make_async_remote_copy(
            src_ref=send_v.at[c, rows_of(kv_peers[o])],
            dst_ref=recv_v.at[c, o],
            send_sem=rs_ssem.at[c, o],
            recv_sem=rs_rsem.at[c, o],
            device_id={"kv": kv_peers[o]},
            device_id_type=pl.DeviceIdType.MESH,
        )

    def relay_copy(c, end):
        far, near = (kv - 1, 1) if end == 0 else (0, kv - 2)
        return pltpu.make_async_remote_copy(
            src_ref=send_v.at[c, rows_of(far)],
            dst_ref=relay_v.at[c],
            send_sem=relay_ssem.at[c],
            recv_sem=relay_rsem.at[c],
            device_id={"kv": near},
            device_id_type=pl.DeviceIdType.MESH,
        )

    def send_blocks(c):
        if not relayed:
            for o in range(kv - 1):
                rs_copy(c, o).start()
            return

        @pl.when(first)
        def _():
            relay_copy(c, 0).start()
            rs_copy(c, 1).start()
            if c > 0:
                rs_copy(c - 1, 0).start()
            if c == chunks - 1:
                rs_copy(c, 0).start()

        @pl.when(last)
        def _():
            relay_copy(c, kv - 1).start()
            rs_copy(c, 1).start()
            if c > 0:
                rs_copy(c - 1, 2).start()
            if c == chunks - 1:
                rs_copy(c, 2).start()

        @pl.when(jnp.logical_not(at_end))
        def _():
            rs_copy(c, 0).start()
            rs_copy(c, 2).start()

    def send_on(c):
        if relayed:

            @pl.when(jnp.logical_not(at_end))
            def _():
                relay_copy(c, 0).wait_recv()
                far = rows_of(kv_peers[1])
                send_v[c, far, :] = (prod_v[c, far, :] + relay_v[c].astype(F32)).astype(BF16)
                rs_copy(c, 1).start()

    def wait_blocks(c):
        for o in range(kv - 1):
            if relayed and o == 0:
                pl.when(jnp.logical_not(first))(lambda o=o: rs_copy(c, o).wait_recv())
            elif relayed and o == kv - 2:
                pl.when(jnp.logical_not(last))(lambda o=o: rs_copy(c, o).wait_recv())
            else:
                rs_copy(c, o).wait_recv()

    def wait_sent(c):
        if not relayed:
            for o in range(kv - 1):
                rs_copy(c, o).wait_send()
            return
        rs_copy(c, 1).wait_send()

        @pl.when(first)
        def _():
            relay_copy(c, 0).wait_send()
            rs_copy(c, 0).wait_send()

        @pl.when(last)
        def _():
            relay_copy(c, kv - 1).wait_send()
            rs_copy(c, 2).wait_send()

        @pl.when(jnp.logical_not(at_end))
        def _():
            rs_copy(c, 0).wait_send()
            rs_copy(c, 2).wait_send()

    terms = None
    for c in range(chunks):
        for copy in w_c[c]:
            copy.wait()
        product = jnp.dot(scaled_v[...], w_v[c], preferred_element_type=F32)
        prod_v[c] = product
        send_v[c] = product.astype(BF16)
        send_blocks(c)
        if terms is None:
            terms = old_terms()
        if c > 0:
            send_on(c - 1)
        take(c, *terms)
    send_on(chunks - 1)

    squares = ssq_v[rows_of(me), :]
    for o in range(kv - 1):
        ssq_c[o].wait_recv()
        squares = squares + ssq_r[o]
    row_scale = lax.rsqrt(squares[:, :1] / width + EPSILON)
    mine_rows = rows_of(me)
    ag_c = []

    def recur(c):
        wait_blocks(c)

        def projected(i):
            total = prod_v[c, mine_rows, pl.ds(i * cw, cw)]
            for o in range(kv - 1):
                total = total + recv_v[c, o, :, pl.ds(i * cw, cw)].astype(F32)
            return total * row_scale

        column = pl.multiple_of(tme * head_cols + c * cw, cw)
        floor_gate = lb_v[:, pl.ds(column, cw)]
        forget = floor_gate + (1.0 - floor_gate) * jax.nn.sigmoid(projected(1))
        keys = 1.0 - forget
        queries = jax.nn.silu(projected(0)) * HEAD ** (-0.5)
        values = projected(2)
        gate = jax.nn.silu(projected(3)) * hg_v[:, pl.ds(column, cw)]
        start = forget
        for lag in range(1, props):
            start = start * jnp.where(prop >= lag, pltpu.roll(forget, lag, 0), 1.0)
        reading = queries * start
        results = []
        for h in range(CHUNK_HEADS):
            cols = slice(h * HEAD, (h + 1) * HEAD)
            lhs = jnp.concatenate(
                [jnp.where(seq == s, reading[:, cols], 0.0) for s in range(own_seqs)], axis=1
            ).astype(BF16)
            results.append(
                jnp.dot(lhs, tkb_v[c * CHUNK_HEADS + h], preferred_element_type=F32)
            )
        decay = queries
        for lag in range(props):
            if lag > 0:
                decay = decay * (forget if lag == 1 else pltpu.roll(forget, lag - 1, 0))
            pair = decay * (keys if lag == 0 else pltpu.roll(keys, lag, 0))
            pair = jnp.where(prop >= lag, pair, 0.0)
            moved = values if lag == 0 else pltpu.roll(values, lag, 0)
            for h in range(CHUNK_HEADS):
                cols = slice(h * HEAD, (h + 1) * HEAD)
                score = jnp.sum(pair[:, cols], axis=1, keepdims=True)
                results[h] = results[h] + score * moved[:, cols]
        outs = []
        for h in range(CHUNK_HEADS):
            cols = slice(h * HEAD, (h + 1) * HEAD)
            r = results[h]
            normed = r * lax.rsqrt(jnp.mean(r * r, axis=1, keepdims=True) + EPSILON)
            outs.append((normed * gate[:, cols]).astype(BF16))
        gath_v[c, mine_rows, :] = jnp.concatenate(outs, axis=1)
        ag_c.append(
            [
                remote(
                    gath_v.at[c, mine_rows],
                    gath_v.at[c, mine_rows],
                    ag_ssem.at[c, o],
                    ag_rsem.at[c, o],
                    "kv",
                    peer,
                )
                for o, peer in enumerate(kv_peers)
            ]
        )

    def product_of(c, o):
        term = jnp.dot(
            gath_v[c], wo_v[o, pl.ds(c * cw, cw), :], preferred_element_type=F32
        )
        return term if c == 0 else acc_v[o] + term

    def gathered(c):
        for o in range(kv - 1):
            ag_c[c][o].wait_recv()

    for c in range(chunks):
        recur(c)
    for copy in wo_c:
        copy.wait()
    for c in range(chunks - 1):
        gathered(c)
        for o in range(tp):
            acc_v[o] = product_of(c, o)
    gathered(chunks - 1)
    tp_c = []
    for o in range(1, tp):
        part_v[o - 1] = product_of(chunks - 1, o).astype(BF16)
        tp_c.append(
            remote(
                part_v.at[o - 1],
                peer_v.at[o - 1],
                tp_ssem.at[o - 1],
                tp_rsem.at[o - 1],
                "tp",
                tp_peers[o - 1],
            )
        )
    own_v[...] = product_of(chunks - 1, 0).astype(BF16)
    for copy in tp_c:
        copy.wait_recv()
    for c in range(chunks):
        wait_sent(c)
    for copies in [ssq_c, *ag_c, tp_c]:
        for copy in copies:
            copy.wait_send()


def kernel_line(
    tp,
    tokens,
    w_query,
    w_forget,
    w_input,
    w_gate,
    w_out,
    gain,
    head_gain,
    lower_bound,
    state,
    last_forget,
    last_values,
    accepted,
    tk_v,
    acc_v,
    last_v,
    wl_v,
    tok_v,
    gain_v,
    hg_v,
    lb_v,
    lf_v,
    lv_v,
    rows_v,
    scaled_v,
    w_v,
    wo_v,
    st_v,
    tkb_v,
    lfr_v,
    lvr_v,
    ssq_v,
    ssq_s,
    ssq_r,
    prod_v,
    send_v,
    recv_v,
    gath_v,
    acc_s,
    load_sem,
    w_sem,
    wo_sem,
    st_sem,
    ssq_ssem,
    ssq_rsem,
    rs_ssem,
    rs_rsem,
    ag_ssem,
    ag_rsem,
    cross_rsem,
    fw_ssem,
    fw_rsem,
    wo_ssem,
    wo_rsem,
    go_sem,
):
    kv = LINE
    me = lax.axis_index("kv")
    tme = lax.axis_index("tp")
    seqs, props, feat = tokens.shape
    own_seqs, heads_dev = state.shape[0], state.shape[1]
    own_rows = own_seqs * props
    rows = seqs * props
    width = gain.shape[1]
    head_cols = heads_dev * HEAD
    chunks = heads_dev // LINE_HEADS
    cw = LINE_HEADS * HEAD
    half = w_out.shape[1] // tp
    weights = (w_query, w_forget, w_input, w_gate)

    at_end = jnp.logical_or(me == 0, me == kv - 1)

    def local(src, dst, sem):
        copy = pltpu.make_async_copy(src, dst, sem)
        copy.start()
        return copy

    tok_c = local(tokens, tok_v, load_sem.at[0])
    gain_c = local(gain, gain_v, load_sem.at[1])

    def held(ref, sem):
        pltpu.make_async_copy(ref, ref, sem).wait()

    def load_w(c):
        for i, w in enumerate(weights):
            local(w.at[:, pl.ds(c * cw, cw)], w_v.at[c, :, pl.ds(i * cw, cw)], w_sem.at[c])

    def load_late():
        small = [
            local(last_forget, lf_v, load_sem.at[2]),
            local(last_values, lv_v, load_sem.at[3]),
            local(head_gain, hg_v, load_sem.at[4]),
            local(lower_bound, lb_v, load_sem.at[5]),
            local(accepted, acc_s, load_sem.at[6]),
        ]
        return small, local(state, st_v, st_sem)

    split = (chunks - 1) * cw
    crossed = chunks - CROSS

    def load_out():
        cols = pl.ds(pl.multiple_of(tme * half, half), half)
        local(w_out.at[:split, cols], wo_v.at[0], wo_sem)
        local(w_out.at[split:, cols], wl_v.at[0], wo_sem)

    def out_held(sem):
        held(w_v.at[0, : head_cols * half // (4 * cw)], sem)

    load_w(0)

    def signal(axis, peer):
        pl.semaphore_signal(
            barrier, inc=1, device_id={axis: peer}, device_id_type=pl.DeviceIdType.MESH
        )

    barrier = pltpu.get_barrier_semaphore()
    tp_peers = [lax.rem(tme + o, tp) for o in range(1, tp)]
    for peer in tp_peers:
        signal("tp", peer)

    @pl.when(me > 0)
    def _():
        signal("kv", me - 1)

    @pl.when(me < kv - 1)
    def _():
        signal("kv", me + 1)

    def remote(src, dst, ssem, rsem, axis, peer):
        return pltpu.make_async_remote_copy(
            src_ref=src,
            dst_ref=dst,
            send_sem=ssem,
            recv_sem=rsem,
            device_id={axis: peer},
            device_id_type=pl.DeviceIdType.MESH,
        )

    gain_c.wait()
    load_w(1)
    tok_c.wait()
    load_w(2)
    for s in range(seqs):
        rows_v[pl.ds(s * props, props), :] = tok_v[s].astype(F32)
    x = rows_v[...]
    my_gain = gain_v[:, pl.ds(pl.multiple_of(me * feat, feat), feat)]
    scaled_v[...] = (x * my_gain).astype(BF16)

    def rows_of(device):
        return pl.ds(pl.multiple_of(device * own_rows, own_rows), own_rows)

    def message(c, name):
        _, to, dest, slot = MESSAGES[name]
        return remote(
            send_v.at[c, rows_of(dest)],
            recv_v.at[c, slot],
            rs_ssem,
            rs_rsem.at[c, max(slot - OWN + 1, 0)],
            "kv",
            to,
        )

    def pass_on(c, name, onward):
        _, _, dest, slot = MESSAGES[name]
        message(c, name).wait_recv()
        into = rows_of(dest)
        send_v[c, into, :] = (prod_v[c, into, :] + recv_v[c, slot].astype(F32)).astype(BF16)
        message(c, onward).start()

    def ssq_copy(i, slot, to):
        return remote(ssq_s.at[i], ssq_r.at[slot], ssq_ssem.at[i], ssq_rsem.at[slot], "kv", to)

    partner = me + 1 - 2 * lax.rem(me, 2)
    across = jnp.where(me == 1, 2, 1)
    beyond = jnp.where(me == 1, 3, 0)
    inside = jnp.logical_not(at_end)
    pl.semaphore_wait(barrier, jnp.where(at_end, tp, tp + 1))
    def go(to):
        pl.semaphore_signal(
            go_sem, inc=1, device_id={"kv": to}, device_id_type=pl.DeviceIdType.MESH
        )

    @pl.when(inside)
    def _():
        go(across)

    direct = chunks - DIRECT

    def terms_of(c):
        return (me == 0) if c < direct else (me < 2)


    place = lax.broadcasted_iota(jnp.int32, (own_rows, 1), 0)
    prop = lax.rem(place, props)
    seq = place // props

    def old_terms():
        for copy in small_c:
            copy.wait()
        for s in range(own_seqs):
            lfr_v[pl.ds(s * props, props), :] = lf_v[s]
            lvr_v[pl.ds(s * props, props), :] = lv_v[s].astype(F32)
        limit = jnp.zeros((own_rows, 1), jnp.int32)
        for s in range(own_seqs):
            limit = jnp.where(seq == s, acc_s[s], limit)
        mask = prop < limit
        old = lfr_v[...]
        decay = jnp.where(mask, old, 1.0)
        weight = jnp.where(mask, 1.0 - old, 0.0)
        after = jnp.ones_like(decay)
        for lag in range(1, props):
            after = after * jnp.where(
                prop < props - lag, pltpu.roll(decay, own_rows - lag, 0), 1.0
            )
        return decay * after, weight * after, lvr_v[...].astype(BF16)

    def take(c, ends, old_weight, old_values):
        if c == 0:
            st_c.wait()
        lane_seq = lax.broadcasted_iota(jnp.int32, (1, own_rows), 1) // props
        for h in range(c * LINE_HEADS, (c + 1) * LINE_HEADS):
            cols = slice(h * HEAD, (h + 1) * HEAD)
            end_t = ends[:, cols].T
            weight_t = old_weight[:, cols].T
            for s in range(own_seqs):
                mine = jnp.where(lane_seq == s, weight_t, 0.0).astype(BF16)
                added = jnp.dot(mine, old_values[:, cols], preferred_element_type=F32)
                new = end_t[:, s * props : s * props + 1] * st_v[s, h] + added
                tk_v[s, h] = new
                tkb_v[h, pl.ds(s * HEAD, HEAD), :] = new.astype(BF16)

    for c in range(chunks):
        held(w_v.at[c], w_sem.at[c])
        if c + 3 < chunks:
            load_w(c + 3)
        elif c + 3 == chunks:
            small_c, st_c = load_late()
        elif c + 2 == chunks:
            load_out()
        product = jnp.dot(scaled_v[...], w_v[c], preferred_element_type=F32)
        prod_v[c] = product
        send_v[c] = product.astype(BF16)

        @pl.when(me == 0)
        def _():
            message(c, "0 for 3").start()

        @pl.when(me == 1)
        def _():
            message(c, "1 to 0").start()

        @pl.when(me == 2)
        def _():
            message(c, "2 to 3").start()
            if c == 0:
                pl.semaphore_wait(go_sem, 1)
                go(3)
            message(c, "2 to 0").start()
            if c >= direct:
                message(c, "2 to 1").start()

        @pl.when(me == 3)
        def _():
            if c == direct:
                pl.semaphore_wait(go_sem, 1)
            message(c, "3 to 1" if c >= direct else "3 for 1").start()

        if c == 0:
            x = rows_v[...]
            squared = jnp.sum(x * x, axis=1, keepdims=True)
            on_row = lax.broadcasted_iota(jnp.int32, (rows, HEAD), 0)
            on_lane = lax.broadcasted_iota(jnp.int32, (rows, HEAD), 1)
            along = jnp.sum(jnp.where(on_row == on_lane, squared, 0.0), axis=0, keepdims=True)
            ssq_v[...] = along
            ssq_s[0] = along
            ssq_copy(0, 0, partner).start()

    @pl.when(me == 0)
    def _():
        for name in ("0 for 2", "0 to 1"):
            for c in range(chunks):
                message(c, name).start()

    @pl.when(me == 3)
    def _():
        for name in ("3 to 2", "3 to 0"):
            for c in range(chunks):
                message(c, name).start()

    for c in range(chunks):

        @pl.when(jnp.logical_not(terms_of(c)))
        def _():
            recv_v[c, OWN - 1] = jnp.zeros_like(recv_v[c, OWN - 1])

    terms = old_terms()
    ssq_copy(0, 0, partner).wait_recv()

    @pl.when(me == 1)
    def _():
        pl.semaphore_wait(go_sem, 1)

    @pl.when(inside)
    def _():
        ssq_s[1] = ssq_v[...] + ssq_r[0]
        ssq_copy(1, 1, across).start()
        ssq_s[2] = ssq_v[...] + ssq_r[0]
        ssq_copy(2, 1, beyond).start()

    for c in range(chunks):
        @pl.when(me == 1)
        def _():
            pass_on(c, "0 for 3", "1 to 3")

        if c < direct:

            @pl.when(me == 2)
            def _():
                pass_on(c, "3 for 1", "2 to 1")

        take(c, *terms)

    @pl.when(me == 1)
    def _():
        for c in range(chunks):
            pass_on(c, "0 for 2", "1 to 2")

    for o in range(1, tp):
        cols = pl.ds(pl.multiple_of(tp_peers[o - 1] * half, half), half)
        for rows_out, into in ((w_out.at[:split, cols], wo_v), (w_out.at[split:, cols], wl_v)):
            copy = remote(
                rows_out, into.at[tp - o], wo_ssem.at[o - 1], wo_rsem.at[tp - o - 1],
                "tp", tp_peers[o - 1],
            )
            copy.start()

    ssq_copy(1, 1, partner).wait_recv()
    whole = ssq_v[...] + ssq_r[0] + ssq_r[1]
    mine_rows = rows_of(me)
    picked = lax.broadcasted_iota(jnp.int32, (own_rows, HEAD), 1) == (
        lax.broadcasted_iota(jnp.int32, (own_rows, HEAD), 0) + me * own_rows
    )
    squares = jnp.sum(jnp.where(picked, whole[:1], 0.0), axis=1, keepdims=True)
    row_scale = lax.rsqrt(squares / width + EPSILON)
    peers = [
        functools.reduce(lambda found, d: jnp.where(me == d, PEERS[d][o], found), range(kv), 0)
        for o in range(kv - 1)
    ]

    def heads_of(c, slot):
        return gath_v.at[slot, c] if c < chunks - 1 else last_v.at[slot]

    def head_copy(c, o):
        mine = heads_of(c, 0).at[mine_rows]
        return remote(mine, mine, ag_ssem, ag_rsem.at[c], "kv", peers[o])

    def cross_copy(c, o, i):
        ids = {"tp": tp_peers[o - 1]}
        if i < kv - 1:
            ids["kv"] = peers[i]
        return pltpu.make_async_remote_copy(
            src_ref=heads_of(c, 0).at[mine_rows],
            dst_ref=heads_of(c, tp - o).at[mine_rows],
            send_sem=ag_ssem,
            recv_sem=cross_rsem.at[c - crossed, tp - o - 1],
            device_id=ids,
            device_id_type=pl.DeviceIdType.MESH,
        )

    def cross_copies(c):
        return [cross_copy(c, o, i) for o in range(1, tp) for i in range(kv)]

    def forward(c, o):
        return remote(
            gath_v.at[0, c], gath_v.at[tp - o, c], fw_ssem.at[o - 1],
            fw_rsem.at[c, tp - o - 1], "tp", tp_peers[o - 1],
        )

    def send_heads(c, o):
        if o < kv - 1:
            head_copy(c, o).start()
        if c >= crossed:
            for away in range(1, tp):
                cross_copy(c, away, o).start()

    def recur(c):
        @pl.when(terms_of(c))
        def _():
            held(recv_v.at[c, :OWN], rs_rsem.at[c, 0])

        @pl.when(jnp.logical_not(terms_of(c)))
        def _():
            held(recv_v.at[c, : OWN - 1], rs_rsem.at[c, 0])

        def projected(i):
            cols = pl.ds(i * cw, cw)
            total = prod_v[c, mine_rows, cols]
            for slot in range(OWN):
                total = total + recv_v[c, slot, :, cols].astype(F32)
            return total * row_scale

        column = pl.multiple_of(tme * head_cols + c * cw, cw)
        floor_gate = lb_v[:, pl.ds(column, cw)]
        forget = floor_gate + (1.0 - floor_gate) * jax.nn.sigmoid(projected(1))
        keys = 1.0 - forget
        queries = jax.nn.silu(projected(0)) * HEAD ** (-0.5)
        values = projected(2)
        gate = jax.nn.silu(projected(3)) * hg_v[:, pl.ds(column, cw)]
        start = forget
        for lag in range(1, props):
            start = start * jnp.where(prop >= lag, pltpu.roll(forget, lag, 0), 1.0)
        reading = queries * start
        results = []
        for h in range(LINE_HEADS):
            cols = slice(h * HEAD, (h + 1) * HEAD)
            lhs = jnp.concatenate(
                [jnp.where(seq == s, reading[:, cols], 0.0) for s in range(own_seqs)], axis=1
            ).astype(BF16)
            results.append(
                jnp.dot(lhs, tkb_v[c * LINE_HEADS + h], preferred_element_type=F32)
            )
        decay = queries
        for lag in range(props):
            if lag > 0:
                decay = decay * (forget if lag == 1 else pltpu.roll(forget, lag - 1, 0))
            pair = decay * (keys if lag == 0 else pltpu.roll(keys, lag, 0))
            pair = jnp.where(prop >= lag, pair, 0.0)
            moved = values if lag == 0 else pltpu.roll(values, lag, 0)
            for h in range(LINE_HEADS):
                cols = slice(h * HEAD, (h + 1) * HEAD)
                score = jnp.sum(pair[:, cols], axis=1, keepdims=True)
                results[h] = results[h] + score * moved[:, cols]
        outs = []
        for h in range(LINE_HEADS):
            cols = slice(h * HEAD, (h + 1) * HEAD)
            r = results[h]
            normed = r * lax.rsqrt(jnp.mean(r * r, axis=1, keepdims=True) + EPSILON)
            outs.append((normed * gate[:, cols]).astype(BF16))
        heads_of(c, 0)[mine_rows, :] = jnp.concatenate(outs, axis=1)
        for o in (0, 1, kv - 1):
            send_heads(c, o)

        @pl.when(me != 2)
        def _():
            send_heads(c, 2)

        if c >= 2:

            @pl.when(me == 2)
            def _():
                send_heads(c - 2, 2)

    def gathered(c):
        held(heads_of(c, 0).at[: (kv - 1) * own_rows], ag_rsem.at[c])

    def product_of(c, slot):
        term = jnp.dot(
            gath_v[slot, c], wo_v[slot, pl.ds(c * cw, cw), :], preferred_element_type=F32
        )
        acc_v[slot] = term if c == 0 else acc_v[slot] + term

    def from_tp(c):
        for o in range(1, tp):
            if c < crossed:
                forward(c, tp - o).wait_recv()
                continue
            held(heads_of(c, o), cross_rsem.at[c - crossed, o - 1])

    for c in range(chunks):
        recur(c)

    @pl.when(me == 2)
    def _():
        for c in range(chunks - 2, chunks):
            send_heads(c, 2)

    out_held(wo_sem)
    for o in range(1, tp):
        out_held(wo_rsem.at[o - 1])
    for c in range(chunks):
        gathered(c)
        if c < crossed:
            for o in range(1, tp):
                forward(c, o).start()
        if c < chunks - 1:
            product_of(c, 0)
        if c == chunks - 2:
            for early in range(chunks - 2):
                from_tp(early)
                for o in range(1, tp):
                    product_of(early, o)
    for c in range(chunks - 2, chunks):
        from_tp(c)
        if c < chunks - 1:
            for o in range(1, tp):
                product_of(c, o)

    held(send_v.at[:, : (kv - 1) * own_rows], rs_ssem)
    ssq_copy(0, 0, partner).wait_send()

    @pl.when(inside)
    def _():
        ssq_copy(1, 1, across).wait_send()
        ssq_copy(2, 1, beyond).wait_send()

    blocks = chunks * (kv - 1) + CROSS * (tp - 1) * kv
    held(w_v.at[0, : blocks * own_rows // 4], ag_ssem)
    for o in range(1, tp):
        out_held(wo_ssem.at[o - 1])
    for o in range(1, tp):
        held(gath_v.at[0, :crossed], fw_ssem.at[o - 1])


def finish_line(tk_v, acc_v, last_v, wl_v, mixed, taken, mix_v, sem):
    tk_c = pltpu.make_async_copy(tk_v, taken, sem.at[0])
    tk_c.start()
    seqs, props, _ = mixed.shape
    total = 0.0
    for slot in range(acc_v.shape[0]):
        term = jnp.dot(last_v[slot], wl_v[slot], preferred_element_type=F32)
        total = total + (acc_v[slot] + term).astype(BF16).astype(F32)
    for s in range(seqs):
        mix_v[s] = total[s * props : (s + 1) * props].astype(BF16)
    mix_c = pltpu.make_async_copy(mix_v, mixed, sem.at[1])
    mix_c.start()
    mix_c.wait()
    tk_c.wait()


def finish(tk_v, own_v, peer_v, mixed, taken, mix_v, sem):
    tk_c = pltpu.make_async_copy(tk_v, taken, sem.at[0])
    tk_c.start()
    seqs, props, _ = mixed.shape
    total = own_v[...].astype(F32)
    for o in range(peer_v.shape[0]):
        total = total + peer_v[o].astype(F32)
    for s in range(seqs):
        mix_v[s] = total[s * props : (s + 1) * props].astype(BF16)
    mix_c = pltpu.make_async_copy(mix_v, mixed, sem.at[1])
    mix_c.start()
    mix_c.wait()
    tk_c.wait()


def per_device(
    kv,
    tp,
    tokens,
    w_query,
    w_forget,
    w_input,
    w_gate,
    w_out,
    gain,
    head_gain,
    lower_bound,
    state,
    last_forget,
    last_values,
    accepted,
):
    seqs, props, feat = tokens.shape
    own_seqs, heads_dev = state.shape[0], state.shape[1]
    own_rows = own_seqs * props
    rows = seqs * props
    head_cols = heads_dev * HEAD
    on_line = kv == LINE and rows <= HEAD
    per_chunk = LINE_HEADS if on_line else CHUNK_HEADS
    chunks = heads_dev // per_chunk
    cw = per_chunk * HEAD
    half = w_out.shape[1] // tp
    peers = kv - 1
    dma = pltpu.SemaphoreType.DMA
    scratch = [
        pltpu.VMEM(tokens.shape, BF16),
        pltpu.VMEM((1, gain.shape[0]), F32),
        pltpu.VMEM((1, head_gain.shape[0]), F32),
        pltpu.VMEM((1, lower_bound.shape[0]), F32),
        pltpu.VMEM(last_forget.shape, F32),
        pltpu.VMEM(last_values.shape, BF16),
        pltpu.VMEM((rows, feat), F32),
        pltpu.VMEM((rows, feat), BF16),
        pltpu.VMEM((chunks, feat, 4 * cw), BF16),
        pltpu.VMEM((tp, head_cols, half), BF16),
        pltpu.VMEM(state.shape, F32),
        pltpu.VMEM((heads_dev, own_seqs * HEAD, HEAD), BF16),
        pltpu.VMEM((own_rows, head_cols), F32),
        pltpu.VMEM((own_rows, head_cols), F32),
    ]
    if on_line:
        body, last = functools.partial(kernel_line, tp), finish_line
        scratch[9] = pltpu.VMEM((tp, head_cols - cw, half), BF16)
        outs = (
            pltpu.VMEM(state.shape, F32),
            pltpu.VMEM((tp, rows, half), F32),
            pltpu.VMEM((tp, rows, cw), BF16),
            pltpu.VMEM((tp, cw, half), BF16),
        )
        scratch += [
            pltpu.VMEM((1, HEAD), F32),
            pltpu.VMEM((3, 1, HEAD), F32),
            pltpu.VMEM((2, 1, HEAD), F32),
            pltpu.VMEM((chunks, rows, 4 * cw), F32),
            pltpu.VMEM((chunks, rows, 4 * cw), BF16),
            pltpu.VMEM((chunks, 5, own_rows, 4 * cw), BF16),
            pltpu.VMEM((tp, chunks - 1, rows, cw), BF16),
            pltpu.SMEM((own_seqs,), jnp.int32),
            dma((7,)),
            dma((chunks,)),
            dma,
            dma,
            dma((3,)),
            dma((2,)),
            dma,
            dma((chunks, 3)),
            dma,
            dma((chunks,)),
            dma((CROSS, tp - 1)),
            dma((tp - 1,)),
            dma((chunks - CROSS, tp - 1)),
            dma((tp - 1,)),
            dma((tp - 1,)),
            pltpu.SemaphoreType.REGULAR,
        ]
    else:
        body, last = functools.partial(kernel_any, kv, tp), finish
        outs = (
            pltpu.VMEM(state.shape, F32),
            pltpu.VMEM((rows, half), BF16),
            pltpu.VMEM((tp - 1, rows, half), BF16),
        )
        scratch += [
            pltpu.VMEM((rows, HEAD), F32),
            pltpu.VMEM((peers, own_rows, HEAD), F32),
            pltpu.VMEM((chunks, rows, 4 * cw), F32),
            pltpu.VMEM((chunks, rows, 4 * cw), BF16),
            pltpu.VMEM((chunks, peers, own_rows, 4 * cw), BF16),
            pltpu.VMEM((chunks, rows, cw), BF16),
            pltpu.VMEM((tp, rows, half), F32),
            pltpu.VMEM((tp - 1, rows, half), BF16),
            pltpu.VMEM((chunks, own_rows, 4 * cw), BF16),
            dma((6,)),
            dma((chunks, 4)),
            dma((tp,)),
            dma((chunks,)),
            dma((peers,)),
            dma((peers,)),
            dma((chunks, peers)),
            dma((chunks, peers)),
            dma((chunks,)),
            dma((chunks,)),
            dma((chunks, peers)),
            dma((chunks, peers)),
            dma((tp - 1,)),
            dma((tp - 1,)),
        ]
    anywhere = pl.BlockSpec(memory_space=pl.ANY)
    held = pl.BlockSpec(memory_space=pltpu.VMEM)
    results = pl.pallas_call(
        body,
        out_shape=outs,
        in_specs=[pl.BlockSpec(memory_space=pltpu.HBM)] * 12
        + [pl.BlockSpec(memory_space=pltpu.HBM if on_line else pltpu.SMEM)],
        out_specs=(held,) * len(outs),
        scratch_shapes=scratch,
        compiler_params=pltpu.CompilerParams(
            collective_id=0, has_side_effects=True, vmem_limit_bytes=VMEM_MIB * 1024 * 1024
        ),
    )(
        tokens,
        w_query,
        w_forget,
        w_input,
        w_gate,
        w_out,
        gain.reshape(1, -1),
        head_gain.reshape(1, -1),
        lower_bound.reshape(1, -1),
        state,
        last_forget,
        last_values,
        accepted,
    )
    return pl.pallas_call(
        last,
        out_shape=(
            jax.ShapeDtypeStruct((seqs, props, half), BF16),
            jax.ShapeDtypeStruct(state.shape, F32),
        ),
        in_specs=[held] * len(outs),
        out_specs=(anywhere, anywhere),
        scratch_shapes=[pltpu.VMEM((seqs, props, half), BF16), dma((2,))],
        compiler_params=pltpu.CompilerParams(vmem_limit_bytes=4 * 1024 * 1024),
    )(*results)


def solution(mesh):
    in_specs = (
        P(("grp", "dp"), None, "kv"),
        P("kv", "tp"),
        P("kv", "tp"),
        P("kv", "tp"),
        P("kv", "tp"),
        P("tp", "kv"),
        P(),
        P(),
        P(),
        P(("grp", "dp", "kv"), "tp", None, None),
        P(("grp", "dp", "kv"), None, "tp"),
        P(("grp", "dp", "kv"), None, "tp"),
        P(("grp", "dp", "kv")),
    )
    out_specs = (P(("grp", "dp"), None, ("kv", "tp")), P(("grp", "dp", "kv"), "tp", None, None))
    return jax.shard_map(
        functools.partial(per_device, mesh.shape["kv"], mesh.shape["tp"]),
        mesh=mesh,
        in_specs=in_specs,
        out_specs=out_specs,
        check_vma=False,
    )
```
